256 devices in a mesh: grp: 2 (over y), sp: 16 (over z), tp: 4 (over x), dp: 2 (over core).
Axes of the slice: x: 4, y: 2, z: 16, core: 2. Of those that a mesh axis runs over, the one named last changes fastest.
The devices are a block of a 4x16x16 slice.
Arguments:
- latent: bfloat16 [24576, 4096], P(('grp', 'sp', 'dp')), parts along dimension 0, may hold values from -6 to 6
- context: bfloat16 [1024, 4096], P(('grp', 'sp')), parts along dimension 0, may hold values from -6 to 6
- condition: bfloat16 [8192], P('grp'), parts along dimension 0, may hold values from -6 to 6
- context_condition: bfloat16 [4096], replicated, may hold values from -6 to 6
- shift_weight: bfloat16 [4096, 4096], P('sp', ('tp', 'dp')), may hold values from -0.09375 to 0.09375
- scale_weight: bfloat16 [4096, 4096], P('sp', ('tp', 'dp')), may hold values from -0.09375 to 0.09375
- gate_weight: bfloat16 [4096, 4096], P('sp', ('tp', 'dp')), may hold values from -0.09375 to 0.09375
- norm_gain: float32 [4096], replicated, may hold values from 0.1 to 1.9
- out_gate_weight: bfloat16 [4096, 2048], P(None, ('tp', 'dp')), may hold values from -0.09375 to 0.09375
- signal_weight: bfloat16 [4096, 2048], P(None, ('tp', 'dp')), may hold values from -0.09375 to 0.09375
- writer_weight: bfloat16 [4096, 1024], P(None, ('tp', 'dp')), may hold values from -0.09375 to 0.09375
- reader_matrix: bfloat16 [4096, 1024], P(None, ('tp', 'dp')), may hold values from -0.09375 to 0.09375
- step_weight: bfloat16 [2, 4096, 32], P(None, None, ('tp', 'dp')), may hold values from -0.09375 to 0.09375
- signal_taps: float32 [3, 2048], P(None, ('tp', 'dp')), may hold values from -3.5 to 3.5
- writer_taps: float32 [3, 1024], P(None, ('tp', 'dp')), may hold values from -3.5 to 3.5
- reader_taps: float32 [3, 1024], P(None, ('tp', 'dp')), may hold values from -3.5 to 3.5
- step_bias: float32 [2, 32], P(None, ('tp', 'dp')), may hold values from -4.5 to -2.5
- decay_log: float32 [2, 32], P(None, ('tp', 'dp')), may hold values from -12 to 1
- decay_extra: float32 [2, 32, 24576], P(None, ('tp', 'dp'), ('grp', 'sp')), parts along dimension 2, may hold values from -3 to 0
- group_gain: float32 [2048], P(('tp', 'dp')), may hold values from 0.1 to 1.9
- output_weight: bfloat16 [2048, 4096], P(None, ('tp', 'dp')), may hold values from -0.125 to 0.125
Outputs:
- updated: bfloat16 [24576, 4096], P(('grp', 'sp'), ('tp', 'dp')), parts along dimension 0
The draws below stay inside these ranges and needn't reach their ends.
There are 2 independent parts, one for each index of `grp`. The reference program is written for one: setup_inputs(seed, part) draws one part's arguments, and reference() takes and returns one part's arrays. A program takes and returns all parts, laid end to end along the dimension named above; an argument that names none is the same for every part. Nothing has to cross between parts.
All inputs are finite; a program needn't handle non-finite values.
Results may differ from the reference program's by a relative error of at most 0.007.
Values may be sent and summed in bfloat16 or wider, within the bound.
A program may use at most 128 MiB of HBM per device.

```python
import math
import jax
import jax.numpy as jnp
from jax import lax

D = 4096
HEADS = 32
HEAD_DIM = 64
GROUPS = 8
STATE = 128
W_INNER = 2048
BLOCK = 128
TAPS = 3
TOK_DEV = 768
TOKENS = 12288
CTX = 512


def draw_decay_log(key, part):
    first, second, third = jax.random.split(key, 3)
    chain_len = TOKENS + CTX
    slow = jax.random.uniform(first, (2, HEADS), jnp.float32, math.log(2.0 / chain_len), math.log(10.0 / chain_len))
    fast = jax.random.uniform(second, (2, HEADS), jnp.float32, math.log(0.5), math.log(2.0))
    picks = jax.random.randint(third, (2, HEADS), 0, 2)
    chosen = jnp.where(picks == 1, fast, slow)
    return chosen


def draw_decay_extra(key, part):
    first, second, third = jax.random.split(key, 3)
    span_count = TOKENS // TOK_DEV
    low_end, high_end = (0.1, 1.2)
    rate = jnp.exp(jax.random.uniform(first, (2, HEADS, span_count), jnp.float32, math.log(low_end), math.log(high_end))) / TOKENS
    equilibrium_memory = jnp.repeat(rate, TOK_DEV, axis=2)
    spots = jax.random.randint(second, (2, HEADS, 4), 0, TOKENS)
    stack_level_index = jax.random.uniform(third, (2, HEADS, 4), jnp.float32, math.log(0.5), math.log(0.8))
    places = lax.iota(jnp.int32, TOKENS)
    agreeing_tally = places[None, None, None, :] == spots[..., None]
    latent_block_tally = jnp.sum(jnp.where(agreeing_tally, stack_level_index[..., None], 0.0), axis=2)
    return latent_block_tally - equilibrium_memory


def level_of(rng, dims, shards, smallest, largest):
    factor_of, own = 1.0, jax.random.fold_in(rng, 6)
    for dim, blocks in shards:
        steps = jnp.exp(jax.random.uniform(jax.random.fold_in(own, dim), (blocks,), jnp.float32, smallest / len(shards), largest / len(shards)))
        factor_of = factor_of * jnp.repeat(steps, dims[dim] // blocks).reshape([-1 if axis == dim else 1 for axis in range(len(dims))])
    return factor_of


def bell_draw(stream_key, dims, spread, most, pieces=(), kind=jnp.bfloat16):
    level = level_of(stream_key, dims, pieces, -0.22, 0.18) if pieces else 1.0
    entries = jax.random.normal(stream_key, dims, jnp.float32) * spread * level
    return jnp.minimum(jnp.maximum(entries, -most), most).astype(kind)


def setup_inputs(seed: int = 0, part: int = 0) -> dict:
    arg_keys = jax.random.split(jax.random.key(seed), 22)
    part_splits = jax.random.split(jax.random.fold_in(arg_keys[21], part), 22)
    return {
        "latent": bell_draw(part_splits[0], (TOKENS, D), 1.0, 6.0, ((0, 32),)),
        "context": bell_draw(part_splits[1], (CTX, D), 1.0, 6.0, ((0, 16),)),
        "condition": bell_draw(part_splits[2], (D,), 1.0, 6.0),
        "context_condition": bell_draw(arg_keys[3], (D,), 1.0, 6.0),
        "shift_weight": bell_draw(arg_keys[4], (D, D), D ** -0.5, 0.09375, ((0, 16), (1, 8))),
        "scale_weight": bell_draw(arg_keys[5], (D, D), D ** -0.5, 0.09375, ((0, 16), (1, 8))),
        "gate_weight": bell_draw(arg_keys[6], (D, D), D ** -0.5, 0.09375, ((0, 16), (1, 8))),
        "norm_gain": jnp.clip(1.0 + 0.18 * jax.random.normal(arg_keys[7], (D,), jnp.float32), 0.1, 1.9),
        "out_gate_weight": bell_draw(arg_keys[8], (D, W_INNER), D ** -0.5, 0.09375, ((1, 8),)),
        "signal_weight": bell_draw(arg_keys[9], (D, W_INNER), D ** -0.5, 0.09375, ((1, 8),)),
        "writer_weight": bell_draw(arg_keys[10], (D, GROUPS * STATE), D ** -0.5, 0.09375, ((1, 8),)),
        "reader_matrix": bell_draw(arg_keys[11], (D, GROUPS * STATE), D ** -0.5, 0.09375, ((1, 8),)),
        "step_weight": bell_draw(arg_keys[12], (2, D, HEADS), D ** -0.5, 0.09375, ((2, 8),)),
        "signal_taps": bell_draw(arg_keys[13], (TAPS, W_INNER), TAPS ** -0.5, 3.5, ((1, 8),), jnp.float32),
        "writer_taps": bell_draw(arg_keys[14], (TAPS, GROUPS * STATE), TAPS ** -0.5, 3.5, ((1, 8),), jnp.float32),
        "reader_taps": bell_draw(arg_keys[15], (TAPS, GROUPS * STATE), TAPS ** -0.5, 3.5, ((1, 8),), jnp.float32),
        "step_bias": jnp.clip(-4.5 + 2.0 * jax.random.uniform(arg_keys[16], (2, HEADS), jnp.float32) ** level_of(arg_keys[16], (2, HEADS), ((1, 8),), -0.2, 0.2), -4.5, -2.5),
        "decay_log": draw_decay_log(jax.random.fold_in(arg_keys[21], 71), part),
        "decay_extra": draw_decay_extra(jax.random.fold_in(jax.random.fold_in(arg_keys[21], part), 71), part),
        "group_gain": jnp.clip(1.0 + 0.18 * jax.random.normal(arg_keys[19], (W_INNER,), jnp.float32), 0.1, 1.9),
        "output_weight": bell_draw(arg_keys[20], (W_INNER, D), W_INNER ** -0.5, 0.125, ((1, 8),)),
    }


EPSILON = 1e-06
HIGHEST = lax.Precision.HIGHEST

def modulate(rows, norm_gain, shift_vec, scale_vec):
    values = rows.astype(jnp.float32)
    normed = values * lax.rsqrt(lax.optimization_barrier(jnp.mean(values * values, axis=-1, keepdims=True)) + EPSILON) * norm_gain
    return (normed * (1.0 + scale_vec) + shift_vec).astype(jnp.bfloat16)

def centred_conv(padded, conv_taps, length):
    running = jnp.zeros((length, padded.shape[1]), jnp.float32)
    for offset in range(conv_taps.shape[0]):
        running = running + conv_taps[offset] * padded[offset:offset + length].astype(jnp.float32)
    return jax.nn.silu(running)

def project_rows(hidden, signal_weight, writer_weight, reader_matrix, step_weight):
    raw_cols = jnp.concatenate([jnp.dot(hidden, signal_weight, preferred_element_type=jnp.float32), jnp.dot(hidden, writer_weight, preferred_element_type=jnp.float32), jnp.dot(hidden, reader_matrix, preferred_element_type=jnp.float32)], axis=1).astype(jnp.bfloat16)
    step_in = jnp.stack([jnp.dot(hidden, step_weight[0], preferred_element_type=jnp.float32), jnp.dot(hidden, step_weight[1], preferred_element_type=jnp.float32)]).astype(jnp.bfloat16)
    return (raw_cols, step_in)

def split_mixed(conv_out, head_count, head_width, group_count, state_width):
    length = conv_out.shape[0]
    signal_end = head_count * head_width
    writer_end = signal_end + group_count * state_width
    signal = conv_out[:, :signal_end].reshape(length, head_count, head_width)
    writer = conv_out[:, signal_end:writer_end].reshape(length, group_count, state_width)
    reader = conv_out[:, writer_end:].reshape(length, group_count, state_width)
    return (signal, writer, reader)

def state_span(signal, step_size, log_decay, writer, reader, start_state, block):
    length, head_count, head_width = signal.shape
    group_count, state_width = (writer.shape[1], writer.shape[2])
    per_group = head_count // group_count
    blocks = length // block
    scaled = (signal * step_size[..., None]).reshape(blocks, block, group_count, per_group, head_width)
    cum_log = jnp.cumsum(log_decay.reshape(blocks, block, group_count, per_group), axis=1)
    writer_blk = writer.reshape(blocks, block, group_count, state_width)
    reader_blk = reader.reshape(blocks, block, group_count, state_width)
    inner_dot = jnp.einsum('bign,bjgn->bgij', reader_blk, writer_blk, precision=HIGHEST)
    moved = jnp.moveaxis(cum_log, 1, -1)
    gap_logs = moved[..., :, None] - moved[..., None, :]
    lower_mask = jnp.tril(jnp.ones((block, block), dtype=bool))
    weights = jnp.exp(jnp.where(lower_mask, gap_logs, -jnp.inf))
    in_block = jnp.einsum('bgij,bgeij,bjgep->bigep', inner_dot, weights, scaled, precision=HIGHEST)
    to_end = jnp.exp(cum_log[:, -1:] - cum_log)
    states = jnp.einsum('bjgn,bjge,bjgep->bgepn', writer_blk, to_end, scaled, precision=HIGHEST)
    block_decay = jnp.exp(cum_log[:, -1])

    def advance(running, block_item):
        state_add, decay_now = block_item
        return (running * decay_now[..., None, None] + state_add, running)
    last_state, before = lax.scan(advance, start_state.reshape(group_count, per_group, head_width, state_width), (states, block_decay))
    carried = jnp.einsum('bign,bgepn,bige->bigep', reader_blk, before, jnp.exp(cum_log), precision=HIGHEST)
    result = (in_block + carried).reshape(length, head_count, head_width)
    return (result, last_state.reshape(head_count, head_width, state_width))

def context_state(signal, row_weights, writer):
    length, head_count, head_width = signal.shape
    group_count, state_width = (writer.shape[1], writer.shape[2])
    per_group = head_count // group_count
    grouped = signal.reshape(length, group_count, per_group, head_width)
    weights = row_weights.reshape(length, group_count, per_group)
    summed = jnp.einsum('tgn,tge,tgep->gepn', writer, weights, grouped, precision=HIGHEST)
    return summed.reshape(head_count, head_width, state_width)

def group_norm(gated, group_count, group_gain):
    length = gated.shape[0]
    grouped = gated.reshape(length, group_count, -1)
    normed = grouped * lax.rsqrt(lax.optimization_barrier(jnp.mean(grouped * grouped, axis=-1, keepdims=True)) + EPSILON)
    return (normed.reshape(length, -1) * group_gain).astype(jnp.bfloat16)

def reference(latent, context, condition, context_condition, shift_weight, scale_weight, gate_weight, norm_gain, out_gate_weight, signal_weight, writer_weight, reader_matrix, step_weight, signal_taps, writer_taps, reader_taps, step_bias, decay_log, decay_extra, group_gain, output_weight):
    cond_act = jax.nn.silu(jnp.stack([condition, context_condition]).astype(jnp.float32)).astype(jnp.bfloat16)
    shift_vec = jnp.dot(cond_act, shift_weight, preferred_element_type=jnp.float32)
    scale_vec = jnp.dot(cond_act, scale_weight, preferred_element_type=jnp.float32)
    gate_vec = jnp.dot(cond_act[:1], gate_weight, preferred_element_type=jnp.float32)[0]
    hidden = modulate(latent, norm_gain, shift_vec[0], scale_vec[0])
    ctx_hidden = modulate(context, norm_gain, shift_vec[1], scale_vec[1])
    conv_taps = jnp.concatenate([signal_taps, writer_taps, reader_taps], axis=1)
    decay_rates = -jnp.exp(decay_log)[:, None, :]
    ctx_raw, ctx_step_in = project_rows(ctx_hidden, signal_weight, writer_weight, reader_matrix, step_weight)
    ctx_conv = centred_conv(jnp.pad(ctx_raw, ((1, 1), (0, 0))), conv_taps, CTX)
    ctx_signal, ctx_writer, _ = split_mixed(ctx_conv, HEADS, HEAD_DIM, GROUPS, STATE)
    prefix_stride_length = jax.nn.softplus(ctx_step_in.astype(jnp.float32) + step_bias[:, None, :])
    ctx_decay = decay_rates * prefix_stride_length
    cum_log = jnp.cumsum(ctx_decay, axis=1)
    ctx_forward = context_state(ctx_signal, jnp.exp(cum_log[0, -1:] - cum_log[0]) * prefix_stride_length[0], ctx_writer)
    ctx_backward = context_state(ctx_signal, jnp.exp(cum_log[1] - ctx_decay[1]) * prefix_stride_length[1], ctx_writer)
    gate_in = jnp.dot(hidden, out_gate_weight, preferred_element_type=jnp.float32).astype(jnp.bfloat16)
    raw_cols, step_in = project_rows(hidden, signal_weight, writer_weight, reader_matrix, step_weight)
    conv_out = centred_conv(jnp.pad(raw_cols, ((1, 1), (0, 0))), conv_taps, TOKENS)
    signal, writer, reader = split_mixed(conv_out, HEADS, HEAD_DIM, GROUPS, STATE)
    step_size = jax.nn.softplus(step_in.astype(jnp.float32) + step_bias[:, None, :])
    log_decay = decay_rates * step_size + jnp.swapaxes(decay_extra, 1, 2)
    forward_out, _ = state_span(signal, step_size[0], log_decay[0], writer, reader, ctx_forward, BLOCK)
    backward_out, _ = state_span(jnp.flip(signal, 0), jnp.flip(step_size[1], 0), jnp.flip(log_decay[1], 0), jnp.flip(writer, 0), jnp.flip(reader, 0), ctx_backward, BLOCK)
    both = (forward_out + jnp.flip(backward_out, 0)).reshape(TOKENS, -1)
    gated = both * jax.nn.silu(gate_in.astype(jnp.float32))
    normed = group_norm(gated, GROUPS, group_gain)
    mix = jnp.dot(normed, output_weight, preferred_element_type=jnp.float32)
    return (latent.astype(jnp.float32) + gate_vec * mix).astype(jnp.bfloat16)
```

```python
import functools

import jax
import jax.numpy as jnp
from jax import lax
from jax.experimental import pallas as pl
from jax.experimental.pallas import tpu as pltpu
from jax.sharding import PartitionSpec as P

EPSILON = 1e-06
MESH = pl.DeviceIdType.MESH
F32 = jnp.float32
BF16 = jnp.bfloat16
LANES = 128
NT = (((1,), (1,)), ((), ()))
TN = (((0,), (0,)), ((), ()))


def silu(v):
    return v * (0.5 + 0.5 * jnp.tanh(0.5 * v))


def softplus(v):
    return jnp.maximum(v, 0.0) + jnp.log1p(jnp.exp(-jnp.abs(v)))


def dot(a, b):
    return jnp.dot(a, b, preferred_element_type=F32)


def dot_nt(a, b):
    return lax.dot_general(a, b, NT, preferred_element_type=F32)


def dot_tn(a, b):
    return lax.dot_general(a, b, TN, preferred_element_type=F32)


def remote(src, dst, send, recv, where):
    return pltpu.make_async_remote_copy(
        src_ref=src, dst_ref=dst, send_sem=send, recv_sem=recv, device_id=where, device_id_type=MESH
    )


def aligned(i, n):
    return pl.multiple_of(i * n, n)


def lane_iota(shape):
    return lax.broadcasted_iota(jnp.int32, shape, len(shape) - 1)


def row_iota(shape):
    return lax.broadcasted_iota(jnp.int32, shape, len(shape) - 2)


def expand(cols, first, pair):
    n = cols.shape[0]
    a = first + 2 * pair
    return jnp.where(lane_iota((n, LANES)) < LANES // 2, cols[:, a : a + 1], cols[:, a + 1 : a + 2])


def kernel(
    nz,
    nx,
    latent,
    context,
    shift_w,
    scale_w,
    gate_w,
    og_w,
    sg_w,
    wr_w,
    rd_w,
    out_w,
    cond,
    stepw,
    gain,
    taps,
    bias,
    dlog,
    extra,
    ggain,
    out,
    mw,
    lat,
    ctx,
    hid,
    wog,
    wsg,
    wrd,
    wout,
    pay,
    zrecv,
    msum,
    mods,
    ab,
    rinv,
    rinvc,
    craw,
    cedge,
    raw,
    edge,
    gbuf,
    steprow,
    sbf,
    wbf,
    rbf,
    ldrow,
    strow,
    xrows,
    xt,
    eexp,
    fst,
    fpre,
    bpre,
    bloc,
    stsend,
    strecv,
    ctsend,
    ctrecv,
    dsend,
    drecv,
    dm,
    ed,
    retsend,
    retrecv,
    ybuf,
    nall,
    lsem,
    zs,
    zr,
    ms,
    mr,
    es,
    er,
    ces,
    cer,
    fs,
    fr,
    cs,
    cr,
    ds,
    dr,
    rs,
    rr,
    lats,
    latr,
    gs,
    gr,
    gs2,
    gr2,
    ps,
    pr,
):
    half_rows, width = latent.shape
    span = 2 * half_rows
    nctx = context.shape[0]
    nb = span // LANES
    chan = og_w.shape[1]
    cols = shift_w.shape[1]
    hcols = cols // 2
    po = chan // nz
    nk = nx * 2
    z = lax.axis_index("sp")
    x = lax.axis_index("tp")
    c = lax.axis_index("dp")
    me = x * 2 + c
    up = lax.rem(z + 1, nz)
    down = lax.rem(z + nz - 1, nz)
    right = lax.rem(x + 1, nx)
    left = lax.rem(x + nx - 1, nx)
    own0 = pl.multiple_of(c * half_rows, half_rows)
    oth0 = pl.multiple_of((1 - c) * half_rows, half_rows)

    pairs = [
        (shift_w, mw.at[0]),
        (scale_w, mw.at[1]),
        (gate_w, mw.at[2]),
        (context, ctx),
        (latent, lat.at[pl.ds(own0, half_rows)]),
        (sg_w, wsg),
        (wr_w, wrd.at[:, 0:LANES]),
        (rd_w, wrd.at[:, LANES : 2 * LANES]),
        (og_w, wog),
        (out_w, wout),
    ]
    loads = [pltpu.make_async_copy(s, d, lsem.at[i]) for i, (s, d) in enumerate(pairs)]
    for load in loads:
        load.start()

    barrier = pltpu.get_barrier_semaphore()

    def greet_z(d, _):
        pl.semaphore_signal(barrier, inc=1, device_id={"sp": lax.rem(z + d, nz)}, device_id_type=MESH)
        return 0

    def greet_k(d, _):
        k = lax.rem(me + d, nk)
        pl.semaphore_signal(
            barrier, inc=1, device_id={"tp": k // 2, "dp": lax.rem(k, 2)}, device_id_type=MESH
        )
        return 0

    lax.fori_loop(1, nz, greet_z, 0)
    lax.fori_loop(1, nk, greet_k, 0)

    for i in range(3):
        loads[i].wait()
    zrows = shift_w.shape[0]
    v = cond[:, pl.ds(aligned(z, zrows), zrows)].astype(F32)
    act = silu(v).astype(BF16)
    y = dot(act, mw[0]) + pltpu.roll(dot(act, mw[1]), 2, 0) + pltpu.roll(dot(act, mw[2]), 4, 0)
    pay[...] = jnp.concatenate([y[:, :hcols], y[:, hcols:]], axis=0).astype(BF16)

    pl.semaphore_wait(barrier, nz - 1 + nk - 1)

    def zcast(d):
        return remote(pay, zrecv.at[z], zs.at[d], zr.at[z], {"sp": lax.rem(z + d, nz)})

    def zcast_start(d, _):
        zcast(d).start()
        return 0

    lax.fori_loop(1, nz, zcast_start, 0)
    lat_copy = remote(latent, lat.at[pl.ds(own0, half_rows)], lats, latr, {"dp": 1 - c})
    lat_copy.start()

    def rms_rows(src, base, dst):
        acc = jnp.zeros((16, LANES), F32)
        for j in range(width // 256):
            xx = src[pl.ds(base, 16), j * 256 : (j + 1) * 256].astype(F32)
            sq = xx * xx
            acc = acc + sq[:, :LANES] + sq[:, LANES:]
        s = jnp.sum(acc, axis=1, keepdims=True)
        dst[pl.ds(base, 16), :] = jnp.broadcast_to(lax.rsqrt(s / width + EPSILON), (16, LANES))

    loads[3].wait()

    def rms_ctx(i, _):
        rms_rows(ctx, aligned(i, 16), rinvc)
        return 0

    lax.fori_loop(0, nctx // 16, rms_ctx, 0)
    loads[4].wait()

    def rms_own(i, _):
        rms_rows(lat, pl.multiple_of(own0 + i * 16, 16), rinv)
        return 0

    lax.fori_loop(0, half_rows // 16, rms_own, 0)
    remote(latent, lat.at[pl.ds(oth0, half_rows)], lats, latr, {"dp": 1 - c}).wait_recv()

    def rms_oth(i, _):
        rms_rows(lat, pl.multiple_of(oth0 + i * 16, 16), rinv)
        return 0

    lax.fori_loop(0, half_rows // 16, rms_oth, 0)

    def add_z(d, acc):
        src = lax.rem(z + nz - d, nz)
        remote(pay, zrecv.at[src], zs.at[d], zr.at[src], {"sp": src}).wait_recv()
        return acc + zrecv[src].astype(F32)

    total = lax.fori_loop(1, nz, add_z, pay[...].astype(F32))
    msum[...] = total
    mods[me] = total

    def mcast(d):
        k = lax.rem(me + d, nk)
        return remote(msum, mods.at[me], ms.at[d], mr.at[me], {"tp": k // 2, "dp": lax.rem(k, 2)})

    def mcast_start(d, _):
        mcast(d).start()
        return 0

    lax.fori_loop(1, nk, mcast_start, 0)

    def mcast_take(d, _):
        k = lax.rem(me + nk - d, nk)
        remote(msum, mods.at[k], ms.at[d], mr.at[k], {"tp": k // 2, "dp": lax.rem(k, 2)}).wait_recv()
        return 0

    lax.fori_loop(1, nk, mcast_take, 0)
    for k in range(nk):
        for h in range(2):
            m = mods[k, h * 8 : h * 8 + 8, :]
            at = slice(k * cols + h * hcols, k * cols + (h + 1) * hcols)
            g = gain[:, at]
            ab[0:1, at] = g * (1.0 + m[2:3])
            ab[1:2, at] = m[0:1]
            ab[2:3, at] = g * (1.0 + m[3:4])
            ab[3:4, at] = m[1:2]

    def modulate(src, base, scale_ref, row, dst_base, rows):
        for i in range(rows // 16):
            r = scale_ref[pl.ds(pl.multiple_of(base + i * 16, 16), 16), :]
            for j in range(width // LANES):
                at = slice(j * LANES, (j + 1) * LANES)
                xx = src[pl.ds(pl.multiple_of(base + i * 16, 16), 16), at].astype(F32)
                val = (xx * r) * ab[row : row + 1, at] + ab[row + 1 : row + 2, at]
                hid[pl.ds(pl.multiple_of(dst_base + i * 16, 16), 16), at] = val.astype(BF16)

    def mod_ctx(i, _):
        modulate(ctx, aligned(i, 16), rinvc, 2, pl.multiple_of(span + i * 16, 16), 16)
        return 0

    lax.fori_loop(0, nctx // 16, mod_ctx, 0)

    for i in range(5, 8):
        loads[i].wait()
    hc = hid[span : span + nctx, :]
    craw[8 : 8 + nctx, 0:chan] = dot(hc, wsg[...])
    craw[8 : 8 + nctx, chan : chan + 2 * LANES] = dot(hc, wrd[...])
    cstep = dot_nt(stepw[...], hid[span : span + LANES, :])
    cedge_up = remote(craw.at[nctx : nctx + 8], cedge.at[0], ces.at[0], cer.at[0], {"sp": up})
    cedge_down = remote(craw.at[8:16], cedge.at[1], ces.at[1], cer.at[1], {"sp": down})
    cedge_up.start()
    cedge_down.start()
    loads[8].wait()

    tile = min(256, span)

    def project(row0):
        def mod_lat(i, _):
            at = pl.multiple_of(row0 + i * 32, 32)
            modulate(lat, at, rinv, 0, at, 32)
            return 0

        lax.fori_loop(0, tile // 32, mod_lat, 0)
        h = hid.at[pl.ds(row0, tile)]
        to = pl.multiple_of(row0 + 8, 8)
        raw[pl.ds(to, tile), 0:chan] = dot(h[...], wsg[...])
        raw[pl.ds(to, tile), chan : chan + 2 * LANES] = dot(h[...], wrd[...])
        gbuf[pl.ds(row0, tile), :] = silu(dot(h[...], wog[...]))
        s = dot_nt(stepw[...], h[...])
        for i in range(tile // LANES):
            steprow[row0 // LANES + i] = s[:, i * LANES : (i + 1) * LANES]

    ntiles = span // tile

    def project_ends(i, _):
        project(aligned(i * (ntiles - 1), tile))
        return 0

    lax.fori_loop(0, min(2, ntiles), project_ends, 0)
    edge_up = remote(raw.at[span : span + 8], edge.at[0], es.at[0], er.at[0], {"sp": up})
    edge_down = remote(raw.at[8:16], edge.at[1], es.at[1], er.at[1], {"sp": down})
    edge_up.start()
    edge_down.start()

    def conv(block, at):
        n = block.shape[0]
        mix = (
            taps[0:1, at] * pltpu.roll(block, 1, 0)
            + taps[1:2, at] * block
            + taps[2:3, at] * pltpu.roll(block, n - 1, 0)
        )
        return silu(mix[8 : n - 8])

    first = (z == 0).astype(F32)
    last = (z == nz - 1).astype(F32)
    cedge_up.wait_recv()
    cedge_down.wait_recv()
    craw[7:8, :] = cedge[0, 7:8, :] * (1.0 - first)
    craw[8 + nctx : 9 + nctx, :] = cedge[1, 0:1, :] * (1.0 - last)
    is_fwd = row_iota((8, LANES)) < 4
    lane8 = lane_iota((8, LANES))
    rate = -jnp.exp(dlog[...])
    tri = (
        lax.broadcasted_iota(jnp.int32, (LANES, LANES), 0)
        <= lax.broadcasted_iota(jnp.int32, (LANES, LANES), 1)
    ).astype(F32)

    def cumulate(a):
        return jnp.dot(a, tri, precision=lax.Precision.HIGHEST, preferred_element_type=F32)

    cst = softplus(cstep.astype(BF16).astype(F32) + bias[...])
    cst = jnp.where(lane8 < nctx, cst, 0.0)
    cld = rate * cst
    ccum = cumulate(cld)
    cend = ccum[:, LANES - 1 : LANES]
    cw = jnp.where(is_fwd, jnp.exp(cend - ccum), jnp.exp(ccum - cld)) * cst
    xrows[0, 0:8, :] = cw
    cwt = jnp.transpose(xrows[0:4].reshape(LANES, LANES))[0:nctx, :]
    cblock = [
        conv(craw[0 : nctx + 16, j * LANES : (j + 1) * LANES], slice(j * LANES, (j + 1) * LANES))
        for j in range(chan // LANES + 1)
    ]
    cwr = cblock[-1].astype(BF16)
    for k in range(2):
        for p in range(chan // LANES):
            sc = (cblock[p] * expand(cwt, 4 * k, p)).astype(BF16)
            st = dot_tn(sc, cwr).astype(BF16)
            per = LANES // po
            ctsend[p * per : (p + 1) * per, k] = st.reshape(per, po, LANES)

    def ctcast(d):
        t = lax.rem(z + d, nz)
        return remote(ctsend.at[t], ctrecv.at[z], cs.at[d], cr.at[z], {"sp": t})

    def ctcast_start(d, _):
        ctcast(d).start()
        return 0

    lax.fori_loop(1, nz, ctcast_start, 0)
    ctrecv[z] = ctsend[z]

    def project_rest(i, _):
        project(aligned(i, tile))
        return 0

    lax.fori_loop(1, ntiles - 1, project_rest, 0)

    edge_up.wait_recv()
    edge_down.wait_recv()
    raw[7:8, :] = edge[0, 7:8, :] * (1.0 - first)
    raw[8 + span : 9 + span, :] = edge[1, 0:1, :] * (1.0 - last)

    def conv_block(b, _):
        base = aligned(b, LANES)
        for j in range(chan // LANES + 2):
            at = slice(j * LANES, (j + 1) * LANES)
            val = conv(raw[pl.ds(base, LANES + 16), at], at).astype(BF16)
            if j < chan // LANES:
                sbf[pl.ds(base, LANES), at] = val
            elif j == chan // LANES:
                wbf[pl.ds(base, LANES), :] = val
            else:
                rbf[pl.ds(base, LANES), :] = val
        return 0

    lax.fori_loop(0, nb, conv_block, 0)

    for b in range(nb):
        st = softplus(steprow[b].astype(BF16).astype(F32) + bias[...])
        strow[b] = st
        ldrow[b] = rate * st + extra[:, b * LANES : (b + 1) * LANES]
    cum = cumulate(ldrow[...].reshape(nb * 8, LANES))
    ends = [cum[b * 8 : b * 8 + 8, LANES - 1 : LANES] for b in range(nb)]
    zero = jnp.zeros((8, 1), F32)
    before = [zero]
    for b in range(nb):
        before.append(before[-1] + ends[b])
    after = [zero]
    for b in reversed(range(nb)):
        after.append(after[-1] + ends[b])
    after = after[::-1]
    isf1 = row_iota((8, 1)) < 4
    for b in range(nb):
        cb = cum[b * 8 : b * 8 + 8]
        e = cb - ldrow[b]
        end = ends[b]
        near = jnp.where(is_fwd, cb, end - e)
        xrows[b, 0:8, :] = jnp.where(is_fwd, cb, e)
        xrows[b, 8:16, :] = jnp.where(is_fwd, jnp.exp(end - cb), jnp.exp(e)) * strow[b]
        xrows[b, 16:24, :] = jnp.exp(near)
        xrows[b, 24:32, :] = jnp.exp(near + jnp.where(isf1, before[b], after[b + 1]))
        eexp[b] = jnp.broadcast_to(jnp.exp(end), (8, LANES))
    for g in range(-(-nb // 4)):
        turned = jnp.transpose(xrows[g * 4 : g * 4 + 4].reshape(LANES, LANES))
        for b in range(g * 4, min(nb, g * 4 + 4)):
            xt[b] = turned[:, (b - g * 4) * 32 : (b - g * 4 + 1) * 32]

    npair = chan // LANES
    fst[...] = jnp.zeros_like(fst)

    def decayed(state, b, row):
        lo = eexp[b, row : row + 1, :]
        hi = eexp[b, row + 1 : row + 2, :]
        return jnp.where(row_iota((LANES, LANES)) < LANES // 2, lo, hi) * state

    def forward(b, _):
        base = aligned(b, LANES)
        w = wbf[pl.ds(base, LANES), :]
        cl = xt[b]
        for p in range(npair):
            at = slice(p * LANES, (p + 1) * LANES)
            s = sbf[pl.ds(base, LANES), at].astype(F32)
            fpre[b, at, :] = fst[at, :].astype(BF16)
            fst[at, :] = decayed(fst[at, :], b, 2 * p) + dot_tn((s * expand(cl, 8, p)).astype(BF16), w)
            bloc[b, at, :] = dot_tn((s * expand(cl, 12, p)).astype(BF16), w)
        return 0

    lax.fori_loop(0, nb, forward, 0)
    stsend[:, 0] = fst[...].astype(BF16).reshape(nz, po, LANES)
    fst[...] = jnp.zeros_like(fst)

    def backward(i, _):
        b = nb - 1 - i
        for p in range(npair):
            at = slice(p * LANES, (p + 1) * LANES)
            bpre[b, at, :] = fst[at, :].astype(BF16)
            fst[at, :] = decayed(fst[at, :], b, 4 + 2 * p) + bloc[b, at, :]
        return 0

    lax.fori_loop(0, nb, backward, 0)
    stsend[:, 1] = fst[...].astype(BF16).reshape(nz, po, LANES)
    sub8 = row_iota((8, LANES))
    dsend[...] = jnp.sum(
        jnp.where(lane8 == sub8, before[nb], 0.0) + jnp.where(lane8 == sub8 + 8, cend, 0.0),
        axis=0,
        keepdims=True,
    )

    def stcast(d):
        t = lax.rem(z + d, nz)
        return remote(stsend.at[t], strecv.at[z], fs.at[d], fr.at[z], {"sp": t})

    def dcast(d):
        return remote(dsend, drecv.at[z], ds.at[d], dr.at[z], {"sp": lax.rem(z + d, nz)})

    def stcast_start(d, _):
        dcast(d).start()
        stcast(d).start()
        return 0

    lax.fori_loop(1, nz, stcast_start, 0)
    strecv[z] = stsend[z]
    drecv[z] = dsend[...]

    lower = lax.broadcasted_iota(jnp.int32, (LANES, LANES), 1) <= lax.broadcasted_iota(
        jnp.int32, (LANES, LANES), 0
    )
    upper = lax.broadcasted_iota(jnp.int32, (LANES, LANES), 1) >= lax.broadcasted_iota(
        jnp.int32, (LANES, LANES), 0
    )

    def inside(b, _):
        base = aligned(b, LANES)
        r = rbf[pl.ds(base, LANES), :]
        g = dot_nt(r, wbf[pl.ds(base, LANES), :])
        cl = xt[b]
        for p in range(npair):
            at = slice(p * LANES, (p + 1) * LANES)
            s = sbf[pl.ds(base, LANES), at]
            own = []
            for h in (2 * p, 2 * p + 1):
                arg = jnp.where(
                    lower,
                    cl[:, h : h + 1] - xrows[b, h : h + 1, :],
                    xrows[b, 4 + h : 5 + h, :] - cl[:, 4 + h : 5 + h],
                )
                wgt = jnp.where(lower, strow[b, h : h + 1, :], 0.0) + jnp.where(
                    upper, strow[b, 4 + h : 5 + h, :], 0.0
                )
                own.append(dot((g * jnp.exp(arg) * wgt).astype(BF16), s))
            carried = expand(cl, 16, p) * dot_nt(r, fpre[b, at, :]) + expand(cl, 20, p) * dot_nt(
                r, bpre[b, at, :]
            )
            ybuf[pl.ds(base, LANES), at] = carried + jnp.where(
                lane_iota((LANES, LANES)) < LANES // 2, own[0], own[1]
            )
        return 0

    lax.fori_loop(0, nb, inside, 0)

    def take_states(d, _):
        src = lax.rem(z + nz - d, nz)
        remote(dsend, drecv.at[src], ds.at[d], dr.at[src], {"sp": src}).wait_recv()
        remote(ctsend.at[src], ctrecv.at[src], cs.at[d], cr.at[src], {"sp": src}).wait_recv()
        remote(stsend.at[src], strecv.at[src], fs.at[d], fr.at[src], {"sp": src}).wait_recv()
        return 0

    lax.fori_loop(1, nz, take_states, 0)
    for k in range(nz):
        dm[k : k + 1, :] = drecv[k]
    head = z * po // (LANES // 2)
    dall = dm[...]
    lane_z = lane_iota((nz, LANES))
    for i in range(4):
        col = jnp.sum(jnp.where(lane_z == 4 * i + head, dall, 0.0), axis=1, keepdims=True)
        ed[i] = jnp.exp(jnp.broadcast_to(col, (nz, LANES)))
    state = jnp.zeros((po, LANES), F32)
    for k in range(nz):
        state = ed[2, k : k + 1, :] * state + ctrecv[k, 0].astype(F32)
    for k in range(nz):
        retsend[k, 0] = state.astype(BF16)
        state = ed[0, k : k + 1, :] * state + strecv[k, 0].astype(F32)
    state = jnp.zeros((po, LANES), F32)
    for k in reversed(range(nz)):
        state = ed[3, k : k + 1, :] * state + ctrecv[k, 1].astype(F32)
    for k in reversed(range(nz)):
        retsend[k, 1] = state.astype(BF16)
        state = ed[1, k : k + 1, :] * state + strecv[k, 1].astype(F32)

    def retcast(d):
        t = lax.rem(z + d, nz)
        return remote(retsend.at[t], retrecv.at[z], rs.at[d], rr.at[z], {"sp": t})

    def retcast_start(d, _):
        retcast(d).start()
        return 0

    lax.fori_loop(1, nz, retcast_start, 0)
    retrecv[z] = retsend[z]

    def take_return(d, _):
        src = lax.rem(z + nz - d, nz)
        remote(retsend.at[src], retrecv.at[src], rs.at[d], rr.at[src], {"sp": src}).wait_recv()
        return 0

    lax.fori_loop(1, nz, take_return, 0)

    hrow = LANES // 2

    def piece(k, b):
        return nall.at[k, pl.ds(aligned(b, LANES), LANES)]

    def part(k, b, h):
        return nall.at[k, pl.ds(pl.multiple_of(b * LANES + h * hrow, hrow), hrow)]

    def to_partner(k, i, b):
        return remote(piece(k, b), piece(k, b), ps.at[i, b], pr.at[i, b], {"dp": 1 - c})

    k_left = left * 2 + c
    k_right = right * 2 + c
    k_far = lax.rem(x + 2, nx) * 2 + c

    def own_right(b):
        return remote(piece(me, b), piece(me, b), gs.at[0, b], gr.at[0, b], {"tp": right})

    def own_left(b):
        return remote(piece(me, b), piece(me, b), gs.at[1, b], gr.at[1, b], {"tp": left})

    def relay_right(b):
        return remote(part(k_left, b, 0), part(k_left, b, 0), gs2.at[0, b], gr2.at[0, b], {"tp": right})

    def relay_left(b):
        return remote(part(k_right, b, 1), part(k_right, b, 1), gs2.at[1, b], gr2.at[1, b], {"tp": left})

    def finish(b, _):
        base = aligned(b, LANES)
        r = rbf[pl.ds(base, LANES), :]
        cl = xt[b]
        vals = []
        for p in range(npair):
            at = slice(p * LANES, (p + 1) * LANES)
            per = LANES // po
            f_in = retrecv[p * per : (p + 1) * per, 0].reshape(LANES, LANES)
            b_in = retrecv[p * per : (p + 1) * per, 1].reshape(LANES, LANES)
            yy = (
                ybuf[pl.ds(base, LANES), at]
                + expand(cl, 24, p) * dot_nt(r, f_in)
                + expand(cl, 28, p) * dot_nt(r, b_in)
            )
            vals.append(yy * gbuf[pl.ds(base, LANES), at])
        sq = sum(jnp.sum(a * a, axis=1, keepdims=True) for a in vals)
        inv = lax.rsqrt(sq / chan + EPSILON)
        for p in range(npair):
            at = slice(p * LANES, (p + 1) * LANES)
            nall[me, pl.ds(base, LANES), at] = (vals[p] * inv * ggain[:, at]).astype(BF16)
        own_right(b).start()
        own_left(b).start()
        to_partner(me, 0, b).start()
        return 0

    lax.fori_loop(0, nb, finish, 0)
    loads[9].wait()
    gate = jnp.concatenate([msum[4:5, :], msum[12:13, :]], axis=1)
    out0 = pl.multiple_of(me * cols, cols)

    def collect(i, _):
        @pl.when(i < nb)
        def _():
            remote(piece(k_left, i), piece(k_left, i), gs.at[0, i], gr.at[0, i], {"tp": left}).wait_recv()
            relay_right(i).start()
            to_partner(k_left, 1, i).start()
            remote(piece(k_right, i), piece(k_right, i), gs.at[1, i], gr.at[1, i], {"tp": right}).wait_recv()
            relay_left(i).start()
            to_partner(k_right, 2, i).start()

        @pl.when(jnp.logical_and(i >= 1, i <= nb))
        def _():
            b = i - 1
            for h in range(2):
                remote(part(k_far, b, h), part(k_far, b, h), gs2.at[h, b], gr2.at[h, b], {"tp": left}).wait_recv()
            to_partner(k_far, 3, b).start()

        @pl.when(i >= 2)
        def _():
            b = i - 2
            flip = 1 - 2 * c
            for n, k in enumerate((me, k_left, k_right, k_far)):
                to_partner(k + flip, n, b).wait_recv()
            base = aligned(b, LANES)
            acc = jnp.zeros((LANES, cols), F32)
            for k in range(nk):
                acc = acc + dot(nall[k, pl.ds(base, LANES), :], wout[k * chan : (k + 1) * chan, :])
            res = lat[pl.ds(base, LANES), pl.ds(out0, cols)].astype(F32)
            out[pl.ds(base, LANES), :] = (res + gate * acc).astype(BF16)

        return 0

    lax.fori_loop(0, nb + 2, collect, 0)

    lat_copy.wait_send()
    cedge_up.wait_send()
    cedge_down.wait_send()
    edge_up.wait_send()
    edge_down.wait_send()

    def drain_z(d, _):
        zcast(d).wait_send()
        ctcast(d).wait_send()
        stcast(d).wait_send()
        dcast(d).wait_send()
        retcast(d).wait_send()
        return 0

    lax.fori_loop(1, nz, drain_z, 0)

    def drain_k(d, _):
        mcast(d).wait_send()
        return 0

    lax.fori_loop(1, nk, drain_k, 0)

    def drain_b(b, _):
        own_right(b).wait_send()
        own_left(b).wait_send()
        relay_right(b).wait_send()
        relay_left(b).wait_send()
        for i in range(4):
            to_partner(me, i, b).wait_send()
        return 0

    lax.fori_loop(0, nb, drain_b, 0)


def on_device(
    latent,
    context,
    condition,
    context_condition,
    shift_weight,
    scale_weight,
    gate_weight,
    norm_gain,
    out_gate_weight,
    signal_weight,
    writer_weight,
    reader_matrix,
    step_weight,
    signal_taps,
    writer_taps,
    reader_taps,
    step_bias,
    decay_log,
    decay_extra,
    group_gain,
    output_weight,
):
    nz, nx = lax.axis_size("sp"), lax.axis_size("tp")
    half_rows, width = latent.shape
    span, nctx = 2 * half_rows, context.shape[0]
    chan, cols = out_gate_weight.shape[1], shift_weight.shape[1]
    nb, nk, po = span // LANES, 2 * nx, chan // nz
    full = chan + 2 * LANES
    rows8 = 2 * step_bias.shape[1]
    cond = jnp.concatenate(
        [condition[None], context_condition[None], jnp.zeros((6, width), BF16)], axis=0
    )
    stepw = jnp.transpose(step_weight, (0, 2, 1)).reshape(rows8, width)
    taps = jnp.concatenate([signal_taps, writer_taps, reader_taps], axis=1)
    hbm = pl.BlockSpec(memory_space=pl.ANY)
    vmem = pl.BlockSpec(memory_space=pltpu.VMEM)
    dma = pltpu.SemaphoreType.DMA
    scratch = [
        ((3, *shift_weight.shape), BF16),
        ((span, width), BF16),
        ((nctx, width), BF16),
        ((span + LANES, width), BF16),
        ((width, chan), BF16),
        ((width, chan), BF16),
        ((width, 2 * LANES), BF16),
        (output_weight.shape, BF16),
        ((16, cols // 2), BF16),
        ((nz, 16, cols // 2), BF16),
        ((16, cols // 2), F32),
        ((nk, 16, cols // 2), F32),
        ((8, width), F32),
        ((span, LANES), F32),
        ((nctx, LANES), F32),
        ((nctx + 16, full), F32),
        ((2, 8, full), F32),
        ((span + 16, full), F32),
        ((2, 8, full), F32),
        ((span, chan), F32),
        ((nb, 8, LANES), F32),
        ((span, chan), BF16),
        ((span, LANES), BF16),
        ((span, LANES), BF16),
        ((nb, 8, LANES), F32),
        ((nb, 8, LANES), F32),
        ((-(-nb // 4) * 4, 32, LANES), F32),
        ((nb, LANES, 32), F32),
        ((nb, 8, LANES), F32),
        ((chan, LANES), F32),
        ((nb, chan, LANES), BF16),
        ((nb, chan, LANES), BF16),
        ((nb, chan, LANES), F32),
        ((nz, 2, po, LANES), BF16),
        ((nz, 2, po, LANES), BF16),
        ((nz, 2, po, LANES), BF16),
        ((nz, 2, po, LANES), BF16),
        ((1, LANES), F32),
        ((nz, 1, LANES), F32),
        ((nz, LANES), F32),
        ((4, nz, LANES), F32),
        ((nz, 2, po, LANES), BF16),
        ((nz, 2, po, LANES), BF16),
        ((span, chan), F32),
        ((nk, span, chan), BF16),
    ]
    sems = [
        (10,),
        (nz,),
        (nz,),
        (nk,),
        (nk,),
        (2,),
        (2,),
        (2,),
        (2,),
        (nz,),
        (nz,),
        (nz,),
        (nz,),
        (nz,),
        (nz,),
        (nz,),
        (nz,),
        None,
        None,
        (2, nb),
        (2, nb),
        (2, nb),
        (2, nb),
        (4, nb),
        (4, nb),
    ]
    return pl.pallas_call(
        functools.partial(kernel, nz, nx),
        out_shape=jax.ShapeDtypeStruct((span, cols), BF16),
        in_specs=[hbm] * 10 + [vmem] * 8,
        out_specs=vmem,
        scratch_shapes=[pltpu.VMEM(s, t) for s, t in scratch]
        + [dma if s is None else dma(s) for s in sems],
        compiler_params=pltpu.CompilerParams(
            collective_id=0, has_side_effects=True, vmem_limit_bytes=60 * 1024 * 1024
        ),
        name="mixing",
    )(
        latent,
        context,
        shift_weight,
        scale_weight,
        gate_weight,
        out_gate_weight,
        signal_weight,
        writer_weight,
        reader_matrix,
        output_weight,
        cond,
        stepw,
        norm_gain.reshape(1, width),
        taps,
        step_bias.reshape(rows8, 1),
        decay_log.reshape(rows8, 1),
        decay_extra.reshape(rows8, span),
        group_gain.reshape(1, chan),
    )


def solution(mesh):
    in_specs = (
        P(("grp", "sp", "dp"), None),
        P(("grp", "sp"), None),
        P("grp"),
        P(),
        P("sp", ("tp", "dp")),
        P("sp", ("tp", "dp")),
        P("sp", ("tp", "dp")),
        P(),
        P(None, ("tp", "dp")),
        P(None, ("tp", "dp")),
        P(None, ("tp", "dp")),
        P(None, ("tp", "dp")),
        P(None, None, ("tp", "dp")),
        P(None, ("tp", "dp")),
        P(None, ("tp", "dp")),
        P(None, ("tp", "dp")),
        P(None, ("tp", "dp")),
        P(None, ("tp", "dp")),
        P(None, ("tp", "dp"), ("grp", "sp")),
        P(("tp", "dp")),
        P(None, ("tp", "dp")),
    )
    out_specs = P(("grp", "sp"), ("tp", "dp"))
    return jax.shard_map(
        on_device, mesh=mesh, in_specs=in_specs, out_specs=out_specs, check_vma=False
    )
```

```python
import functools

import jax
import jax.numpy as jnp
from jax import lax
from jax.experimental import pallas as pl
from jax.experimental.pallas import tpu as pltpu
from jax.sharding import PartitionSpec as P

EPSILON = 1e-06
OVERLAP = True
MESH = pl.DeviceIdType.MESH
F32 = jnp.float32
BF16 = jnp.bfloat16
LANES = 128
NT = (((1,), (1,)), ((), ()))
TN = (((0,), (0,)), ((), ()))


def silu(v):
    return v * (0.5 + 0.5 * jnp.tanh(0.5 * v))


def softplus(v):
    return jnp.maximum(v, 0.0) + jnp.log1p(jnp.exp(-jnp.abs(v)))


def dot(a, b):
    return jnp.dot(a, b, preferred_element_type=F32)


def dot_nt(a, b):
    return lax.dot_general(a, b, NT, preferred_element_type=F32)


def dot_tn(a, b):
    return lax.dot_general(a, b, TN, preferred_element_type=F32)


def remote(src, dst, send, recv, where):
    return pltpu.make_async_remote_copy(
        src_ref=src, dst_ref=dst, send_sem=send, recv_sem=recv, device_id=where, device_id_type=MESH
    )


def aligned(i, n):
    return pl.multiple_of(i * n, n)


def lane_iota(shape):
    return lax.broadcasted_iota(jnp.int32, shape, len(shape) - 1)


def row_iota(shape):
    return lax.broadcasted_iota(jnp.int32, shape, len(shape) - 2)


def expand(cols, first, pair):
    n = cols.shape[0]
    a = first + 2 * pair
    return jnp.where(lane_iota((n, LANES)) < LANES // 2, cols[:, a : a + 1], cols[:, a + 1 : a + 2])


def kernel(
    nz,
    nx,
    latent,
    context,
    shift_w,
    scale_w,
    gate_w,
    og_w,
    sg_w,
    wr_w,
    rd_w,
    out_w,
    cond,
    ctx_cond,
    stepw_in,
    gain,
    signal_taps,
    writer_taps,
    reader_taps,
    bias_in,
    dlog_in,
    extra,
    ggain,
    out,
    condrow,
    taps,
    mw,
    lat,
    ctx,
    hid0,
    hid1,
    hid2,
    acc,
    wog,
    wsg,
    wsw,
    wrd,
    wout,
    pay,
    zrecv,
    gpay,
    grecv,
    msum,
    mods,
    ab,
    rinv,
    rinvc,
    craw,
    cedge,
    cstepc,
    raw,
    edge,
    rraw,
    redge,
    rsend,
    gbuf,
    stepc,
    sbf,
    wbf,
    rbf,
    ldrow,
    strow,
    xrows,
    xt,
    eexp,
    loc,
    fpre,
    bpre,
    fsend,
    frecv,
    bsend,
    brecv,
    ctsend,
    ctrecv,
    dsend,
    drecv,
    dm,
    ed,
    fback,
    fin,
    bback,
    bin_,
    ybuf,
    nall,
    oacc,
    obuf,
    lsem,
    zs,
    zr,
    ms,
    mr,
    es,
    er,
    res,
    rer,
    ces,
    cer,
    gzs,
    gzr,
    fs,
    fr,
    bs,
    br,
    cs,
    cr,
    ds,
    dr,
    rs,
    rr,
    rbs,
    rbr,
    lats,
    latr,
    gs,
    gr,
    gs2,
    gr2,
    ps,
    pr,
    osem,
):
    scopes = []

    def phase(name):
        if scopes:
            scopes.pop().__exit__(None, None, None)
        if name:
            scopes.append(jax.named_scope(name))
            scopes[-1].__enter__()

    phase("p_start")
    half_rows, width = latent.shape
    span = 2 * half_rows
    nctx = context.shape[0]
    nb = span // LANES
    chan = og_w.shape[1]
    cols = shift_w.shape[1]
    po = chan // nz
    nk = nx * 2
    z = lax.axis_index("sp")
    x = lax.axis_index("tp")
    c = lax.axis_index("dp")
    me = x * 2 + c
    up = lax.rem(z + 1, nz)
    down = lax.rem(z + nz - 1, nz)
    right = lax.rem(x + 1, nx)
    left = lax.rem(x + nx - 1, nx)
    own0 = pl.multiple_of(c * half_rows, half_rows)
    oth0 = pl.multiple_of((1 - c) * half_rows, half_rows)

    pairs = [
        (shift_w, mw.at[0]),
        (scale_w, mw.at[1]),
        (gate_w, mw.at[2]),
        (context, ctx),
        (latent, lat.at[pl.ds(own0, half_rows)]),
        (sg_w, wsg),
        (wr_w, wsw.at[:, 0:LANES]),
        (rd_w, wrd),
        (og_w, wog),
        (out_w, wout),
    ]
    loads = [pltpu.make_async_copy(s, d, lsem.at[i]) for i, (s, d) in enumerate(pairs)]
    for load in loads:
        load.start()

    barrier = pltpu.get_barrier_semaphore()

    def greet_z(d, _):
        pl.semaphore_signal(barrier, inc=1, device_id={"sp": lax.rem(z + d, nz)}, device_id_type=MESH)
        return 0

    def greet_k(d, _):
        k = lax.rem(me + d, nk)
        pl.semaphore_signal(
            barrier, inc=1, device_id={"tp": k // 2, "dp": lax.rem(k, 2)}, device_id_type=MESH
        )
        return 0

    lax.fori_loop(1, nz, greet_z, 0)
    lax.fori_loop(1, nk, greet_k, 0)

    phase("p_matvec")
    zrows = shift_w.shape[0]
    condrow[...] = jnp.zeros_like(condrow)
    condrow[0:1, :] = cond[...].astype(F32).reshape(1, width)
    condrow[1:2, :] = ctx_cond[...].astype(F32).reshape(1, width)
    act = silu(condrow[:, pl.ds(aligned(z, zrows), zrows)]).astype(BF16)
    for i in range(3):
        loads[i].wait()
    y = dot(act, mw[0]) + pltpu.roll(dot(act, mw[1]), 2, 0)
    pay[...] = jnp.concatenate(
        [y[0:4, j * LANES : (j + 1) * LANES] for j in range(cols // LANES)], axis=0
    ).astype(BF16)
    gpay[...] = dot(act, mw[2])[0:1, :]

    phase("p_barrier")
    pl.semaphore_wait(barrier, nz - 1 + nk - 1)
    phase("p_zcast")

    def zcast(d):
        return remote(pay, zrecv.at[z], zs.at[d], zr.at[z], {"sp": lax.rem(z + d, nz)})

    def zcast_start(d, _):
        zcast(d).start()
        return 0

    lax.fori_loop(1, nz, zcast_start, 0)
    lat_copy = remote(latent, lat.at[pl.ds(own0, half_rows)], lats, latr, {"dp": 1 - c})
    lat_copy.start()

    taps[:, 0:chan] = signal_taps[...]
    taps[:, chan : chan + LANES] = writer_taps[...]
    taps[:, chan + LANES : chan + 2 * LANES] = reader_taps[...]
    sub4 = lax.broadcasted_iota(jnp.int32, (8, 4), 0)
    pick4 = lax.broadcasted_iota(jnp.int32, (8, 4), 1) == lax.rem(sub4, 4)

    def column(ref):
        both = jnp.where(sub4 < 4, ref[0:1, :], ref[1:2, :])
        return jnp.sum(jnp.where(pick4, both, 0.0), axis=1, keepdims=True)

    bias = column(bias_in)
    rate = -jnp.exp(column(dlog_in))

    def step_cols(i, _):
        at = pl.ds(aligned(i, LANES), LANES)
        rows = [
            stepw_in[0, :, at].astype(F32),
            stepw_in[1, :, at].astype(F32),
            jnp.zeros((LANES - 8, LANES), F32),
        ]
        wsw[at, LANES : 2 * LANES] = jnp.transpose(jnp.concatenate(rows, axis=0)).astype(BF16)

    def step_cols4(i, _):
        for n in range(4):
            step_cols(i * 4 + n, 0)
        return 0

    lax.fori_loop(0, width // LANES // 4, step_cols4, 0)

    def rms_rows(src, base, rows, dst):
        at = pl.ds(base, rows)
        sums = jnp.zeros((rows, LANES), F32)
        for j in range(width // LANES):
            xx = src[at, j * LANES : (j + 1) * LANES].astype(F32)
            sums = sums + xx * xx
        total = jnp.sum(sums, axis=1, keepdims=True)
        dst[at, :] = jnp.broadcast_to(lax.rsqrt(total / width + EPSILON), (rows, LANES))

    loads[3].wait()
    rms_rows(ctx, 0, nctx, rinvc)
    loads[4].wait()
    rblock = 64

    def rms_own(i, _):
        rms_rows(lat, pl.multiple_of(own0 + i * rblock, rblock), rblock, rinv)
        return 0

    lax.fori_loop(0, half_rows // rblock, rms_own, 0)
    remote(latent, lat.at[pl.ds(oth0, half_rows)], lats, latr, {"dp": 1 - c}).wait_recv()

    def rms_oth(i, _):
        rms_rows(lat, pl.multiple_of(oth0 + i * rblock, rblock), rblock, rinv)
        return 0

    lax.fori_loop(0, half_rows // rblock, rms_oth, 0)

    phase("p_zwait")
    def add_z(d, acc):
        src = lax.rem(z + nz - d, nz)
        remote(pay, zrecv.at[src], zs.at[d], zr.at[src], {"sp": src}).wait_recv()
        return acc + zrecv[src].astype(F32)

    total = lax.fori_loop(1, nz, add_z, pay[...].astype(F32))
    msum[...] = total
    mods[me] = total

    def mcast(d):
        k = lax.rem(me + d, nk)
        return remote(msum, mods.at[me], ms.at[d], mr.at[me], {"tp": k // 2, "dp": lax.rem(k, 2)})

    def mcast_start(d, _):
        mcast(d).start()
        return 0

    lax.fori_loop(1, nk, mcast_start, 0)
    phase("p_mwait")

    def gcast(d):
        return remote(gpay, grecv.at[z], gzs.at[d], gzr.at[z], {"sp": lax.rem(z + d, nz)})

    def gcast_start(d, _):
        gcast(d).start()
        return 0

    lax.fori_loop(1, nz, gcast_start, 0)

    def mcast_take(d, _):
        k = lax.rem(me + nk - d, nk)
        remote(msum, mods.at[k], ms.at[d], mr.at[k], {"tp": k // 2, "dp": lax.rem(k, 2)}).wait_recv()
        return 0

    lax.fori_loop(1, nk, mcast_take, 0)
    for k in range(nk):
        for j in range(cols // LANES):
            m = mods[k, j * 4 : j * 4 + 4, :]
            at = slice(k * cols + j * LANES, k * cols + (j + 1) * LANES)
            g = gain[:, at]
            ab[0:1, at] = g * (1.0 + m[2:3])
            ab[1:2, at] = m[0:1]
            ab[2:3, at] = g * (1.0 + m[3:4])
            ab[3:4, at] = m[1:2]
    phase("p_mod0")
    tile = hid1.shape[0]
    both = chan + LANES
    piece_cols = 512
    steps = width // piece_cols

    def modulate(src, base, rows, inv, row, dst, to, kk):
        for j in range(piece_cols // LANES):
            start = kk * piece_cols + j * LANES
            at = pl.ds(start if isinstance(start, int) else pl.multiple_of(start, LANES), LANES)
            up_row = ab[row : row + 1, at]
            add_row = ab[row + 1 : row + 2, at]
            for i in range(rows // 32):
                r = inv[base + i * 32 : base + (i + 1) * 32, :]
                xx = src[base + i * 32 : base + (i + 1) * 32, at].astype(F32)
                dst[to + i * 32 : to + (i + 1) * 32, at] = (xx * r * up_row + add_row).astype(BF16)

    def multiply(h):
        rows = h.shape[0]
        acc[0:rows, 0:chan] = dot(h[...], wsg[...])
        acc[0:rows, chan : chan + 2 * LANES] = dot(h[...], wsw[...])

    def modulate_tile(t, dst):
        if OVERLAP:
            for kk in range(steps):
                modulate(lat, t * tile, tile, rinv, 0, dst, 0, kk)
        else:

            def turn(kk, _):
                modulate(lat, t * tile, tile, rinv, 0, dst, 0, kk)
                return 0

            lax.fori_loop(0, steps, turn, 0)

    def mod_first(kk, _):
        modulate(ctx, 0, nctx, rinvc, 2, hid0, 0, kk)
        modulate(lat, 0, tile, rinv, 0, hid0, nctx, kk)
        return 0

    lax.fori_loop(0, steps, mod_first, 0)
    for i in range(5, 7):
        loads[i].wait()
    phase("p_dots0")
    multiply(hid0)
    modulate_tile(2, hid2)
    craw[8 : 8 + nctx, :] = acc[0:nctx, 0:both]
    cstepc[0:nctx, :] = acc[0:nctx, both : both + LANES]
    raw[8 : 8 + tile, :] = acc[nctx : nctx + tile, 0:both]
    stepc[0:tile, :] = acc[nctx : nctx + tile, both : both + LANES]
    cedge_up = remote(craw.at[nctx : nctx + 8], cedge.at[0], ces.at[0], cer.at[0], {"sp": up})
    cedge_down = remote(craw.at[8:16], cedge.at[1], ces.at[1], cer.at[1], {"sp": down})
    cedge_up.start()
    cedge_down.start()
    phase("p_dots2")
    multiply(hid2)
    modulate_tile(1, hid1)
    raw[8 + 2 * tile : 8 + 3 * tile, :] = acc[0:tile, 0:both]
    stepc[2 * tile : 3 * tile, :] = acc[0:tile, both : both + LANES]
    edge_up = remote(raw.at[span : span + 8], edge.at[0], es.at[0], er.at[0], {"sp": up})
    edge_down = remote(raw.at[8:16], edge.at[1], es.at[1], er.at[1], {"sp": down})
    edge_up.start()
    edge_down.start()
    loads[7].wait()
    ends = jnp.concatenate([hid0[nctx : nctx + 16, :], hid2[tile - 16 : tile, :]], axis=0)
    rends = dot(ends, wrd[...])
    rsend[0] = rends[24:32, :]
    rsend[1] = rends[0:8, :]
    redge_up = remote(rsend.at[0], redge.at[0], res.at[0], rer.at[0], {"sp": up})
    redge_down = remote(rsend.at[1], redge.at[1], res.at[1], rer.at[1], {"sp": down})
    redge_up.start()
    redge_down.start()
    phase("p_dots1")
    multiply(hid1)
    raw[8 + tile : 8 + 2 * tile, :] = acc[0:tile, 0:both]
    stepc[tile : 2 * tile, :] = acc[0:tile, both : both + LANES]

    phase("p_ctxstate")
    def conv(block, at):
        n = block.shape[0]
        mix = (
            taps[0:1, at] * pltpu.roll(block, 1, 0)
            + taps[1:2, at] * block
            + taps[2:3, at] * pltpu.roll(block, n - 1, 0)
        )
        return silu(mix[8 : n - 8])

    first = (z == 0).astype(F32)
    last = (z == nz - 1).astype(F32)
    cedge_up.wait_recv()
    cedge_down.wait_recv()
    craw[7:8, :] = cedge[0, 7:8, :] * (1.0 - first)
    craw[8 + nctx : 9 + nctx, :] = cedge[1, 0:1, :] * (1.0 - last)
    is_fwd = row_iota((8, LANES)) < 4
    lane8 = lane_iota((8, LANES))
    tri = (
        lax.broadcasted_iota(jnp.int32, (LANES, LANES), 0)
        <= lax.broadcasted_iota(jnp.int32, (LANES, LANES), 1)
    ).astype(F32)

    def cumulate(a):
        return jnp.dot(a, tri, precision=lax.Precision.HIGHEST, preferred_element_type=F32)

    cstep = jnp.transpose(cstepc[...])[0:8, :]
    cst = softplus(cstep.astype(BF16).astype(F32) + bias)
    cst = jnp.where(lane8 < nctx, cst, 0.0)
    cld = rate * cst
    ccum = cumulate(cld)
    cend = ccum[:, LANES - 1 : LANES]
    cw = jnp.where(is_fwd, jnp.exp(cend - ccum), jnp.exp(ccum - cld)) * cst
    xrows[0, 0:8, :] = cw
    cwt = jnp.transpose(xrows[0:4].reshape(LANES, LANES))[0:nctx, :]
    cblock = [
        conv(craw[0 : nctx + 16, j * LANES : (j + 1) * LANES], slice(j * LANES, (j + 1) * LANES))
        for j in range(chan // LANES + 1)
    ]
    cwr = cblock[-1].astype(BF16)
    for k in range(2):
        for p in range(chan // LANES):
            sc = (cblock[p] * expand(cwt, 4 * k, p)).astype(BF16)
            st = dot_tn(sc, cwr).astype(BF16)
            per = LANES // po
            ctsend[p * per : (p + 1) * per, k] = st.reshape(per, po, LANES)

    def ctcast(d):
        t = lax.rem(z + d, nz)
        return remote(ctsend.at[t], ctrecv.at[z], cs.at[d], cr.at[z], {"sp": t})

    def ctcast_start(d, _):
        ctcast(d).start()
        return 0

    lax.fori_loop(1, nz, ctcast_start, 0)
    ctrecv[z] = ctsend[z]
    phase("p_edge")
    edge_up.wait_recv()
    edge_down.wait_recv()
    raw[7:8, :] = edge[0, 7:8, :] * (1.0 - first)
    raw[8 + span : 9 + span, :] = edge[1, 0:1, :] * (1.0 - last)

    phase("p_conv")

    def conv_block(b, _):
        base = aligned(b, LANES)
        for j in range(chan // LANES + 1):
            at = slice(j * LANES, (j + 1) * LANES)
            val = conv(raw[pl.ds(base, LANES + 16), at], at).astype(BF16)
            if j < chan // LANES:
                sbf[pl.ds(base, LANES), at] = val
            else:
                wbf[pl.ds(base, LANES), :] = val
        return 0

    lax.fori_loop(0, nb, conv_block, 0)

    phase("p_rows")
    for b in range(nb):
        turned = jnp.transpose(stepc[b * LANES : (b + 1) * LANES, :])[0:8, :]
        st = softplus(turned.astype(BF16).astype(F32) + bias)
        strow[b] = st
        ldrow[b] = rate * st + jnp.concatenate(
            [extra[0, :, b * LANES : (b + 1) * LANES], extra[1, :, b * LANES : (b + 1) * LANES]], axis=0
        )
    cum = cumulate(ldrow[...].reshape(nb * 8, LANES))
    ends = [cum[b * 8 : b * 8 + 8, LANES - 1 : LANES] for b in range(nb)]
    zero = jnp.zeros((8, 1), F32)
    before = [zero]
    for b in range(nb):
        before.append(before[-1] + ends[b])
    after = [zero]
    for b in reversed(range(nb)):
        after.append(after[-1] + ends[b])
    after = after[::-1]
    isf1 = row_iota((8, 1)) < 4
    for b in range(nb):
        cb = cum[b * 8 : b * 8 + 8]
        e = cb - ldrow[b]
        end = ends[b]
        near = jnp.where(is_fwd, cb, end - e)
        xrows[b, 0:8, :] = jnp.where(is_fwd, cb, e)
        xrows[b, 8:16, :] = jnp.where(is_fwd, jnp.exp(end - cb), jnp.exp(e)) * strow[b]
        xrows[b, 16:24, :] = jnp.exp(near)
        xrows[b, 24:32, :] = jnp.exp(near + jnp.where(isf1, before[b], after[b + 1]))
        eexp[b] = jnp.broadcast_to(jnp.exp(end), (8, LANES))
    for g in range(-(-nb // 4)):
        turned = jnp.transpose(xrows[g * 4 : g * 4 + 4].reshape(LANES, LANES))
        for b in range(g * 4, min(nb, g * 4 + 4)):
            xt[b] = turned[:, (b - g * 4) * 32 : (b - g * 4 + 1) * 32]

    phase("p_states")
    npair = chan // LANES
    def decayed(state, b, row):
        lo = eexp[b, row : row + 1, :]
        hi = eexp[b, row + 1 : row + 2, :]
        return jnp.where(row_iota((LANES, LANES)) < LANES // 2, lo, hi) * state

    sub8 = row_iota((8, LANES))
    dsend[...] = jnp.sum(
        jnp.where(lane8 == sub8, before[nb], 0.0) + jnp.where(lane8 == sub8 + 8, cend, 0.0),
        axis=0,
        keepdims=True,
    )

    def dcast(d):
        return remote(dsend, drecv.at[z], ds.at[d], dr.at[z], {"sp": lax.rem(z + d, nz)})

    def fcast(d):
        t = lax.rem(z + d, nz)
        return remote(fsend.at[t], frecv.at[z], fs.at[d], fr.at[z], {"sp": t})

    def bcast(d):
        t = lax.rem(z + d, nz)
        return remote(bsend.at[t], brecv.at[z], bs.at[d], br.at[z], {"sp": t})

    def dcast_start(d, _):
        dcast(d).start()
        return 0

    def fcast_start(d, _):
        fcast(d).start()
        return 0

    def bcast_start(d, _):
        bcast(d).start()
        return 0

    lax.fori_loop(1, nz, dcast_start, 0)
    drecv[z] = dsend[...]

    def contribute(first):
        for b in range(nb):
            base = b * LANES
            w = wbf[base : base + LANES, :]
            cl = xt[b]
            for p in range(npair):
                at = slice(p * LANES, (p + 1) * LANES)
                v = sbf[base : base + LANES, at].astype(F32) * expand(cl, first, p)
                loc[b, at, :] = dot_tn(v.astype(BF16), w)

    def chain(order, row, before_ref, send_ref):
        per = LANES // po
        for p in range(npair):
            at = slice(p * LANES, (p + 1) * LANES)
            state = jnp.zeros((LANES, LANES), F32)
            for b in order:
                before_ref[b, at, :] = state.astype(BF16)
                state = decayed(state, b, row + 2 * p) + loc[b, at, :]
            send_ref[p * per : (p + 1) * per] = state.astype(BF16).reshape(per, po, LANES)

    contribute(8)
    chain(range(nb), 0, fpre, fsend)
    lax.fori_loop(1, nz, fcast_start, 0)
    frecv[z] = fsend[z]
    contribute(12)
    chain(range(nb - 1, -1, -1), 4, bpre, bsend)
    lax.fori_loop(1, nz, bcast_start, 0)
    brecv[z] = bsend[z]

    phase("p_gate")
    loads[8].wait()
    hids = (hid0, hid1, hid2)
    for t in (0, 2, 1):
        skip = nctx if t == 0 else 0
        rraw[8 + t * tile : 8 + (t + 1) * tile, :] = dot(hids[t][skip : skip + tile, :], wrd[...])
    for t in range(3):
        skip = nctx if t == 0 else 0
        gbuf[t * tile : (t + 1) * tile, :] = silu(dot(hids[t][skip : skip + tile, :], wog[...]))
    redge_up.wait_recv()
    redge_down.wait_recv()
    rraw[7:8, :] = redge[0, 7:8, :] * (1.0 - first)
    rraw[8 + span : 9 + span, :] = redge[1, 0:1, :] * (1.0 - last)

    def conv_reader(b, _):
        base = aligned(b, LANES)
        block = rraw[pl.ds(base, LANES + 16), :]
        rbf[pl.ds(base, LANES), :] = conv(block, slice(both, both + LANES)).astype(BF16)
        return 0

    lax.fori_loop(0, nb, conv_reader, 0)

    phase("p_inside")
    lower = lax.broadcasted_iota(jnp.int32, (LANES, LANES), 1) <= lax.broadcasted_iota(
        jnp.int32, (LANES, LANES), 0
    )
    upper = lax.broadcasted_iota(jnp.int32, (LANES, LANES), 1) >= lax.broadcasted_iota(
        jnp.int32, (LANES, LANES), 0
    )

    def inside(b, _):
        base = aligned(b, LANES)
        r = rbf[pl.ds(base, LANES), :]
        g = dot_nt(r, wbf[pl.ds(base, LANES), :])
        cl = xt[b]
        for p in range(npair):
            at = slice(p * LANES, (p + 1) * LANES)
            s = sbf[pl.ds(base, LANES), at]
            own = []
            for h in (2 * p, 2 * p + 1):
                arg = jnp.where(
                    lower,
                    cl[:, h : h + 1] - xrows[b, h : h + 1, :],
                    xrows[b, 4 + h : 5 + h, :] - cl[:, 4 + h : 5 + h],
                )
                wgt = jnp.where(lower, strow[b, h : h + 1, :], 0.0) + jnp.where(
                    upper, strow[b, 4 + h : 5 + h, :], 0.0
                )
                own.append(dot((g * jnp.exp(arg) * wgt).astype(BF16), s))
            carried = expand(cl, 16, p) * dot_nt(r, fpre[b, at, :]) + expand(cl, 20, p) * dot_nt(
                r, bpre[b, at, :]
            )
            ybuf[pl.ds(base, LANES), at] = carried + jnp.where(
                lane_iota((LANES, LANES)) < LANES // 2, own[0], own[1]
            )
        return 0

    def inside2(i, _):
        inside(2 * i, 0)
        inside(2 * i + 1, 0)
        return 0

    lax.fori_loop(0, nb // 2, inside2, 0)

    phase("p_fwait")

    def take_forward(d, _):
        src = lax.rem(z + nz - d, nz)
        remote(dsend, drecv.at[src], ds.at[d], dr.at[src], {"sp": src}).wait_recv()
        remote(ctsend.at[src], ctrecv.at[src], cs.at[d], cr.at[src], {"sp": src}).wait_recv()
        remote(fsend.at[src], frecv.at[src], fs.at[d], fr.at[src], {"sp": src}).wait_recv()
        return 0

    lax.fori_loop(1, nz, take_forward, 0)
    phase("p_fscan")
    for k in range(nz):
        dm[k : k + 1, :] = drecv[k]
    head = z * po // (LANES // 2)
    dall = dm[...]
    lane_z = lane_iota((nz, LANES))
    for i in range(4):
        col = jnp.sum(jnp.where(lane_z == 4 * i + head, dall, 0.0), axis=1, keepdims=True)
        ed[i] = jnp.exp(jnp.broadcast_to(col, (nz, LANES)))
    state = jnp.zeros((po, LANES), F32)
    for k in range(nz):
        state = ed[2, k : k + 1, :] * state + ctrecv[k, 0].astype(F32)
    for k in range(nz):
        fback[k] = state.astype(BF16)
        state = ed[0, k : k + 1, :] * state + frecv[k].astype(F32)

    def fret(d):
        t = lax.rem(z + d, nz)
        return remote(fback.at[t], fin.at[z], rs.at[d], rr.at[z], {"sp": t})

    def fret_start(d, _):
        fret(d).start()
        return 0

    def bret(d):
        t = lax.rem(z + d, nz)
        return remote(bback.at[t], bin_.at[z], rbs.at[d], rbr.at[z], {"sp": t})

    def bret_start(d, _):
        bret(d).start()
        return 0

    lax.fori_loop(1, nz, fret_start, 0)
    fin[z] = fback[z]
    phase("p_bwait")

    def take_backward(d, _):
        src = lax.rem(z + nz - d, nz)
        remote(bsend.at[src], brecv.at[src], bs.at[d], br.at[src], {"sp": src}).wait_recv()
        return 0

    lax.fori_loop(1, nz, take_backward, 0)
    phase("p_bscan")
    state = jnp.zeros((po, LANES), F32)
    for k in reversed(range(nz)):
        state = ed[3, k : k + 1, :] * state + ctrecv[k, 1].astype(F32)
    for k in reversed(range(nz)):
        bback[k] = state.astype(BF16)
        state = ed[1, k : k + 1, :] * state + brecv[k].astype(F32)
    lax.fori_loop(1, nz, bret_start, 0)
    bin_[z] = bback[z]
    phase("p_retwait")
    lat_copy.wait_send()
    for sent in (cedge_up, cedge_down, edge_up, edge_down, redge_up, redge_down):
        sent.wait_send()

    def drain_z(d, _):
        zcast(d).wait_send()
        ctcast(d).wait_send()
        gcast(d).wait_send()
        fcast(d).wait_send()
        bcast(d).wait_send()
        dcast(d).wait_send()
        return 0

    lax.fori_loop(1, nz, drain_z, 0)

    def drain_k(d, _):
        mcast(d).wait_send()
        return 0

    lax.fori_loop(1, nk, drain_k, 0)

    def take_return(d, _):
        src = lax.rem(z + nz - d, nz)
        remote(fback.at[src], fin.at[src], rs.at[d], rr.at[src], {"sp": src}).wait_recv()
        remote(bback.at[src], bin_.at[src], rbs.at[d], rbr.at[src], {"sp": src}).wait_recv()
        return 0

    def add_gate(d, total):
        src = lax.rem(z + nz - d, nz)
        remote(gpay, grecv.at[src], gzs.at[d], gzr.at[src], {"sp": src}).wait_recv()
        return total + grecv[src]

    gate = lax.fori_loop(1, nz, add_gate, gpay[...])
    lax.fori_loop(1, nz, take_return, 0)

    phase("p_finish")
    hrow = LANES // 2

    def piece(k, b):
        return nall.at[k, pl.ds(aligned(b, LANES), LANES)]

    def part(k, b, h):
        return nall.at[k, pl.ds(pl.multiple_of(b * LANES + h * hrow, hrow), hrow)]

    def to_partner(k, i, b):
        return remote(piece(k, b), piece(k, b), ps.at[i, b], pr.at[i, b], {"dp": 1 - c})

    k_left = left * 2 + c
    k_right = right * 2 + c
    k_far = lax.rem(x + 2, nx) * 2 + c

    def own_right(b):
        return remote(piece(me, b), piece(me, b), gs.at[0, b], gr.at[0, b], {"tp": right})

    def own_left(b):
        return remote(piece(me, b), piece(me, b), gs.at[1, b], gr.at[1, b], {"tp": left})

    def relay_right(b):
        return remote(part(k_left, b, 0), part(k_left, b, 0), gs2.at[0, b], gr2.at[0, b], {"tp": right})

    def relay_left(b):
        return remote(part(k_right, b, 1), part(k_right, b, 1), gs2.at[1, b], gr2.at[1, b], {"tp": left})

    def finish(b, _):
        base = aligned(b, LANES)
        r = rbf[pl.ds(base, LANES), :]
        cl = xt[b]
        vals = []
        for p in range(npair):
            at = slice(p * LANES, (p + 1) * LANES)
            per = LANES // po
            f_in = fin[p * per : (p + 1) * per].reshape(LANES, LANES)
            b_in = bin_[p * per : (p + 1) * per].reshape(LANES, LANES)
            yy = (
                ybuf[pl.ds(base, LANES), at]
                + expand(cl, 24, p) * dot_nt(r, f_in)
                + expand(cl, 28, p) * dot_nt(r, b_in)
            )
            vals.append(yy * gbuf[pl.ds(base, LANES), at])
        sq = sum(jnp.sum(a * a, axis=1, keepdims=True) for a in vals)
        inv = lax.rsqrt(sq / chan + EPSILON)
        for p in range(npair):
            at = slice(p * LANES, (p + 1) * LANES)
            nall[me, pl.ds(base, LANES), at] = (vals[p] * inv * ggain[:, at]).astype(BF16)
        own_right(b).start()
        own_left(b).start()
        to_partner(me, 0, b).start()
        return 0

    lax.fori_loop(0, nb, finish, 0)
    loads[9].wait()

    phase("p_collect")
    out0 = pl.multiple_of(me * cols, cols)

    flip = 1 - 2 * c

    def product(b, ks):
        base = aligned(b, LANES)
        total = None
        for k in ks:
            w = wout[pl.ds(aligned(k, chan), chan), :]
            part_sum = dot(nall[k, pl.ds(base, LANES), :], w)
            total = part_sum if total is None else total + part_sum
        return total

    def near(b):
        remote(piece(k_left, b), piece(k_left, b), gs.at[0, b], gr.at[0, b], {"tp": left}).wait_recv()
        relay_right(b).start()
        to_partner(k_left, 1, b).start()
        remote(piece(k_right, b), piece(k_right, b), gs.at[1, b], gr.at[1, b], {"tp": right}).wait_recv()
        relay_left(b).start()
        to_partner(k_right, 2, b).start()

    def near_product(b):
        for n, k in enumerate((me, k_left, k_right)):
            to_partner(k + flip, n, b).wait_recv()
        ks = (me, k_left, k_right, me + flip, k_left + flip, k_right + flip)
        oacc[pl.ds(aligned(b, LANES), LANES), :] = product(b, ks)

    near(0)

    def near_turn(b, _):
        near(b)
        near_product(b - 1)
        return 0

    lax.fori_loop(1, nb, near_turn, 0)
    near_product(nb - 1)
    phase("p_far")

    def far(b):
        for h in range(2):
            remote(part(k_far, b, h), part(k_far, b, h), gs2.at[h, b], gr2.at[h, b], {"tp": left}).wait_recv()
        to_partner(k_far, 3, b).start()

    def store(b):
        rows = pl.ds(aligned(b, LANES), LANES)
        return pltpu.make_async_copy(obuf.at[rows], out.at[rows], osem.at[b])

    def far_product(b):
        to_partner(k_far + flip, 3, b).wait_recv()
        rows = pl.ds(aligned(b, LANES), LANES)
        mix = oacc[rows, :] + product(b, (k_far, k_far + flip))
        res_rows = lat[rows, pl.ds(out0, cols)].astype(F32)
        obuf[rows, :] = (res_rows + gate * mix).astype(BF16)
        store(b).start()

    far(0)

    def far_turn(b, _):
        far(b)
        far_product(b - 1)
        return 0

    lax.fori_loop(1, nb, far_turn, 0)
    far_product(nb - 1)

    phase("p_drain")

    def drain_back(d, _):
        fret(d).wait_send()
        bret(d).wait_send()
        return 0

    lax.fori_loop(1, nz, drain_back, 0)

    def drain_b(b, _):
        own_right(b).wait_send()
        own_left(b).wait_send()
        relay_right(b).wait_send()
        relay_left(b).wait_send()
        for i in range(4):
            to_partner(me, i, b).wait_send()
        store(b).wait()
        return 0

    lax.fori_loop(0, nb, drain_b, 0)
    phase(None)


def on_device(
    latent,
    context,
    condition,
    context_condition,
    shift_weight,
    scale_weight,
    gate_weight,
    norm_gain,
    out_gate_weight,
    signal_weight,
    writer_weight,
    reader_matrix,
    step_weight,
    signal_taps,
    writer_taps,
    reader_taps,
    step_bias,
    decay_log,
    decay_extra,
    group_gain,
    output_weight,
):
    nz, nx = lax.axis_size("sp"), lax.axis_size("tp")
    half_rows, width = latent.shape
    span, nctx = 2 * half_rows, context.shape[0]
    chan, cols = out_gate_weight.shape[1], shift_weight.shape[1]
    nb, nk, po = span // LANES, 2 * nx, chan // nz
    full = chan + 2 * LANES
    tile = span // 3
    both = chan + LANES
    hbm = pl.BlockSpec(memory_space=pl.ANY)
    vmem = pl.BlockSpec(memory_space=pltpu.VMEM)
    dma = pltpu.SemaphoreType.DMA
    scratch = [
        ((8, width), F32),
        ((3, full), F32),
        ((3, *shift_weight.shape), BF16),
        ((span, width), BF16),
        ((nctx, width), BF16),
        ((nctx + tile, width), BF16),
        ((tile, width), BF16),
        ((tile, width), BF16),
        ((nctx + tile, full), F32),
        ((width, chan), BF16),
        ((width, chan), BF16),
        ((width, 2 * LANES), BF16),
        ((width, LANES), BF16),
        (output_weight.shape, BF16),
        ((cols // LANES * 4, LANES), BF16),
        ((nz, cols // LANES * 4, LANES), BF16),
        ((1, cols), F32),
        ((nz, 1, cols), F32),
        ((cols // LANES * 4, LANES), F32),
        ((nk, cols // LANES * 4, LANES), F32),
        ((8, width), F32),
        ((span, LANES), F32),
        ((nctx, LANES), F32),
        ((nctx + 16, both), F32),
        ((2, 8, both), F32),
        ((LANES, LANES), F32),
        ((span + 16, both), F32),
        ((2, 8, both), F32),
        ((span + 16, LANES), F32),
        ((2, 8, LANES), F32),
        ((2, 8, LANES), F32),
        ((span, chan), F32),
        ((span, LANES), F32),
        ((span, chan), BF16),
        ((span, LANES), BF16),
        ((span, LANES), BF16),
        ((nb, 8, LANES), F32),
        ((nb, 8, LANES), F32),
        ((-(-nb // 4) * 4, 32, LANES), F32),
        ((nb, LANES, 32), F32),
        ((nb, 8, LANES), F32),
        ((nb, chan, LANES), F32),
        ((nb, chan, LANES), BF16),
        ((nb, chan, LANES), BF16),
        ((nz, po, LANES), BF16),
        ((nz, po, LANES), BF16),
        ((nz, po, LANES), BF16),
        ((nz, po, LANES), BF16),
        ((nz, 2, po, LANES), BF16),
        ((nz, 2, po, LANES), BF16),
        ((1, LANES), F32),
        ((nz, 1, LANES), F32),
        ((nz, LANES), F32),
        ((4, nz, LANES), F32),
        ((nz, po, LANES), BF16),
        ((nz, po, LANES), BF16),
        ((nz, po, LANES), BF16),
        ((nz, po, LANES), BF16),
        ((span, chan), F32),
        ((nk, span, chan), BF16),
        ((span, cols), F32),
        ((span, cols), BF16),
    ]
    sems = (
        [(10,), (nz,), (nz,), (nk,), (nk,)]
        + [(2,)] * 6
        + [(nz,)] * 14
        + [None, None]
        + [(2, nb)] * 4
        + [(4, nb)] * 2
        + [(nb,)]
    )
    return pl.pallas_call(
        functools.partial(kernel, nz, nx),
        out_shape=jax.ShapeDtypeStruct((span, cols), BF16),
        in_specs=[hbm] * 10 + [vmem] * 11,
        out_specs=hbm,
        scratch_shapes=[pltpu.VMEM(s, t) for s, t in scratch]
        + [dma if s is None else dma(s) for s in sems],
        compiler_params=pltpu.CompilerParams(
            collective_id=0, has_side_effects=True, vmem_limit_bytes=56 * 1024 * 1024
        ),
        name="mixing",
    )(
        latent,
        context,
        shift_weight,
        scale_weight,
        gate_weight,
        out_gate_weight,
        signal_weight,
        writer_weight,
        reader_matrix,
        output_weight,
        condition,
        context_condition,
        jnp.transpose(step_weight, (0, 2, 1)),
        norm_gain.reshape(1, width),
        signal_taps,
        writer_taps,
        reader_taps,
        step_bias,
        decay_log,
        decay_extra,
        group_gain.reshape(1, chan),
    )


def solution(mesh):
    in_specs = (
        P(("grp", "sp", "dp"), None),
        P(("grp", "sp"), None),
        P("grp"),
        P(),
        P("sp", ("tp", "dp")),
        P("sp", ("tp", "dp")),
        P("sp", ("tp", "dp")),
        P(),
        P(None, ("tp", "dp")),
        P(None, ("tp", "dp")),
        P(None, ("tp", "dp")),
        P(None, ("tp", "dp")),
        P(None, None, ("tp", "dp")),
        P(None, ("tp", "dp")),
        P(None, ("tp", "dp")),
        P(None, ("tp", "dp")),
        P(None, ("tp", "dp")),
        P(None, ("tp", "dp")),
        P(None, ("tp", "dp"), ("grp", "sp")),
        P(("tp", "dp")),
        P(None, ("tp", "dp")),
    )
    out_specs = P(("grp", "sp"), ("tp", "dp"))
    return jax.shard_map(
        on_device, mesh=mesh, in_specs=in_specs, out_specs=out_specs, check_vma=False
    )
```

```python
import functools

import jax
import jax.numpy as jnp
from jax import lax
from jax.experimental import pallas as pl
from jax.experimental.pallas import tpu as pltpu
from jax.sharding import PartitionSpec as P

EPSILON = 1e-06
OVERLAP = True
MESH = pl.DeviceIdType.MESH
F32 = jnp.float32
BF16 = jnp.bfloat16
LANES = 128
NT = (((1,), (1,)), ((), ()))
TN = (((0,), (0,)), ((), ()))


def silu(v):
    return v * (0.5 + 0.5 * jnp.tanh(0.5 * v))


def softplus(v):
    return jnp.maximum(v, 0.0) + jnp.log1p(jnp.exp(-jnp.abs(v)))


def dot(a, b):
    return jnp.dot(a, b, preferred_element_type=F32)


def dot_nt(a, b):
    return lax.dot_general(a, b, NT, preferred_element_type=F32)


def dot_tn(a, b):
    return lax.dot_general(a, b, TN, preferred_element_type=F32)


def remote(src, dst, send, recv, where):
    return pltpu.make_async_remote_copy(
        src_ref=src, dst_ref=dst, send_sem=send, recv_sem=recv, device_id=where, device_id_type=MESH
    )


def aligned(i, n):
    return pl.multiple_of(i * n, n)


def lane_iota(shape):
    return lax.broadcasted_iota(jnp.int32, shape, len(shape) - 1)


def row_iota(shape):
    return lax.broadcasted_iota(jnp.int32, shape, len(shape) - 2)


def expand(cols, first, pair):
    n = cols.shape[0]
    a = first + 2 * pair
    return jnp.where(lane_iota((n, LANES)) < LANES // 2, cols[:, a : a + 1], cols[:, a + 1 : a + 2])


def kernel(
    nz,
    nx,
    latent,
    context,
    shift_w,
    scale_w,
    gate_w,
    og_w,
    sg_w,
    wr_w,
    rd_w,
    out_w,
    *rest,
):
    small_in, rest = rest[:11], rest[11:]
    (
        out,
        cond,
        ctx_cond,
        stepw_in,
        gain,
        signal_taps,
        writer_taps,
        reader_taps,
        bias_in,
        dlog_in,
        extra,
        ggain,
        condrow,
        taps,
        mw,
        lat,
        ctx,
        hid0,
        hid1,
        hid2,
        acc,
        wog,
        wsg,
        wsw,
        wrd,
        wout,
        pay,
        zrecv,
        gpay,
        grecv,
        msum,
        mods,
        ab,
        rinv,
        rinvc,
        craw,
        cedge,
        cstepc,
        raw,
        edge,
        rraw,
        redge,
        rsend,
        gbuf,
        stepc,
        sbf,
        wtr,
        rbf,
        ldrow,
        strow,
        xrows,
        xt,
        eexp,
        loc,
        fpre,
        bpre,
        fsend,
        frecv,
        bsend,
        brecv,
        ctsend,
        ctrecv,
        dsend,
        drecv,
        dm,
        ed,
        fback,
        fin,
        bback,
        bin_,
        ybuf,
        nall,
        oacc,
        obuf,
        lsem,
        zs,
        zr,
        ms,
        mr,
        es,
        er,
        res,
        rer,
        ces,
        cer,
        gzs,
        gzr,
        fs,
        fr,
        bs,
        br,
        cs,
        cr,
        ds,
        dr,
        rs,
        rr,
        rbs,
        rbr,
        lats,
        latr,
        gs,
        gr,
        gs2,
        gr2,
        ps,
        pr,
        osem,
    ) = rest
    small = (
        cond,
        ctx_cond,
        stepw_in,
        gain,
        signal_taps,
        writer_taps,
        reader_taps,
        bias_in,
        dlog_in,
        extra,
        ggain,
    )
    scopes = []

    def phase(name):
        if scopes:
            scopes.pop().__exit__(None, None, None)
        if name:
            scopes.append(jax.named_scope(name))
            scopes[-1].__enter__()

    phase("p_start")
    half_rows, width = latent.shape
    span = 2 * half_rows
    nctx = context.shape[0]
    nb = span // LANES
    chan = og_w.shape[1]
    cols = shift_w.shape[1]
    po = chan // nz
    nk = nx * 2
    z = lax.axis_index("sp")
    x = lax.axis_index("tp")
    c = lax.axis_index("dp")
    me = x * 2 + c
    up = lax.rem(z + 1, nz)
    down = lax.rem(z + nz - 1, nz)
    right = lax.rem(x + 1, nx)
    left = lax.rem(x + nx - 1, nx)
    own0 = pl.multiple_of(c * half_rows, half_rows)
    oth0 = pl.multiple_of((1 - c) * half_rows, half_rows)

    pairs = [
        (shift_w, mw.at[0]),
        (scale_w, mw.at[1]),
        (gate_w, mw.at[2]),
        (context, ctx),
        (latent, lat.at[pl.ds(own0, half_rows)]),
        (sg_w, wsg),
        (wr_w, wsw.at[:, 0:LANES]),
        (rd_w, wrd),
        (og_w, wog),
        (out_w, wout),
        *zip(small_in, small),
    ]
    loads = [pltpu.make_async_copy(s, d, lsem.at[i]) for i, (s, d) in enumerate(pairs)]
    barrier = pltpu.get_barrier_semaphore()

    def greet_z(d, _):
        pl.semaphore_signal(barrier, inc=1, device_id={"sp": lax.rem(z + d, nz)}, device_id_type=MESH)
        return 0

    def greet_k(d, _):
        k = lax.rem(me + d, nk)
        pl.semaphore_signal(
            barrier, inc=1, device_id={"tp": k // 2, "dp": lax.rem(k, 2)}, device_id_type=MESH
        )
        return 0

    lax.fori_loop(1, nz, greet_z, 0)
    lax.fori_loop(1, nk, greet_k, 0)
    for i in (10, 11, *range(10), *range(12, len(loads))):
        loads[i].start()

    phase("p_matvec")
    zrows = shift_w.shape[0]
    condrow[...] = jnp.zeros_like(condrow)
    loads[10].wait()
    loads[11].wait()
    condrow[0:1, :] = cond[...].astype(F32).reshape(1, width)
    condrow[1:2, :] = ctx_cond[...].astype(F32).reshape(1, width)
    act = silu(condrow[:, pl.ds(aligned(z, zrows), zrows)]).astype(BF16)
    for i in range(3):
        loads[i].wait()
    y = dot(act, mw[0]) + pltpu.roll(dot(act, mw[1]), 2, 0)
    pay[...] = jnp.concatenate(
        [y[0:4, j * LANES : (j + 1) * LANES] for j in range(cols // LANES)], axis=0
    ).astype(BF16)
    gpay[...] = dot(act, mw[2])[0:1, :]

    phase("p_barrier")
    pl.semaphore_wait(barrier, nz - 1 + nk - 1)
    phase("p_zcast")

    def zcast(d):
        return remote(pay, zrecv.at[z], zs.at[d], zr.at[z], {"sp": lax.rem(z + d, nz)})

    def zcast_start(d, _):
        zcast(d).start()
        return 0

    lax.fori_loop(1, nz, zcast_start, 0)
    lat_copy = remote(latent, lat.at[pl.ds(own0, half_rows)], lats, latr, {"dp": 1 - c})
    lat_copy.start()

    for i in range(12, len(loads)):
        loads[i].wait()

    taps[:, 0:chan] = signal_taps[...]
    taps[:, chan : chan + LANES] = writer_taps[...]
    taps[:, chan + LANES : chan + 2 * LANES] = reader_taps[...]
    sub4 = lax.broadcasted_iota(jnp.int32, (8, 4), 0)
    pick4 = lax.broadcasted_iota(jnp.int32, (8, 4), 1) == lax.rem(sub4, 4)

    def column(ref):
        both = jnp.where(sub4 < 4, ref[0:1, :], ref[1:2, :])
        return jnp.sum(jnp.where(pick4, both, 0.0), axis=1, keepdims=True)

    bias = column(bias_in)
    rate = -jnp.exp(column(dlog_in))

    def step_cols(i, _):
        at = pl.ds(aligned(i, LANES), LANES)
        rows = [
            stepw_in[0, :, at].astype(F32),
            stepw_in[1, :, at].astype(F32),
            jnp.zeros((LANES - 8, LANES), F32),
        ]
        wsw[at, LANES : 2 * LANES] = jnp.transpose(jnp.concatenate(rows, axis=0)).astype(BF16)

    def step_cols4(i, _):
        for n in range(4):
            step_cols(i * 4 + n, 0)
        return 0

    lax.fori_loop(0, width // LANES // 4, step_cols4, 0)

    def rms_rows(src, base, rows, dst):
        at = pl.ds(base, rows)
        sums = jnp.zeros((rows, LANES), F32)
        for j in range(width // LANES):
            xx = src[at, j * LANES : (j + 1) * LANES].astype(F32)
            sums = sums + xx * xx
        total = jnp.sum(sums, axis=1, keepdims=True)
        dst[at, :] = jnp.broadcast_to(lax.rsqrt(total / width + EPSILON), (rows, LANES))

    loads[3].wait()
    rms_rows(ctx, 0, nctx, rinvc)
    loads[4].wait()
    rblock = 64

    def rms_own(i, _):
        rms_rows(lat, pl.multiple_of(own0 + i * rblock, rblock), rblock, rinv)
        return 0

    lax.fori_loop(0, half_rows // rblock, rms_own, 0)
    remote(latent, lat.at[pl.ds(oth0, half_rows)], lats, latr, {"dp": 1 - c}).wait_recv()

    def rms_oth(i, _):
        rms_rows(lat, pl.multiple_of(oth0 + i * rblock, rblock), rblock, rinv)
        return 0

    lax.fori_loop(0, half_rows // rblock, rms_oth, 0)

    phase("p_zwait")
    def add_z(d, acc):
        src = lax.rem(z + nz - d, nz)
        remote(pay, zrecv.at[src], zs.at[d], zr.at[src], {"sp": src}).wait_recv()
        return acc + zrecv[src].astype(F32)

    total = lax.fori_loop(1, nz, add_z, pay[...].astype(F32))
    msum[...] = total
    mods[me] = total

    def mcast(d):
        k = lax.rem(me + d, nk)
        return remote(msum, mods.at[me], ms.at[d], mr.at[me], {"tp": k // 2, "dp": lax.rem(k, 2)})

    def mcast_start(d, _):
        mcast(d).start()
        return 0

    lax.fori_loop(1, nk, mcast_start, 0)
    phase("p_mwait")

    def gcast(d):
        return remote(gpay, grecv.at[z], gzs.at[d], gzr.at[z], {"sp": lax.rem(z + d, nz)})

    def gcast_start(d, _):
        gcast(d).start()
        return 0

    lax.fori_loop(1, nz, gcast_start, 0)

    def mcast_take(d, _):
        k = lax.rem(me + nk - d, nk)
        remote(msum, mods.at[k], ms.at[d], mr.at[k], {"tp": k // 2, "dp": lax.rem(k, 2)}).wait_recv()
        return 0

    lax.fori_loop(1, nk, mcast_take, 0)
    for k in range(nk):
        for j in range(cols // LANES):
            m = mods[k, j * 4 : j * 4 + 4, :]
            at = slice(k * cols + j * LANES, k * cols + (j + 1) * LANES)
            g = gain[:, at]
            ab[0:1, at] = g * (1.0 + m[2:3])
            ab[1:2, at] = m[0:1]
            ab[2:3, at] = g * (1.0 + m[3:4])
            ab[3:4, at] = m[1:2]
    phase("p_mod0")
    tile = hid1.shape[0]
    both = chan + LANES
    piece_cols = 512
    steps = width // piece_cols

    def modulate(src, base, rows, inv, row, dst, to, kk):
        for j in range(piece_cols // LANES):
            start = kk * piece_cols + j * LANES
            at = pl.ds(start if isinstance(start, int) else pl.multiple_of(start, LANES), LANES)
            up_row = ab[row : row + 1, at]
            add_row = ab[row + 1 : row + 2, at]
            for i in range(rows // 32):
                r = inv[base + i * 32 : base + (i + 1) * 32, :]
                xx = src[base + i * 32 : base + (i + 1) * 32, at].astype(F32)
                dst[to + i * 32 : to + (i + 1) * 32, at] = (xx * r * up_row + add_row).astype(BF16)

    def multiply(h):
        rows = h.shape[0]
        acc[0:rows, 0:chan] = dot(h[...], wsg[...])
        acc[0:rows, chan : chan + 2 * LANES] = dot(h[...], wsw[...])

    def modulate_tile(t, dst):
        if OVERLAP:
            for kk in range(steps):
                modulate(lat, t * tile, tile, rinv, 0, dst, 0, kk)
        else:

            def turn(kk, _):
                modulate(lat, t * tile, tile, rinv, 0, dst, 0, kk)
                return 0

            lax.fori_loop(0, steps, turn, 0)

    def mod_ctx(kk, _):
        modulate(ctx, 0, nctx, rinvc, 2, hid0, 0, kk)
        return 0

    lax.fori_loop(0, steps, mod_ctx, 0)
    for i in range(5, 7):
        loads[i].wait()
    multiply(hid0.at[0:nctx])
    craw[8 : 8 + nctx, :] = acc[0:nctx, 0:both]
    cstepc[0:nctx, :] = acc[0:nctx, both : both + LANES]
    cedge_up = remote(craw.at[nctx : nctx + 8], cedge.at[0], ces.at[0], cer.at[0], {"sp": up})
    cedge_down = remote(craw.at[8:16], cedge.at[1], ces.at[1], cer.at[1], {"sp": down})
    cedge_up.start()
    cedge_down.start()

    def mod_first(kk, _):
        modulate(lat, 0, tile, rinv, 0, hid0, nctx, kk)
        return 0

    lax.fori_loop(0, steps, mod_first, 0)
    phase("p_dots0")
    modulate_tile(2, hid2)
    multiply(hid0.at[nctx : nctx + tile])
    raw[8 : 8 + tile, :] = acc[0:tile, 0:both]
    stepc[0:tile, :] = acc[0:tile, both : both + LANES]
    phase("p_ctxstate")
    def conv(block, at):
        n = block.shape[0]
        mix = (
            taps[0:1, at] * pltpu.roll(block, 1, 0)
            + taps[1:2, at] * block
            + taps[2:3, at] * pltpu.roll(block, n - 1, 0)
        )
        return silu(mix[8 : n - 8])

    first = (z == 0).astype(F32)
    last = (z == nz - 1).astype(F32)
    cedge_up.wait_recv()
    cedge_down.wait_recv()
    craw[7:8, :] = cedge[0, 7:8, :] * (1.0 - first)
    craw[8 + nctx : 9 + nctx, :] = cedge[1, 0:1, :] * (1.0 - last)
    is_fwd = row_iota((8, LANES)) < 4
    lane8 = lane_iota((8, LANES))
    tri = (
        lax.broadcasted_iota(jnp.int32, (LANES, LANES), 0)
        <= lax.broadcasted_iota(jnp.int32, (LANES, LANES), 1)
    ).astype(F32)

    def cumulate(a):
        return jnp.dot(a, tri, precision=lax.Precision.HIGHEST, preferred_element_type=F32)

    cstep = jnp.transpose(cstepc[...])[0:8, :]
    cst = softplus(cstep.astype(BF16).astype(F32) + bias)
    cst = jnp.where(lane8 < nctx, cst, 0.0)
    cld = rate * cst
    ccum = cumulate(cld)
    cend = ccum[:, LANES - 1 : LANES]
    cw = jnp.where(is_fwd, jnp.exp(cend - ccum), jnp.exp(ccum - cld)) * cst
    xrows[0, 0:8, :] = cw
    cwt = jnp.transpose(xrows[0:4].reshape(LANES, LANES))[0:nctx, :]
    cblock = [
        conv(craw[0 : nctx + 16, j * LANES : (j + 1) * LANES], slice(j * LANES, (j + 1) * LANES))
        for j in range(chan // LANES + 1)
    ]
    cwr = cblock[-1].astype(BF16)
    for k in range(2):
        for p in range(chan // LANES):
            sc = (cblock[p] * expand(cwt, 4 * k, p)).astype(BF16)
            st = dot_tn(sc, cwr).astype(BF16)
            per = LANES // po
            ctsend[p * per : (p + 1) * per, k] = st.reshape(per, po, LANES)

    def ctcast(d):
        t = lax.rem(z + d, nz)
        return remote(ctsend.at[t], ctrecv.at[z], cs.at[d], cr.at[z], {"sp": t})

    def ctcast_start(d, _):
        ctcast(d).start()
        return 0

    lax.fori_loop(1, nz, ctcast_start, 0)
    ctrecv[z] = ctsend[z]
    phase("p_dots2")
    modulate_tile(1, hid1)
    multiply(hid2)
    raw[8 + 2 * tile : 8 + 3 * tile, :] = acc[0:tile, 0:both]
    stepc[2 * tile : 3 * tile, :] = acc[0:tile, both : both + LANES]
    edge_up = remote(raw.at[span : span + 8], edge.at[0], es.at[0], er.at[0], {"sp": up})
    edge_down = remote(raw.at[8:16], edge.at[1], es.at[1], er.at[1], {"sp": down})
    edge_up.start()
    edge_down.start()
    loads[7].wait()
    ends = jnp.concatenate([hid0[nctx : nctx + 16, :], hid2[tile - 16 : tile, :]], axis=0)
    rends = dot(ends, wrd[...])
    rsend[0] = rends[24:32, :]
    rsend[1] = rends[0:8, :]
    redge_up = remote(rsend.at[0], redge.at[0], res.at[0], rer.at[0], {"sp": up})
    redge_down = remote(rsend.at[1], redge.at[1], res.at[1], rer.at[1], {"sp": down})
    redge_up.start()
    redge_down.start()

    phase("p_dots1")
    multiply(hid1)
    raw[8 + tile : 8 + 2 * tile, :] = acc[0:tile, 0:both]
    stepc[tile : 2 * tile, :] = acc[0:tile, both : both + LANES]

    phase("p_edge")
    edge_up.wait_recv()
    edge_down.wait_recv()
    raw[7:8, :] = edge[0, 7:8, :] * (1.0 - first)
    raw[8 + span : 9 + span, :] = edge[1, 0:1, :] * (1.0 - last)

    phase("p_conv")

    def conv_block(b, _):
        base = aligned(b, LANES)
        for j in range(chan // LANES + 1):
            at = slice(j * LANES, (j + 1) * LANES)
            val = conv(raw[pl.ds(base, LANES + 16), at], at)
            if j < chan // LANES:
                sbf[pl.ds(base, LANES), at] = val.astype(BF16)
            else:
                wtr[b] = jnp.transpose(val).astype(BF16)
        return 0

    lax.fori_loop(0, nb, conv_block, 0)

    phase("p_rows")
    for b in range(nb):
        turned = jnp.transpose(stepc[b * LANES : (b + 1) * LANES, :])[0:8, :]
        st = softplus(turned.astype(BF16).astype(F32) + bias)
        strow[b] = st
        ldrow[b] = rate * st + jnp.concatenate(
            [extra[0, :, b * LANES : (b + 1) * LANES], extra[1, :, b * LANES : (b + 1) * LANES]], axis=0
        )
    cum = cumulate(ldrow[...].reshape(nb * 8, LANES))
    ends = [cum[b * 8 : b * 8 + 8, LANES - 1 : LANES] for b in range(nb)]
    zero = jnp.zeros((8, 1), F32)
    before = [zero]
    for b in range(nb):
        before.append(before[-1] + ends[b])
    after = [zero]
    for b in reversed(range(nb)):
        after.append(after[-1] + ends[b])
    after = after[::-1]
    isf1 = row_iota((8, 1)) < 4
    for b in range(nb):
        cb = cum[b * 8 : b * 8 + 8]
        e = cb - ldrow[b]
        end = ends[b]
        near = jnp.where(is_fwd, cb, end - e)
        xrows[b, 0:8, :] = jnp.where(is_fwd, cb, e)
        xrows[b, 8:16, :] = jnp.where(is_fwd, jnp.exp(end - cb), jnp.exp(e)) * strow[b]
        xrows[b, 16:24, :] = jnp.exp(near)
        xrows[b, 24:32, :] = jnp.exp(near + jnp.where(isf1, before[b], after[b + 1]))
        eexp[b] = jnp.broadcast_to(jnp.exp(end), (8, LANES))
    for g in range(-(-nb // 4)):
        turned = jnp.transpose(xrows[g * 4 : g * 4 + 4].reshape(LANES, LANES))
        for b in range(g * 4, min(nb, g * 4 + 4)):
            xt[b] = turned[:, (b - g * 4) * 32 : (b - g * 4 + 1) * 32]

    phase("p_states")
    npair = chan // LANES
    def decays(b, row):
        lanes = lane_iota((1, LANES)) < LANES // 2
        return [
            jnp.where(lanes, eexp[b, r : r + 1, :], eexp[b, r + 1 : r + 2, :])
            for r in range(row, row + 2 * npair, 2)
        ]

    sub8 = row_iota((8, LANES))
    dsend[...] = jnp.sum(
        jnp.where(lane8 == sub8, before[nb], 0.0) + jnp.where(lane8 == sub8 + 8, cend, 0.0),
        axis=0,
        keepdims=True,
    )

    def dcast(d):
        return remote(dsend, drecv.at[z], ds.at[d], dr.at[z], {"sp": lax.rem(z + d, nz)})

    def fcast(d):
        t = lax.rem(z + d, nz)
        return remote(fsend.at[t], frecv.at[z], fs.at[d], fr.at[z], {"sp": t})

    def bcast(d):
        t = lax.rem(z + d, nz)
        return remote(bsend.at[t], brecv.at[z], bs.at[d], br.at[z], {"sp": t})

    def dcast_start(d, _):
        dcast(d).start()
        return 0

    def fcast_start(d, _):
        fcast(d).start()
        return 0

    def bcast_start(d, _):
        bcast(d).start()
        return 0

    lax.fori_loop(1, nz, dcast_start, 0)
    drecv[z] = dsend[...]

    def contribute(first):
        for b in range(nb):
            cl = xt[b]
            parts = [
                sbf[b * LANES : (b + 1) * LANES, p * LANES : (p + 1) * LANES].astype(F32)
                * expand(cl, first, p)
                for p in range(npair)
            ]
            loc[b] = dot(wtr[b], jnp.concatenate(parts, axis=1).astype(BF16))

    def chain(order, row, before_ref, send_ref):
        per = LANES // po
        state = [jnp.zeros((LANES, LANES), F32) for _ in range(npair)]
        for b in order:
            by = decays(b, row)
            for p in range(npair):
                at = slice(p * LANES, (p + 1) * LANES)
                before_ref[b, :, at] = state[p].astype(BF16)
                state[p] = state[p] * by[p] + loc[b, :, at]
        for p in range(npair):
            turned = jnp.transpose(state[p]).astype(BF16)
            send_ref[p * per : (p + 1) * per] = turned.reshape(per, po, LANES)

    contribute(8)
    chain(range(nb), 0, fpre, fsend)
    lax.fori_loop(1, nz, fcast_start, 0)
    frecv[z] = fsend[z]
    contribute(12)
    chain(range(nb - 1, -1, -1), 4, bpre, bsend)
    lax.fori_loop(1, nz, bcast_start, 0)
    brecv[z] = bsend[z]

    phase("p_gate")
    loads[8].wait()
    hids = (hid0, hid1, hid2)
    for t in (0, 2, 1):
        skip = nctx if t == 0 else 0
        rraw[8 + t * tile : 8 + (t + 1) * tile, :] = dot(hids[t][skip : skip + tile, :], wrd[...])
    for t in range(3):
        skip = nctx if t == 0 else 0
        gbuf[t * tile : (t + 1) * tile, :] = silu(dot(hids[t][skip : skip + tile, :], wog[...]))
    redge_up.wait_recv()
    redge_down.wait_recv()
    rraw[7:8, :] = redge[0, 7:8, :] * (1.0 - first)
    rraw[8 + span : 9 + span, :] = redge[1, 0:1, :] * (1.0 - last)

    def conv_reader(b, _):
        base = aligned(b, LANES)
        block = rraw[pl.ds(base, LANES + 16), :]
        rbf[pl.ds(base, LANES), :] = conv(block, slice(both, both + LANES)).astype(BF16)
        return 0

    lax.fori_loop(0, nb, conv_reader, 0)

    phase("p_inside")
    lower = lax.broadcasted_iota(jnp.int32, (LANES, LANES), 1) <= lax.broadcasted_iota(
        jnp.int32, (LANES, LANES), 0
    )
    upper = lax.broadcasted_iota(jnp.int32, (LANES, LANES), 1) >= lax.broadcasted_iota(
        jnp.int32, (LANES, LANES), 0
    )

    def inside(b, _):
        base = aligned(b, LANES)
        r = rbf[pl.ds(base, LANES), :]
        g = dot(r, wtr[b])
        from_left = dot(r, fpre[b])
        from_right = dot(r, bpre[b])
        cl = xt[b]
        for p in range(npair):
            at = slice(p * LANES, (p + 1) * LANES)
            s = sbf[pl.ds(base, LANES), at]
            own = []
            for h in (2 * p, 2 * p + 1):
                arg = jnp.where(
                    lower,
                    cl[:, h : h + 1] - xrows[b, h : h + 1, :],
                    xrows[b, 4 + h : 5 + h, :] - cl[:, 4 + h : 5 + h],
                )
                wgt = jnp.where(lower, strow[b, h : h + 1, :], 0.0) + jnp.where(
                    upper, strow[b, 4 + h : 5 + h, :], 0.0
                )
                own.append(dot((g * jnp.exp(arg) * wgt).astype(BF16), s))
            carried = expand(cl, 16, p) * from_left[:, at] + expand(cl, 20, p) * from_right[:, at]
            ybuf[pl.ds(base, LANES), at] = carried + jnp.where(
                lane_iota((LANES, LANES)) < LANES // 2, own[0], own[1]
            )
        return 0

    def inside2(i, _):
        inside(2 * i, 0)
        inside(2 * i + 1, 0)
        return 0

    lax.fori_loop(0, nb // 2, inside2, 0)

    phase("p_fwait")

    def take_forward(d, _):
        src = lax.rem(z + nz - d, nz)
        remote(dsend, drecv.at[src], ds.at[d], dr.at[src], {"sp": src}).wait_recv()
        remote(ctsend.at[src], ctrecv.at[src], cs.at[d], cr.at[src], {"sp": src}).wait_recv()
        remote(fsend.at[src], frecv.at[src], fs.at[d], fr.at[src], {"sp": src}).wait_recv()
        return 0

    lax.fori_loop(1, nz, take_forward, 0)
    phase("p_fscan")
    for k in range(nz):
        dm[k : k + 1, :] = drecv[k]
    head = z * po // (LANES // 2)
    dall = dm[...]
    lane_z = lane_iota((nz, LANES))
    for i in range(4):
        col = jnp.sum(jnp.where(lane_z == 4 * i + head, dall, 0.0), axis=1, keepdims=True)
        ed[i] = jnp.exp(jnp.broadcast_to(col, (nz, LANES)))
    state = jnp.zeros((po, LANES), F32)
    for k in range(nz):
        state = ed[2, k : k + 1, :] * state + ctrecv[k, 0].astype(F32)
    for k in range(nz):
        fback[k] = state.astype(BF16)
        state = ed[0, k : k + 1, :] * state + frecv[k].astype(F32)

    def fret(d):
        t = lax.rem(z + d, nz)
        return remote(fback.at[t], fin.at[z], rs.at[d], rr.at[z], {"sp": t})

    def fret_start(d, _):
        fret(d).start()
        return 0

    def bret(d):
        t = lax.rem(z + d, nz)
        return remote(bback.at[t], bin_.at[z], rbs.at[d], rbr.at[z], {"sp": t})

    def bret_start(d, _):
        bret(d).start()
        return 0

    lax.fori_loop(1, nz, fret_start, 0)
    fin[z] = fback[z]
    phase("p_bwait")

    def take_backward(d, _):
        src = lax.rem(z + nz - d, nz)
        remote(bsend.at[src], brecv.at[src], bs.at[d], br.at[src], {"sp": src}).wait_recv()
        return 0

    lax.fori_loop(1, nz, take_backward, 0)
    phase("p_bscan")
    state = jnp.zeros((po, LANES), F32)
    for k in reversed(range(nz)):
        state = ed[3, k : k + 1, :] * state + ctrecv[k, 1].astype(F32)
    for k in reversed(range(nz)):
        bback[k] = state.astype(BF16)
        state = ed[1, k : k + 1, :] * state + brecv[k].astype(F32)
    lax.fori_loop(1, nz, bret_start, 0)
    bin_[z] = bback[z]
    phase("p_retwait")
    lat_copy.wait_send()
    for sent in (cedge_up, cedge_down, edge_up, edge_down, redge_up, redge_down):
        sent.wait_send()

    def drain_z(d, _):
        zcast(d).wait_send()
        ctcast(d).wait_send()
        gcast(d).wait_send()
        fcast(d).wait_send()
        bcast(d).wait_send()
        dcast(d).wait_send()
        return 0

    lax.fori_loop(1, nz, drain_z, 0)

    def drain_k(d, _):
        mcast(d).wait_send()
        return 0

    lax.fori_loop(1, nk, drain_k, 0)

    def take_return(d, _):
        src = lax.rem(z + nz - d, nz)
        remote(fback.at[src], fin.at[src], rs.at[d], rr.at[src], {"sp": src}).wait_recv()
        remote(bback.at[src], bin_.at[src], rbs.at[d], rbr.at[src], {"sp": src}).wait_recv()
        return 0

    def add_gate(d, total):
        src = lax.rem(z + nz - d, nz)
        remote(gpay, grecv.at[src], gzs.at[d], gzr.at[src], {"sp": src}).wait_recv()
        return total + grecv[src]

    gate = lax.fori_loop(1, nz, add_gate, gpay[...])
    lax.fori_loop(1, nz, take_return, 0)

    phase("p_finish")
    hrow = LANES // 2

    def piece(k, b):
        return nall.at[k, pl.ds(aligned(b, LANES), LANES)]

    def part(k, b, h):
        return nall.at[k, pl.ds(pl.multiple_of(b * LANES + h * hrow, hrow), hrow)]

    def to_partner(k, i, b):
        return remote(piece(k, b), piece(k, b), ps.at[i, b], pr.at[i, b], {"dp": 1 - c})

    k_left = left * 2 + c
    k_right = right * 2 + c
    k_far = lax.rem(x + 2, nx) * 2 + c

    def own_right(b):
        return remote(piece(me, b), piece(me, b), gs.at[0, b], gr.at[0, b], {"tp": right})

    def own_left(b):
        return remote(piece(me, b), piece(me, b), gs.at[1, b], gr.at[1, b], {"tp": left})

    def relay_right(b):
        return remote(part(k_left, b, 0), part(k_left, b, 0), gs2.at[0, b], gr2.at[0, b], {"tp": right})

    def relay_left(b):
        return remote(part(k_right, b, 1), part(k_right, b, 1), gs2.at[1, b], gr2.at[1, b], {"tp": left})

    def finish(b, _):
        base = aligned(b, LANES)
        r = rbf[pl.ds(base, LANES), :]
        cl = xt[b]
        vals = []
        for p in range(npair):
            at = slice(p * LANES, (p + 1) * LANES)
            per = LANES // po
            f_in = fin[p * per : (p + 1) * per].reshape(LANES, LANES)
            b_in = bin_[p * per : (p + 1) * per].reshape(LANES, LANES)
            yy = (
                ybuf[pl.ds(base, LANES), at]
                + expand(cl, 24, p) * dot_nt(r, f_in)
                + expand(cl, 28, p) * dot_nt(r, b_in)
            )
            vals.append(yy * gbuf[pl.ds(base, LANES), at])
        sq = sum(jnp.sum(a * a, axis=1, keepdims=True) for a in vals)
        inv = lax.rsqrt(sq / chan + EPSILON)
        for p in range(npair):
            at = slice(p * LANES, (p + 1) * LANES)
            nall[me, pl.ds(base, LANES), at] = (vals[p] * inv * ggain[:, at]).astype(BF16)
        own_right(b).start()
        own_left(b).start()
        to_partner(me, 0, b).start()
        return 0

    lax.fori_loop(0, nb, finish, 0)
    loads[9].wait()

    phase("p_collect")
    out0 = pl.multiple_of(me * cols, cols)

    flip = 1 - 2 * c

    def product(b, ks):
        base = aligned(b, LANES)
        total = None
        for k in ks:
            w = wout[pl.ds(aligned(k, chan), chan), :]
            part_sum = dot(nall[k, pl.ds(base, LANES), :], w)
            total = part_sum if total is None else total + part_sum
        return total

    def near(b):
        remote(piece(k_left, b), piece(k_left, b), gs.at[0, b], gr.at[0, b], {"tp": left}).wait_recv()
        relay_right(b).start()
        to_partner(k_left, 1, b).start()
        remote(piece(k_right, b), piece(k_right, b), gs.at[1, b], gr.at[1, b], {"tp": right}).wait_recv()
        relay_left(b).start()
        to_partner(k_right, 2, b).start()

    def near_product(b):
        for n, k in enumerate((me, k_left, k_right)):
            to_partner(k + flip, n, b).wait_recv()
        ks = (me, k_left, k_right, me + flip, k_left + flip, k_right + flip)
        oacc[pl.ds(aligned(b, LANES), LANES), :] = product(b, ks)

    near(0)

    def near_turn(b, _):
        near(b)
        near_product(b - 1)
        return 0

    lax.fori_loop(1, nb, near_turn, 0)
    near_product(nb - 1)
    phase("p_far")

    def far(b):
        for h in range(2):
            remote(part(k_far, b, h), part(k_far, b, h), gs2.at[h, b], gr2.at[h, b], {"tp": left}).wait_recv()
        to_partner(k_far, 3, b).start()

    def store(b):
        rows = pl.ds(aligned(b, LANES), LANES)
        return pltpu.make_async_copy(obuf.at[rows], out.at[rows], osem.at[b])

    def far_product(b):
        to_partner(k_far + flip, 3, b).wait_recv()
        rows = pl.ds(aligned(b, LANES), LANES)
        mix = oacc[rows, :] + product(b, (k_far, k_far + flip))
        res_rows = lat[rows, pl.ds(out0, cols)].astype(F32)
        obuf[rows, :] = (res_rows + gate * mix).astype(BF16)
        store(b).start()

    far(0)

    def far_turn(b, _):
        far(b)
        far_product(b - 1)
        return 0

    lax.fori_loop(1, nb, far_turn, 0)
    far_product(nb - 1)

    phase("p_drain")

    def drain_back(d, _):
        fret(d).wait_send()
        bret(d).wait_send()
        return 0

    lax.fori_loop(1, nz, drain_back, 0)

    def drain_b(b, _):
        own_right(b).wait_send()
        own_left(b).wait_send()
        relay_right(b).wait_send()
        relay_left(b).wait_send()
        for i in range(4):
            to_partner(me, i, b).wait_send()
        store(b).wait()
        return 0

    lax.fori_loop(0, nb, drain_b, 0)
    phase(None)


def on_device(
    latent,
    context,
    condition,
    context_condition,
    shift_weight,
    scale_weight,
    gate_weight,
    norm_gain,
    out_gate_weight,
    signal_weight,
    writer_weight,
    reader_matrix,
    step_weight,
    signal_taps,
    writer_taps,
    reader_taps,
    step_bias,
    decay_log,
    decay_extra,
    group_gain,
    output_weight,
):
    nz, nx = lax.axis_size("sp"), lax.axis_size("tp")
    half_rows, width = latent.shape
    span, nctx = 2 * half_rows, context.shape[0]
    chan, cols = out_gate_weight.shape[1], shift_weight.shape[1]
    nb, nk, po = span // LANES, 2 * nx, chan // nz
    full = chan + 2 * LANES
    tile = span // 3
    both = chan + LANES
    hbm = pl.BlockSpec(memory_space=pl.ANY)
    dma = pltpu.SemaphoreType.DMA
    heads = step_bias.shape[1]
    scratch = [
        (condition.shape, BF16),
        (context_condition.shape, BF16),
        ((2, heads, width), BF16),
        ((1, width), F32),
        (signal_taps.shape, F32),
        (writer_taps.shape, F32),
        (reader_taps.shape, F32),
        (step_bias.shape, F32),
        (decay_log.shape, F32),
        (decay_extra.shape, F32),
        ((1, chan), F32),
        ((8, width), F32),
        ((3, full), F32),
        ((3, *shift_weight.shape), BF16),
        ((span, width), BF16),
        ((nctx, width), BF16),
        ((nctx + tile, width), BF16),
        ((tile, width), BF16),
        ((tile, width), BF16),
        ((nctx + tile, full), F32),
        ((width, chan), BF16),
        ((width, chan), BF16),
        ((width, 2 * LANES), BF16),
        ((width, LANES), BF16),
        (output_weight.shape, BF16),
        ((cols // LANES * 4, LANES), BF16),
        ((nz, cols // LANES * 4, LANES), BF16),
        ((1, cols), F32),
        ((nz, 1, cols), F32),
        ((cols // LANES * 4, LANES), F32),
        ((nk, cols // LANES * 4, LANES), F32),
        ((8, width), F32),
        ((span, LANES), F32),
        ((nctx, LANES), F32),
        ((nctx + 16, both), F32),
        ((2, 8, both), F32),
        ((LANES, LANES), F32),
        ((span + 16, both), F32),
        ((2, 8, both), F32),
        ((span + 16, LANES), F32),
        ((2, 8, LANES), F32),
        ((2, 8, LANES), F32),
        ((span, chan), F32),
        ((span, LANES), F32),
        ((span, chan), BF16),
        ((nb, LANES, LANES), BF16),
        ((span, LANES), BF16),
        ((nb, 8, LANES), F32),
        ((nb, 8, LANES), F32),
        ((-(-nb // 4) * 4, 32, LANES), F32),
        ((nb, LANES, 32), F32),
        ((nb, 8, LANES), F32),
        ((nb, LANES, chan), F32),
        ((nb, LANES, chan), BF16),
        ((nb, LANES, chan), BF16),
        ((nz, po, LANES), BF16),
        ((nz, po, LANES), BF16),
        ((nz, po, LANES), BF16),
        ((nz, po, LANES), BF16),
        ((nz, 2, po, LANES), BF16),
        ((nz, 2, po, LANES), BF16),
        ((1, LANES), F32),
        ((nz, 1, LANES), F32),
        ((nz, LANES), F32),
        ((4, nz, LANES), F32),
        ((nz, po, LANES), BF16),
        ((nz, po, LANES), BF16),
        ((nz, po, LANES), BF16),
        ((nz, po, LANES), BF16),
        ((span, chan), F32),
        ((nk, span, chan), BF16),
        ((span, cols), F32),
        ((span, cols), BF16),
    ]
    sems = (
        [(21,), (nz,), (nz,), (nk,), (nk,)]
        + [(2,)] * 6
        + [(nz,)] * 14
        + [None, None]
        + [(2, nb)] * 4
        + [(4, nb)] * 2
        + [(nb,)]
    )
    return pl.pallas_call(
        functools.partial(kernel, nz, nx),
        out_shape=jax.ShapeDtypeStruct((span, cols), BF16),
        in_specs=[hbm] * 21,
        out_specs=hbm,
        scratch_shapes=[pltpu.VMEM(s, t) for s, t in scratch]
        + [dma if s is None else dma(s) for s in sems],
        compiler_params=pltpu.CompilerParams(
            collective_id=0, has_side_effects=True, vmem_limit_bytes=56 * 1024 * 1024
        ),
        name="mixing",
    )(
        latent,
        context,
        shift_weight,
        scale_weight,
        gate_weight,
        out_gate_weight,
        signal_weight,
        writer_weight,
        reader_matrix,
        output_weight,
        condition,
        context_condition,
        jnp.transpose(step_weight, (0, 2, 1)),
        norm_gain.reshape(1, width),
        signal_taps,
        writer_taps,
        reader_taps,
        step_bias,
        decay_log,
        decay_extra,
        group_gain.reshape(1, chan),
    )


def solution(mesh):
    in_specs = (
        P(("grp", "sp", "dp"), None),
        P(("grp", "sp"), None),
        P("grp"),
        P(),
        P("sp", ("tp", "dp")),
        P("sp", ("tp", "dp")),
        P("sp", ("tp", "dp")),
        P(),
        P(None, ("tp", "dp")),
        P(None, ("tp", "dp")),
        P(None, ("tp", "dp")),
        P(None, ("tp", "dp")),
        P(None, None, ("tp", "dp")),
        P(None, ("tp", "dp")),
        P(None, ("tp", "dp")),
        P(None, ("tp", "dp")),
        P(None, ("tp", "dp")),
        P(None, ("tp", "dp")),
        P(None, ("tp", "dp"), ("grp", "sp")),
        P(("tp", "dp")),
        P(None, ("tp", "dp")),
    )
    out_specs = P(("grp", "sp"), ("tp", "dp"))
    return jax.shard_map(
        on_device, mesh=mesh, in_specs=in_specs, out_specs=out_specs, check_vma=False
    )
```

```python
import functools

import jax
import jax.numpy as jnp
from jax import lax
from jax.experimental import pallas as pl
from jax.experimental.pallas import tpu as pltpu
from jax.sharding import PartitionSpec as P

EPSILON = 1e-06
OVERLAP = True
MESH = pl.DeviceIdType.MESH
F32 = jnp.float32
BF16 = jnp.bfloat16
LANES = 128
NT = (((1,), (1,)), ((), ()))
TN = (((0,), (0,)), ((), ()))


def silu(v):
    return v * (0.5 + 0.5 * jnp.tanh(0.5 * v))


def softplus(v):
    return jnp.maximum(v, 0.0) + jnp.log1p(jnp.exp(-jnp.abs(v)))


def dot(a, b):
    return jnp.dot(a, b, preferred_element_type=F32)


def dot_nt(a, b):
    return lax.dot_general(a, b, NT, preferred_element_type=F32)


def dot_tn(a, b):
    return lax.dot_general(a, b, TN, preferred_element_type=F32)


def remote(src, dst, send, recv, where):
    return pltpu.make_async_remote_copy(
        src_ref=src, dst_ref=dst, send_sem=send, recv_sem=recv, device_id=where, device_id_type=MESH
    )


def aligned(i, n):
    return pl.multiple_of(i * n, n)


def lane_iota(shape):
    return lax.broadcasted_iota(jnp.int32, shape, len(shape) - 1)


def row_iota(shape):
    return lax.broadcasted_iota(jnp.int32, shape, len(shape) - 2)


def expand(cols, first, pair):
    n = cols.shape[0]
    a = first + 2 * pair
    return jnp.where(lane_iota((n, LANES)) < LANES // 2, cols[:, a : a + 1], cols[:, a + 1 : a + 2])


def kernel(
    nz,
    nx,
    latent,
    context,
    shift_w,
    scale_w,
    gate_w,
    og_w,
    sg_w,
    wr_w,
    rd_w,
    out_w,
    *rest,
):
    small_in, rest = rest[:11], rest[11:]
    (
        out,
        cond,
        ctx_cond,
        stepw_in,
        gain,
        signal_taps,
        writer_taps,
        reader_taps,
        bias_in,
        dlog_in,
        extra,
        ggain,
        condrow,
        taps,
        mw,
        lat,
        ctx,
        hidc,
        hid0,
        hid1,
        hid2,
        acc,
        wog,
        wsg,
        wsw,
        wrd,
        wout,
        pay,
        zrecv,
        gpay,
        grecv,
        msum,
        mods,
        ab,
        rinv,
        rinvc,
        craw,
        cedge,
        cstepc,
        raw,
        edge,
        rraw,
        redge,
        rsend,
        esend,
        gbuf,
        stepc,
        sbf,
        wtr,
        rbf,
        ldrow,
        strow,
        xrows,
        xt,
        eexp,
        loc,
        fpre,
        bpre,
        fsend,
        frecv,
        bsend,
        brecv,
        ctsend,
        ctrecv,
        dsend,
        drecv,
        dm,
        ed,
        fback,
        fin,
        bback,
        bin_,
        ybuf,
        nall,
        oacc,
        obuf,
        lsem,
        zs,
        zr,
        ms,
        mr,
        es,
        er,
        res,
        rer,
        ces,
        cer,
        gzs,
        gzr,
        fs,
        fr,
        bs,
        br,
        cs,
        cr,
        ds,
        dr,
        rs,
        rr,
        rbs,
        rbr,
        lats,
        latr,
        gs,
        gr,
        gs2,
        gr2,
        ps,
        pr,
        osem,
    ) = rest
    small = (
        cond,
        ctx_cond,
        stepw_in,
        gain,
        signal_taps,
        writer_taps,
        reader_taps,
        bias_in,
        dlog_in,
        extra,
        ggain,
    )
    scopes = []

    def phase(name):
        if scopes:
            scopes.pop().__exit__(None, None, None)
        if name:
            scopes.append(jax.named_scope(name))
            scopes[-1].__enter__()

    phase("p_start")
    half_rows, width = latent.shape
    span = 2 * half_rows
    nctx = context.shape[0]
    nb = span // LANES
    chan = og_w.shape[1]
    cols = shift_w.shape[1]
    po = chan // nz
    nk = nx * 2
    z = lax.axis_index("sp")
    x = lax.axis_index("tp")
    c = lax.axis_index("dp")
    me = x * 2 + c
    up = lax.rem(z + 1, nz)
    down = lax.rem(z + nz - 1, nz)
    right = lax.rem(x + 1, nx)
    left = lax.rem(x + nx - 1, nx)
    own0 = pl.multiple_of(c * half_rows, half_rows)
    oth0 = pl.multiple_of((1 - c) * half_rows, half_rows)

    pairs = [
        (shift_w, mw.at[0]),
        (scale_w, mw.at[1]),
        (gate_w, mw.at[2]),
        (context, ctx),
        (latent, lat.at[pl.ds(own0, half_rows)]),
        (sg_w, wsg),
        (wr_w, wsw.at[:, 0:LANES]),
        (rd_w, wrd),
        (og_w, wog),
        (out_w, wout),
        *zip(small_in, small),
    ]
    loads = [pltpu.make_async_copy(s, d, lsem.at[i]) for i, (s, d) in enumerate(pairs)]
    barrier = pltpu.get_barrier_semaphore()

    def greet_z(d, _):
        pl.semaphore_signal(barrier, inc=1, device_id={"sp": lax.rem(z + d, nz)}, device_id_type=MESH)
        return 0

    def greet_k(d, _):
        k = lax.rem(me + d, nk)
        pl.semaphore_signal(
            barrier, inc=1, device_id={"tp": k // 2, "dp": lax.rem(k, 2)}, device_id_type=MESH
        )
        return 0

    lax.fori_loop(1, nz, greet_z, 0)
    lax.fori_loop(1, nk, greet_k, 0)
    for i in (10, 11, *range(10), *range(12, len(loads))):
        loads[i].start()

    phase("p_matvec")
    zrows = shift_w.shape[0]
    condrow[...] = jnp.zeros_like(condrow)
    loads[10].wait()
    loads[11].wait()
    condrow[0:1, :] = cond[...].astype(F32).reshape(1, width)
    condrow[1:2, :] = ctx_cond[...].astype(F32).reshape(1, width)
    act = silu(condrow[:, pl.ds(aligned(z, zrows), zrows)]).astype(BF16)
    for i in range(3):
        loads[i].wait()
    y = dot(act, mw[0]) + pltpu.roll(dot(act, mw[1]), 2, 0)
    pay[...] = jnp.concatenate(
        [y[0:4, j * LANES : (j + 1) * LANES] for j in range(cols // LANES)], axis=0
    ).astype(BF16)
    gpay[...] = dot(act, mw[2])[0:1, :]

    phase("p_barrier")
    pl.semaphore_wait(barrier, nz - 1 + nk - 1)
    phase("p_zcast")

    def zcast(d):
        return remote(pay, zrecv.at[z], zs.at[d], zr.at[z], {"sp": lax.rem(z + d, nz)})

    def zcast_start(d, _):
        zcast(d).start()
        return 0

    lax.fori_loop(1, nz, zcast_start, 0)
    lat_copy = remote(latent, lat.at[pl.ds(own0, half_rows)], lats, latr, {"dp": 1 - c})
    lat_copy.start()

    for i in range(12, len(loads)):
        loads[i].wait()

    taps[:, 0:chan] = signal_taps[...]
    taps[:, chan : chan + LANES] = writer_taps[...]
    taps[:, chan + LANES : chan + 2 * LANES] = reader_taps[...]
    sub4 = lax.broadcasted_iota(jnp.int32, (8, 4), 0)
    pick4 = lax.broadcasted_iota(jnp.int32, (8, 4), 1) == lax.rem(sub4, 4)

    def column(ref):
        both = jnp.where(sub4 < 4, ref[0:1, :], ref[1:2, :])
        return jnp.sum(jnp.where(pick4, both, 0.0), axis=1, keepdims=True)

    bias = column(bias_in)
    rate = -jnp.exp(column(dlog_in))

    def step_cols(i, _):
        at = pl.ds(aligned(i, LANES), LANES)
        rows = [
            stepw_in[0, :, at].astype(F32),
            stepw_in[1, :, at].astype(F32),
            jnp.zeros((LANES - 8, LANES), F32),
        ]
        wsw[at, LANES : 2 * LANES] = jnp.transpose(jnp.concatenate(rows, axis=0)).astype(BF16)

    def step_cols4(i, _):
        for n in range(4):
            step_cols(i * 4 + n, 0)
        return 0

    lax.fori_loop(0, width // LANES // 4, step_cols4, 0)

    def rms_rows(src, base, rows, dst):
        at = pl.ds(base, rows)
        sums = jnp.zeros((rows, LANES), F32)
        for j in range(width // LANES):
            xx = src[at, j * LANES : (j + 1) * LANES].astype(F32)
            sums = sums + xx * xx
        total = jnp.sum(sums, axis=1, keepdims=True)
        dst[at, :] = jnp.broadcast_to(lax.rsqrt(total / width + EPSILON), (rows, LANES))

    loads[3].wait()
    rms_rows(ctx, 0, nctx, rinvc)
    loads[4].wait()
    rblock = 64

    def rms_own(i, _):
        rms_rows(lat, pl.multiple_of(own0 + i * rblock, rblock), rblock, rinv)
        return 0

    lax.fori_loop(0, half_rows // rblock, rms_own, 0)
    remote(latent, lat.at[pl.ds(oth0, half_rows)], lats, latr, {"dp": 1 - c}).wait_recv()

    def rms_oth(i, _):
        rms_rows(lat, pl.multiple_of(oth0 + i * rblock, rblock), rblock, rinv)
        return 0

    lax.fori_loop(0, half_rows // rblock, rms_oth, 0)

    phase("p_zwait")
    def add_z(d, acc):
        src = lax.rem(z + nz - d, nz)
        remote(pay, zrecv.at[src], zs.at[d], zr.at[src], {"sp": src}).wait_recv()
        return acc + zrecv[src].astype(F32)

    total = lax.fori_loop(1, nz, add_z, pay[...].astype(F32))
    msum[...] = total
    mods[me] = total

    def mcast(d):
        k = lax.rem(me + d, nk)
        return remote(msum, mods.at[me], ms.at[d], mr.at[me], {"tp": k // 2, "dp": lax.rem(k, 2)})

    def mcast_start(d, _):
        mcast(d).start()
        return 0

    lax.fori_loop(1, nk, mcast_start, 0)
    phase("p_mwait")

    def gcast(d):
        return remote(gpay, grecv.at[z], gzs.at[d], gzr.at[z], {"sp": lax.rem(z + d, nz)})

    def gcast_start(d, _):
        gcast(d).start()
        return 0

    lax.fori_loop(1, nz, gcast_start, 0)

    def mcast_take(d, _):
        k = lax.rem(me + nk - d, nk)
        remote(msum, mods.at[k], ms.at[d], mr.at[k], {"tp": k // 2, "dp": lax.rem(k, 2)}).wait_recv()
        return 0

    lax.fori_loop(1, nk, mcast_take, 0)
    for k in range(nk):
        for j in range(cols // LANES):
            m = mods[k, j * 4 : j * 4 + 4, :]
            at = slice(k * cols + j * LANES, k * cols + (j + 1) * LANES)
            g = gain[:, at]
            ab[0:1, at] = g * (1.0 + m[2:3])
            ab[1:2, at] = m[0:1]
            ab[2:3, at] = g * (1.0 + m[3:4])
            ab[3:4, at] = m[1:2]
    phase("p_mod0")
    tile = hid1.shape[0]
    both = chan + LANES
    piece_cols = 512
    steps = width // piece_cols

    def modulate(src, base, rows, inv, row, dst, to, kk):
        for j in range(piece_cols // LANES):
            start = kk * piece_cols + j * LANES
            at = pl.ds(start if isinstance(start, int) else pl.multiple_of(start, LANES), LANES)
            up_row = ab[row : row + 1, at]
            add_row = ab[row + 1 : row + 2, at]
            for i in range(rows // 32):
                r = inv[base + i * 32 : base + (i + 1) * 32, :]
                xx = src[base + i * 32 : base + (i + 1) * 32, at].astype(F32)
                dst[to + i * 32 : to + (i + 1) * 32, at] = (xx * r * up_row + add_row).astype(BF16)

    def multiply(h):
        rows = h.shape[0]
        acc[0:rows, 0:chan] = dot(h[...], wsg[...])
        acc[0:rows, chan : chan + 2 * LANES] = dot(h[...], wsw[...])

    def modulate_tile(t, dst):
        if OVERLAP:
            for kk in range(steps):
                modulate(lat, t * tile, tile, rinv, 0, dst, 0, kk)
        else:

            def turn(kk, _):
                modulate(lat, t * tile, tile, rinv, 0, dst, 0, kk)
                return 0

            lax.fori_loop(0, steps, turn, 0)

    def mod_ctx(kk, _):
        modulate(ctx, 0, nctx, rinvc, 2, hidc, 0, kk)
        modulate(lat, 0, 32, rinv, 0, hidc, nctx, kk)
        modulate(lat, span - 32, 32, rinv, 0, hidc, nctx + 32, kk)
        return 0

    lax.fori_loop(0, steps, mod_ctx, 0)
    for i in range(5, 8):
        loads[i].wait()
    multiply(hidc)
    craw[8 : 8 + nctx, :] = acc[0:nctx, 0:both]
    cstepc[0:nctx, :] = acc[0:nctx, both : both + LANES]
    cedge_up = remote(craw.at[nctx : nctx + 8], cedge.at[0], ces.at[0], cer.at[0], {"sp": up})
    cedge_down = remote(craw.at[8:16], cedge.at[1], ces.at[1], cer.at[1], {"sp": down})
    cedge_up.start()
    cedge_down.start()
    esend[0] = acc[nctx + 56 : nctx + 64, 0:both]
    esend[1] = acc[nctx : nctx + 8, 0:both]
    rends = dot(hidc[nctx : nctx + 64, :], wrd[...])
    rsend[0] = rends[56:64, :]
    rsend[1] = rends[0:8, :]
    edge_up = remote(esend.at[0], edge.at[0], es.at[0], er.at[0], {"sp": up})
    edge_down = remote(esend.at[1], edge.at[1], es.at[1], er.at[1], {"sp": down})
    redge_up = remote(rsend.at[0], redge.at[0], res.at[0], rer.at[0], {"sp": up})
    redge_down = remote(rsend.at[1], redge.at[1], res.at[1], rer.at[1], {"sp": down})
    for sent in (edge_up, edge_down, redge_up, redge_down):
        sent.start()

    def mod_first(kk, _):
        modulate(lat, 0, tile, rinv, 0, hid0, 0, kk)
        return 0

    lax.fori_loop(0, steps, mod_first, 0)
    phase("p_dots0")
    modulate_tile(2, hid2)
    multiply(hid0)
    raw[8 : 8 + tile, :] = acc[0:tile, 0:both]
    stepc[0:tile, :] = acc[0:tile, both : both + LANES]
    phase("p_ctxstate")
    def conv(block, at):
        n = block.shape[0]
        mix = (
            taps[0:1, at] * pltpu.roll(block, 1, 0)
            + taps[1:2, at] * block
            + taps[2:3, at] * pltpu.roll(block, n - 1, 0)
        )
        return silu(mix[8 : n - 8])

    first = (z == 0).astype(F32)
    last = (z == nz - 1).astype(F32)
    cedge_up.wait_recv()
    cedge_down.wait_recv()
    craw[7:8, :] = cedge[0, 7:8, :] * (1.0 - first)
    craw[8 + nctx : 9 + nctx, :] = cedge[1, 0:1, :] * (1.0 - last)
    is_fwd = row_iota((8, LANES)) < 4
    lane8 = lane_iota((8, LANES))
    tri = (
        lax.broadcasted_iota(jnp.int32, (LANES, LANES), 0)
        <= lax.broadcasted_iota(jnp.int32, (LANES, LANES), 1)
    ).astype(F32)

    def cumulate(a):
        return jnp.dot(a, tri, precision=lax.Precision.HIGHEST, preferred_element_type=F32)

    cstep = jnp.transpose(cstepc[...])[0:8, :]
    cst = softplus(cstep.astype(BF16).astype(F32) + bias)
    cst = jnp.where(lane8 < nctx, cst, 0.0)
    cld = rate * cst
    ccum = cumulate(cld)
    cend = ccum[:, LANES - 1 : LANES]
    cw = jnp.where(is_fwd, jnp.exp(cend - ccum), jnp.exp(ccum - cld)) * cst
    xrows[0, 0:8, :] = cw
    cwt = jnp.transpose(xrows[0:4].reshape(LANES, LANES))[0:nctx, :]
    cblock = [
        conv(craw[0 : nctx + 16, j * LANES : (j + 1) * LANES], slice(j * LANES, (j + 1) * LANES))
        for j in range(chan // LANES + 1)
    ]
    cwr = cblock[-1].astype(BF16)
    for k in range(2):
        for p in range(chan // LANES):
            sc = (cblock[p] * expand(cwt, 4 * k, p)).astype(BF16)
            st = dot_tn(sc, cwr).astype(BF16)
            per = LANES // po
            ctsend[p * per : (p + 1) * per, k] = st.reshape(per, po, LANES)

    def ctcast(d):
        t = lax.rem(z + d, nz)
        return remote(ctsend.at[t], ctrecv.at[z], cs.at[d], cr.at[z], {"sp": t})

    def ctcast_start(d, _):
        ctcast(d).start()
        return 0

    lax.fori_loop(1, nz, ctcast_start, 0)
    ctrecv[z] = ctsend[z]
    phase("p_dots2")
    modulate_tile(1, hid1)
    multiply(hid2)
    raw[8 + 2 * tile : 8 + 3 * tile, :] = acc[0:tile, 0:both]
    stepc[2 * tile : 3 * tile, :] = acc[0:tile, both : both + LANES]
    phase("p_dots1")
    multiply(hid1)
    raw[8 + tile : 8 + 2 * tile, :] = acc[0:tile, 0:both]
    stepc[tile : 2 * tile, :] = acc[0:tile, both : both + LANES]

    phase("p_edge")
    edge_up.wait_recv()
    edge_down.wait_recv()
    raw[7:8, :] = edge[0, 7:8, :] * (1.0 - first)
    raw[8 + span : 9 + span, :] = edge[1, 0:1, :] * (1.0 - last)

    phase("p_conv")

    def conv_block(b, _):
        base = aligned(b, LANES)
        for j in range(chan // LANES + 1):
            at = slice(j * LANES, (j + 1) * LANES)
            val = conv(raw[pl.ds(base, LANES + 16), at], at)
            if j < chan // LANES:
                sbf[pl.ds(base, LANES), at] = val.astype(BF16)
            else:
                wtr[b] = jnp.transpose(val).astype(BF16)
        return 0

    lax.fori_loop(0, nb, conv_block, 0)

    phase("p_rows")
    for b in range(nb):
        turned = jnp.transpose(stepc[b * LANES : (b + 1) * LANES, :])[0:8, :]
        st = softplus(turned.astype(BF16).astype(F32) + bias)
        strow[b] = st
        ldrow[b] = rate * st + jnp.concatenate(
            [extra[0, :, b * LANES : (b + 1) * LANES], extra[1, :, b * LANES : (b + 1) * LANES]], axis=0
        )
    cum = cumulate(ldrow[...].reshape(nb * 8, LANES))
    ends = [cum[b * 8 : b * 8 + 8, LANES - 1 : LANES] for b in range(nb)]
    zero = jnp.zeros((8, 1), F32)
    before = [zero]
    for b in range(nb):
        before.append(before[-1] + ends[b])
    after = [zero]
    for b in reversed(range(nb)):
        after.append(after[-1] + ends[b])
    after = after[::-1]
    isf1 = row_iota((8, 1)) < 4
    for b in range(nb):
        cb = cum[b * 8 : b * 8 + 8]
        e = cb - ldrow[b]
        end = ends[b]
        near = jnp.where(is_fwd, cb, end - e)
        xrows[b, 0:8, :] = jnp.where(is_fwd, cb, e)
        xrows[b, 8:16, :] = jnp.where(is_fwd, jnp.exp(end - cb), jnp.exp(e)) * strow[b]
        xrows[b, 16:24, :] = jnp.exp(near)
        xrows[b, 24:32, :] = jnp.exp(near + jnp.where(isf1, before[b], after[b + 1]))
        eexp[b] = jnp.broadcast_to(jnp.exp(end), (8, LANES))
    for g in range(-(-nb // 4)):
        turned = jnp.transpose(xrows[g * 4 : g * 4 + 4].reshape(LANES, LANES))
        for b in range(g * 4, min(nb, g * 4 + 4)):
            xt[b] = turned[:, (b - g * 4) * 32 : (b - g * 4 + 1) * 32]

    phase("p_states")
    npair = chan // LANES
    def decays(b, row):
        lanes = lane_iota((1, LANES)) < LANES // 2
        return [
            jnp.where(lanes, eexp[b, r : r + 1, :], eexp[b, r + 1 : r + 2, :])
            for r in range(row, row + 2 * npair, 2)
        ]

    sub8 = row_iota((8, LANES))
    dsend[...] = jnp.sum(
        jnp.where(lane8 == sub8, before[nb], 0.0) + jnp.where(lane8 == sub8 + 8, cend, 0.0),
        axis=0,
        keepdims=True,
    )

    def dcast(d):
        return remote(dsend, drecv.at[z], ds.at[d], dr.at[z], {"sp": lax.rem(z + d, nz)})

    def fcast(d):
        t = lax.rem(z + d, nz)
        return remote(fsend.at[t], frecv.at[z], fs.at[d], fr.at[z], {"sp": t})

    def bcast(d):
        t = lax.rem(z + d, nz)
        return remote(bsend.at[t], brecv.at[z], bs.at[d], br.at[z], {"sp": t})

    def dcast_start(d, _):
        dcast(d).start()
        return 0

    def fcast_start(d, _):
        fcast(d).start()
        return 0

    def bcast_start(d, _):
        bcast(d).start()
        return 0

    lax.fori_loop(1, nz, dcast_start, 0)
    drecv[z] = dsend[...]

    def contribute(first):
        for b in range(nb):
            cl = xt[b]
            parts = [
                sbf[b * LANES : (b + 1) * LANES, p * LANES : (p + 1) * LANES].astype(F32)
                * expand(cl, first, p)
                for p in range(npair)
            ]
            loc[b] = dot(wtr[b], jnp.concatenate(parts, axis=1).astype(BF16))

    def chain(order, row, before_ref, send_ref):
        per = LANES // po
        state = [jnp.zeros((LANES, LANES), F32) for _ in range(npair)]
        for b in order:
            by = decays(b, row)
            for p in range(npair):
                at = slice(p * LANES, (p + 1) * LANES)
                before_ref[b, :, at] = state[p].astype(BF16)
                state[p] = state[p] * by[p] + loc[b, :, at]
        for p in range(npair):
            turned = jnp.transpose(state[p]).astype(BF16)
            send_ref[p * per : (p + 1) * per] = turned.reshape(per, po, LANES)

    contribute(8)
    chain(range(nb), 0, fpre, fsend)
    lax.fori_loop(1, nz, fcast_start, 0)
    frecv[z] = fsend[z]
    contribute(12)
    chain(range(nb - 1, -1, -1), 4, bpre, bsend)
    lax.fori_loop(1, nz, bcast_start, 0)
    brecv[z] = bsend[z]

    phase("p_gate")
    loads[8].wait()
    hids = (hid0, hid1, hid2)
    for t in (0, 2, 1):
        rraw[8 + t * tile : 8 + (t + 1) * tile, :] = dot(hids[t][...], wrd[...])
    for t in range(3):
        gbuf[t * tile : (t + 1) * tile, :] = silu(dot(hids[t][...], wog[...]))
    redge_up.wait_recv()
    redge_down.wait_recv()
    rraw[7:8, :] = redge[0, 7:8, :] * (1.0 - first)
    rraw[8 + span : 9 + span, :] = redge[1, 0:1, :] * (1.0 - last)

    def conv_reader(b, _):
        base = aligned(b, LANES)
        block = rraw[pl.ds(base, LANES + 16), :]
        rbf[pl.ds(base, LANES), :] = conv(block, slice(both, both + LANES)).astype(BF16)
        return 0

    lax.fori_loop(0, nb, conv_reader, 0)

    phase("p_inside")
    lower = lax.broadcasted_iota(jnp.int32, (LANES, LANES), 1) <= lax.broadcasted_iota(
        jnp.int32, (LANES, LANES), 0
    )
    upper = lax.broadcasted_iota(jnp.int32, (LANES, LANES), 1) >= lax.broadcasted_iota(
        jnp.int32, (LANES, LANES), 0
    )

    def inside(b, _):
        base = aligned(b, LANES)
        r = rbf[pl.ds(base, LANES), :]
        g = dot(r, wtr[b])
        from_left = dot(r, fpre[b])
        from_right = dot(r, bpre[b])
        cl = xt[b]
        for p in range(npair):
            at = slice(p * LANES, (p + 1) * LANES)
            s = sbf[pl.ds(base, LANES), at]
            own = []
            for h in (2 * p, 2 * p + 1):
                arg = jnp.where(
                    lower,
                    cl[:, h : h + 1] - xrows[b, h : h + 1, :],
                    xrows[b, 4 + h : 5 + h, :] - cl[:, 4 + h : 5 + h],
                )
                wgt = jnp.where(lower, strow[b, h : h + 1, :], 0.0) + jnp.where(
                    upper, strow[b, 4 + h : 5 + h, :], 0.0
                )
                own.append(dot((g * jnp.exp(arg) * wgt).astype(BF16), s))
            carried = expand(cl, 16, p) * from_left[:, at] + expand(cl, 20, p) * from_right[:, at]
            ybuf[pl.ds(base, LANES), at] = carried + jnp.where(
                lane_iota((LANES, LANES)) < LANES // 2, own[0], own[1]
            )
        return 0

    def inside2(i, _):
        inside(2 * i, 0)
        inside(2 * i + 1, 0)
        return 0

    lax.fori_loop(0, nb // 2, inside2, 0)

    phase("p_fwait")

    def take_forward(d, _):
        src = lax.rem(z + nz - d, nz)
        remote(dsend, drecv.at[src], ds.at[d], dr.at[src], {"sp": src}).wait_recv()
        remote(ctsend.at[src], ctrecv.at[src], cs.at[d], cr.at[src], {"sp": src}).wait_recv()
        remote(fsend.at[src], frecv.at[src], fs.at[d], fr.at[src], {"sp": src}).wait_recv()
        return 0

    lax.fori_loop(1, nz, take_forward, 0)
    phase("p_fscan")
    for k in range(nz):
        dm[k : k + 1, :] = drecv[k]
    head = z * po // (LANES // 2)
    dall = dm[...]
    lane_z = lane_iota((nz, LANES))
    for i in range(4):
        col = jnp.sum(jnp.where(lane_z == 4 * i + head, dall, 0.0), axis=1, keepdims=True)
        ed[i] = jnp.exp(jnp.broadcast_to(col, (nz, LANES)))
    state = jnp.zeros((po, LANES), F32)
    for k in range(nz):
        state = ed[2, k : k + 1, :] * state + ctrecv[k, 0].astype(F32)
    for k in range(nz):
        fback[k] = state.astype(BF16)
        state = ed[0, k : k + 1, :] * state + frecv[k].astype(F32)

    def fret(d):
        t = lax.rem(z + d, nz)
        return remote(fback.at[t], fin.at[z], rs.at[d], rr.at[z], {"sp": t})

    def fret_start(d, _):
        fret(d).start()
        return 0

    def bret(d):
        t = lax.rem(z + d, nz)
        return remote(bback.at[t], bin_.at[z], rbs.at[d], rbr.at[z], {"sp": t})

    def bret_start(d, _):
        bret(d).start()
        return 0

    lax.fori_loop(1, nz, fret_start, 0)
    fin[z] = fback[z]
    phase("p_bwait")

    def take_backward(d, _):
        src = lax.rem(z + nz - d, nz)
        remote(bsend.at[src], brecv.at[src], bs.at[d], br.at[src], {"sp": src}).wait_recv()
        return 0

    lax.fori_loop(1, nz, take_backward, 0)
    phase("p_bscan")
    state = jnp.zeros((po, LANES), F32)
    for k in reversed(range(nz)):
        state = ed[3, k : k + 1, :] * state + ctrecv[k, 1].astype(F32)
    for k in reversed(range(nz)):
        bback[k] = state.astype(BF16)
        state = ed[1, k : k + 1, :] * state + brecv[k].astype(F32)
    lax.fori_loop(1, nz, bret_start, 0)
    bin_[z] = bback[z]
    phase("p_retwait")
    lat_copy.wait_send()
    for sent in (cedge_up, cedge_down, edge_up, edge_down, redge_up, redge_down):
        sent.wait_send()

    def drain_z(d, _):
        zcast(d).wait_send()
        ctcast(d).wait_send()
        gcast(d).wait_send()
        fcast(d).wait_send()
        bcast(d).wait_send()
        dcast(d).wait_send()
        return 0

    lax.fori_loop(1, nz, drain_z, 0)

    def drain_k(d, _):
        mcast(d).wait_send()
        return 0

    lax.fori_loop(1, nk, drain_k, 0)

    def take_return(d, _):
        src = lax.rem(z + nz - d, nz)
        remote(fback.at[src], fin.at[src], rs.at[d], rr.at[src], {"sp": src}).wait_recv()
        remote(bback.at[src], bin_.at[src], rbs.at[d], rbr.at[src], {"sp": src}).wait_recv()
        return 0

    def add_gate(d, total):
        src = lax.rem(z + nz - d, nz)
        remote(gpay, grecv.at[src], gzs.at[d], gzr.at[src], {"sp": src}).wait_recv()
        return total + grecv[src]

    gate = lax.fori_loop(1, nz, add_gate, gpay[...])
    lax.fori_loop(1, nz, take_return, 0)

    phase("p_finish")
    hrow = LANES // 2

    def piece(k, b):
        return nall.at[k, pl.ds(aligned(b, LANES), LANES)]

    def part(k, b, h):
        return nall.at[k, pl.ds(pl.multiple_of(b * LANES + h * hrow, hrow), hrow)]

    def to_partner(k, i, b):
        return remote(piece(k, b), piece(k, b), ps.at[i, b], pr.at[i, b], {"dp": 1 - c})

    k_left = left * 2 + c
    k_right = right * 2 + c
    k_far = lax.rem(x + 2, nx) * 2 + c

    def own_right(b):
        return remote(piece(me, b), piece(me, b), gs.at[0, b], gr.at[0, b], {"tp": right})

    def own_left(b):
        return remote(piece(me, b), piece(me, b), gs.at[1, b], gr.at[1, b], {"tp": left})

    def relay_right(b):
        return remote(part(k_left, b, 0), part(k_left, b, 0), gs2.at[0, b], gr2.at[0, b], {"tp": right})

    def relay_left(b):
        return remote(part(k_right, b, 1), part(k_right, b, 1), gs2.at[1, b], gr2.at[1, b], {"tp": left})

    def finish(b, _):
        base = aligned(b, LANES)
        r = rbf[pl.ds(base, LANES), :]
        cl = xt[b]
        vals = []
        for p in range(npair):
            at = slice(p * LANES, (p + 1) * LANES)
            per = LANES // po
            f_in = fin[p * per : (p + 1) * per].reshape(LANES, LANES)
            b_in = bin_[p * per : (p + 1) * per].reshape(LANES, LANES)
            yy = (
                ybuf[pl.ds(base, LANES), at]
                + expand(cl, 24, p) * dot_nt(r, f_in)
                + expand(cl, 28, p) * dot_nt(r, b_in)
            )
            vals.append(yy * gbuf[pl.ds(base, LANES), at])
        sq = sum(jnp.sum(a * a, axis=1, keepdims=True) for a in vals)
        inv = lax.rsqrt(sq / chan + EPSILON)
        for p in range(npair):
            at = slice(p * LANES, (p + 1) * LANES)
            nall[me, pl.ds(base, LANES), at] = (vals[p] * inv * ggain[:, at]).astype(BF16)
        own_right(b).start()
        own_left(b).start()
        to_partner(me, 0, b).start()
        return 0

    lax.fori_loop(0, nb, finish, 0)
    loads[9].wait()

    phase("p_collect")
    out0 = pl.multiple_of(me * cols, cols)

    flip = 1 - 2 * c

    def product(b, ks):
        base = aligned(b, LANES)
        total = None
        for k in ks:
            w = wout[pl.ds(aligned(k, chan), chan), :]
            part_sum = dot(nall[k, pl.ds(base, LANES), :], w)
            total = part_sum if total is None else total + part_sum
        return total

    def near(b):
        remote(piece(k_left, b), piece(k_left, b), gs.at[0, b], gr.at[0, b], {"tp": left}).wait_recv()
        relay_right(b).start()
        to_partner(k_left, 1, b).start()
        remote(piece(k_right, b), piece(k_right, b), gs.at[1, b], gr.at[1, b], {"tp": right}).wait_recv()
        relay_left(b).start()
        to_partner(k_right, 2, b).start()

    def near_product(b):
        for n, k in enumerate((me, k_left, k_right)):
            to_partner(k + flip, n, b).wait_recv()
        ks = (me, k_left, k_right, me + flip, k_left + flip, k_right + flip)
        oacc[pl.ds(aligned(b, LANES), LANES), :] = product(b, ks)

    near(0)

    def near_turn(b, _):
        near(b)
        near_product(b - 1)
        return 0

    lax.fori_loop(1, nb, near_turn, 0)
    near_product(nb - 1)
    phase("p_far")

    def far(b):
        for h in range(2):
            remote(part(k_far, b, h), part(k_far, b, h), gs2.at[h, b], gr2.at[h, b], {"tp": left}).wait_recv()
        to_partner(k_far, 3, b).start()

    def store(b):
        rows = pl.ds(aligned(b, LANES), LANES)
        return pltpu.make_async_copy(obuf.at[rows], out.at[rows], osem.at[b])

    def far_product(b):
        to_partner(k_far + flip, 3, b).wait_recv()
        rows = pl.ds(aligned(b, LANES), LANES)
        mix = oacc[rows, :] + product(b, (k_far, k_far + flip))
        res_rows = lat[rows, pl.ds(out0, cols)].astype(F32)
        obuf[rows, :] = (res_rows + gate * mix).astype(BF16)
        store(b).start()

    far(0)

    def far_turn(b, _):
        far(b)
        far_product(b - 1)
        return 0

    lax.fori_loop(1, nb, far_turn, 0)
    far_product(nb - 1)

    phase("p_drain")

    def drain_back(d, _):
        fret(d).wait_send()
        bret(d).wait_send()
        return 0

    lax.fori_loop(1, nz, drain_back, 0)

    def drain_b(b, _):
        own_right(b).wait_send()
        own_left(b).wait_send()
        relay_right(b).wait_send()
        relay_left(b).wait_send()
        for i in range(4):
            to_partner(me, i, b).wait_send()
        store(b).wait()
        return 0

    lax.fori_loop(0, nb, drain_b, 0)
    phase(None)


def on_device(
    latent,
    context,
    condition,
    context_condition,
    shift_weight,
    scale_weight,
    gate_weight,
    norm_gain,
    out_gate_weight,
    signal_weight,
    writer_weight,
    reader_matrix,
    step_weight,
    signal_taps,
    writer_taps,
    reader_taps,
    step_bias,
    decay_log,
    decay_extra,
    group_gain,
    output_weight,
):
    nz, nx = lax.axis_size("sp"), lax.axis_size("tp")
    half_rows, width = latent.shape
    span, nctx = 2 * half_rows, context.shape[0]
    chan, cols = out_gate_weight.shape[1], shift_weight.shape[1]
    nb, nk, po = span // LANES, 2 * nx, chan // nz
    full = chan + 2 * LANES
    tile = span // 3
    both = chan + LANES
    hbm = pl.BlockSpec(memory_space=pl.ANY)
    dma = pltpu.SemaphoreType.DMA
    heads = step_bias.shape[1]
    scratch = [
        (condition.shape, BF16),
        (context_condition.shape, BF16),
        ((2, heads, width), BF16),
        ((1, width), F32),
        (signal_taps.shape, F32),
        (writer_taps.shape, F32),
        (reader_taps.shape, F32),
        (step_bias.shape, F32),
        (decay_log.shape, F32),
        (decay_extra.shape, F32),
        ((1, chan), F32),
        ((8, width), F32),
        ((3, full), F32),
        ((3, *shift_weight.shape), BF16),
        ((span, width), BF16),
        ((nctx, width), BF16),
        ((nctx + 64, width), BF16),
        ((tile, width), BF16),
        ((tile, width), BF16),
        ((tile, width), BF16),
        ((tile, full), F32),
        ((width, chan), BF16),
        ((width, chan), BF16),
        ((width, 2 * LANES), BF16),
        ((width, LANES), BF16),
        (output_weight.shape, BF16),
        ((cols // LANES * 4, LANES), BF16),
        ((nz, cols // LANES * 4, LANES), BF16),
        ((1, cols), F32),
        ((nz, 1, cols), F32),
        ((cols // LANES * 4, LANES), F32),
        ((nk, cols // LANES * 4, LANES), F32),
        ((8, width), F32),
        ((span, LANES), F32),
        ((nctx, LANES), F32),
        ((nctx + 16, both), F32),
        ((2, 8, both), F32),
        ((LANES, LANES), F32),
        ((span + 16, both), F32),
        ((2, 8, both), F32),
        ((span + 16, LANES), F32),
        ((2, 8, LANES), F32),
        ((2, 8, LANES), F32),
        ((2, 8, both), F32),
        ((span, chan), F32),
        ((span, LANES), F32),
        ((span, chan), BF16),
        ((nb, LANES, LANES), BF16),
        ((span, LANES), BF16),
        ((nb, 8, LANES), F32),
        ((nb, 8, LANES), F32),
        ((-(-nb // 4) * 4, 32, LANES), F32),
        ((nb, LANES, 32), F32),
        ((nb, 8, LANES), F32),
        ((nb, LANES, chan), F32),
        ((nb, LANES, chan), BF16),
        ((nb, LANES, chan), BF16),
        ((nz, po, LANES), BF16),
        ((nz, po, LANES), BF16),
        ((nz, po, LANES), BF16),
        ((nz, po, LANES), BF16),
        ((nz, 2, po, LANES), BF16),
        ((nz, 2, po, LANES), BF16),
        ((1, LANES), F32),
        ((nz, 1, LANES), F32),
        ((nz, LANES), F32),
        ((4, nz, LANES), F32),
        ((nz, po, LANES), BF16),
        ((nz, po, LANES), BF16),
        ((nz, po, LANES), BF16),
        ((nz, po, LANES), BF16),
        ((span, chan), F32),
        ((nk, span, chan), BF16),
        ((span, cols), F32),
        ((span, cols), BF16),
    ]
    sems = (
        [(21,), (nz,), (nz,), (nk,), (nk,)]
        + [(2,)] * 6
        + [(nz,)] * 14
        + [None, None]
        + [(2, nb)] * 4
        + [(4, nb)] * 2
        + [(nb,)]
    )
    return pl.pallas_call(
        functools.partial(kernel, nz, nx),
        out_shape=jax.ShapeDtypeStruct((span, cols), BF16),
        in_specs=[hbm] * 21,
        out_specs=hbm,
        scratch_shapes=[pltpu.VMEM(s, t) for s, t in scratch]
        + [dma if s is None else dma(s) for s in sems],
        compiler_params=pltpu.CompilerParams(
            collective_id=0, has_side_effects=True, vmem_limit_bytes=56 * 1024 * 1024
        ),
        name="mixing",
    )(
        latent,
        context,
        shift_weight,
        scale_weight,
        gate_weight,
        out_gate_weight,
        signal_weight,
        writer_weight,
        reader_matrix,
        output_weight,
        condition,
        context_condition,
        jnp.transpose(step_weight, (0, 2, 1)),
        norm_gain.reshape(1, width),
        signal_taps,
        writer_taps,
        reader_taps,
        step_bias,
        decay_log,
        decay_extra,
        group_gain.reshape(1, chan),
    )


def solution(mesh):
    in_specs = (
        P(("grp", "sp", "dp"), None),
        P(("grp", "sp"), None),
        P("grp"),
        P(),
        P("sp", ("tp", "dp")),
        P("sp", ("tp", "dp")),
        P("sp", ("tp", "dp")),
        P(),
        P(None, ("tp", "dp")),
        P(None, ("tp", "dp")),
        P(None, ("tp", "dp")),
        P(None, ("tp", "dp")),
        P(None, None, ("tp", "dp")),
        P(None, ("tp", "dp")),
        P(None, ("tp", "dp")),
        P(None, ("tp", "dp")),
        P(None, ("tp", "dp")),
        P(None, ("tp", "dp")),
        P(None, ("tp", "dp"), ("grp", "sp")),
        P(("tp", "dp")),
        P(None, ("tp", "dp")),
    )
    out_specs = P(("grp", "sp"), ("tp", "dp"))
    return jax.shard_map(
        on_device, mesh=mesh, in_specs=in_specs, out_specs=out_specs, check_vma=False
    )
```

```python
import functools

import jax
import jax.numpy as jnp
from jax import lax
from jax.experimental import pallas as pl
from jax.experimental.pallas import tpu as pltpu
from jax.sharding import PartitionSpec as P

EPSILON = 1e-06
OVERLAP = True
MESH = pl.DeviceIdType.MESH
F32 = jnp.float32
BF16 = jnp.bfloat16
LANES = 128
NT = (((1,), (1,)), ((), ()))
TN = (((0,), (0,)), ((), ()))


def silu(v):
    return v * (0.5 + 0.5 * jnp.tanh(0.5 * v))


def softplus(v):
    return jnp.maximum(v, 0.0) + jnp.log1p(jnp.exp(-jnp.abs(v)))


def dot(a, b):
    return jnp.dot(a, b, preferred_element_type=F32)


def dot_nt(a, b):
    return lax.dot_general(a, b, NT, preferred_element_type=F32)


def dot_tn(a, b):
    return lax.dot_general(a, b, TN, preferred_element_type=F32)


def remote(src, dst, send, recv, where):
    return pltpu.make_async_remote_copy(
        src_ref=src, dst_ref=dst, send_sem=send, recv_sem=recv, device_id=where, device_id_type=MESH
    )


def aligned(i, n):
    return pl.multiple_of(i * n, n)


def lane_iota(shape):
    return lax.broadcasted_iota(jnp.int32, shape, len(shape) - 1)


def row_iota(shape):
    return lax.broadcasted_iota(jnp.int32, shape, len(shape) - 2)


def expand(cols, first, pair):
    n = cols.shape[0]
    a = first + 2 * pair
    return jnp.where(lane_iota((n, LANES)) < LANES // 2, cols[:, a : a + 1], cols[:, a + 1 : a + 2])


def kernel(
    nz,
    nx,
    latent,
    context,
    shift_w,
    scale_w,
    gate_w,
    og_w,
    sg_w,
    wr_w,
    rd_w,
    out_w,
    *rest,
):
    small_in, rest = rest[:11], rest[11:]
    (
        out,
        cond,
        ctx_cond,
        stepw_in,
        gain,
        signal_taps,
        writer_taps,
        reader_taps,
        bias_in,
        dlog_in,
        extra,
        ggain,
        condrow,
        taps,
        mw,
        lat,
        ctx,
        hidc,
        hid0,
        hid1,
        hid2,
        acc,
        wog,
        wsg,
        wsw,
        wrd,
        wout,
        pay,
        zrecv,
        gpay,
        grecv,
        msum,
        mods,
        ab,
        rinv,
        rinvc,
        craw,
        cedge,
        cstepc,
        raw,
        edge,
        rraw,
        redge,
        rsend,
        esend,
        gbuf,
        stepc,
        sbf,
        wtr,
        rbf,
        ldrow,
        strow,
        xrows,
        xt,
        eexp,
        loc,
        fpre,
        bpre,
        fsend,
        frecv,
        bsend,
        brecv,
        ctsend,
        ctrecv,
        dsend,
        drecv,
        dm,
        ed,
        fback,
        fin,
        bback,
        bin_,
        ybuf,
        nall,
        oacc,
        obuf,
        lsem,
        zs,
        zr,
        ms,
        mr,
        es,
        er,
        res,
        rer,
        ces,
        cer,
        gzs,
        gzr,
        fs,
        fr,
        bs,
        br,
        cs,
        cr,
        ds,
        dr,
        rs,
        rr,
        rbs,
        rbr,
        lats,
        latr,
        gs,
        gr,
        gs2,
        gr2,
        ps,
        pr,
        osem,
    ) = rest
    small = (
        cond,
        ctx_cond,
        stepw_in,
        gain,
        signal_taps,
        writer_taps,
        reader_taps,
        bias_in,
        dlog_in,
        extra,
        ggain,
    )
    scopes = []

    def phase(name):
        if scopes:
            scopes.pop().__exit__(None, None, None)
        if name:
            scopes.append(jax.named_scope(name))
            scopes[-1].__enter__()

    phase("p_start")
    half_rows, width = latent.shape
    span = 2 * half_rows
    nctx = context.shape[0]
    nb = span // LANES
    chan = og_w.shape[1]
    cols = shift_w.shape[1]
    po = chan // nz
    nk = nx * 2
    z = lax.axis_index("sp")
    x = lax.axis_index("tp")
    c = lax.axis_index("dp")
    me = x * 2 + c
    up = lax.rem(z + 1, nz)
    down = lax.rem(z + nz - 1, nz)
    right = lax.rem(x + 1, nx)
    left = lax.rem(x + nx - 1, nx)
    own0 = pl.multiple_of(c * half_rows, half_rows)
    oth0 = pl.multiple_of((1 - c) * half_rows, half_rows)

    pairs = [
        (shift_w, mw.at[0]),
        (scale_w, mw.at[1]),
        (gate_w, mw.at[2]),
        (context, ctx),
        (latent, lat.at[pl.ds(own0, half_rows)]),
        (sg_w, wsg),
        (wr_w, wsw.at[:, 0:LANES]),
        (rd_w, wrd),
        (og_w, wog),
        (out_w, wout),
        *zip(small_in, small),
    ]
    loads = [pltpu.make_async_copy(s, d, lsem.at[i]) for i, (s, d) in enumerate(pairs)]
    barrier = pltpu.get_barrier_semaphore()

    def greet_z(d, _):
        pl.semaphore_signal(barrier, inc=1, device_id={"sp": lax.rem(z + d, nz)}, device_id_type=MESH)
        return 0

    def greet_k(d, _):
        k = lax.rem(me + d, nk)
        pl.semaphore_signal(
            barrier, inc=1, device_id={"tp": k // 2, "dp": lax.rem(k, 2)}, device_id_type=MESH
        )
        return 0

    lax.fori_loop(1, nz, greet_z, 0)
    lax.fori_loop(1, nk, greet_k, 0)
    for i in (10, 11, *range(10), *range(12, len(loads))):
        loads[i].start()

    phase("p_matvec")
    zrows = shift_w.shape[0]
    condrow[...] = jnp.zeros_like(condrow)
    loads[10].wait()
    loads[11].wait()
    condrow[0:1, :] = cond[...].astype(F32).reshape(1, width)
    condrow[1:2, :] = ctx_cond[...].astype(F32).reshape(1, width)
    act = silu(condrow[:, pl.ds(aligned(z, zrows), zrows)]).astype(BF16)
    for i in range(3):
        loads[i].wait()
    y = dot(act, mw[0]) + pltpu.roll(dot(act, mw[1]), 2, 0)
    pay[...] = jnp.concatenate(
        [y[0:4, j * LANES : (j + 1) * LANES] for j in range(cols // LANES)], axis=0
    ).astype(BF16)
    gpay[...] = dot(act, mw[2])[0:1, :]

    phase("p_barrier")
    pl.semaphore_wait(barrier, nz - 1 + nk - 1)
    phase("p_zcast")

    def zcast(d):
        return remote(pay, zrecv.at[z], zs.at[d], zr.at[z], {"sp": lax.rem(z + d, nz)})

    def zcast_start(d, _):
        zcast(d).start()
        return 0

    lax.fori_loop(1, nz, zcast_start, 0)
    lat_copy = remote(latent, lat.at[pl.ds(own0, half_rows)], lats, latr, {"dp": 1 - c})
    lat_copy.start()

    for i in range(12, len(loads)):
        loads[i].wait()

    taps[:, 0:chan] = signal_taps[...]
    taps[:, chan : chan + LANES] = writer_taps[...]
    taps[:, chan + LANES : chan + 2 * LANES] = reader_taps[...]
    sub4 = lax.broadcasted_iota(jnp.int32, (8, 4), 0)
    pick4 = lax.broadcasted_iota(jnp.int32, (8, 4), 1) == lax.rem(sub4, 4)

    def column(ref):
        both = jnp.where(sub4 < 4, ref[0:1, :], ref[1:2, :])
        return jnp.sum(jnp.where(pick4, both, 0.0), axis=1, keepdims=True)

    bias = column(bias_in)
    rate = -jnp.exp(column(dlog_in))

    def step_cols(i, _):
        at = pl.ds(aligned(i, LANES), LANES)
        rows = [
            stepw_in[0, :, at].astype(F32),
            stepw_in[1, :, at].astype(F32),
            jnp.zeros((LANES - 8, LANES), F32),
        ]
        wsw[at, LANES : 2 * LANES] = jnp.transpose(jnp.concatenate(rows, axis=0)).astype(BF16)

    def step_cols4(i, _):
        for n in range(4):
            step_cols(i * 4 + n, 0)
        return 0

    lax.fori_loop(0, width // LANES // 4, step_cols4, 0)

    def rms_rows(src, base, rows, dst):
        at = pl.ds(base, rows)
        sums = jnp.zeros((rows, LANES), F32)
        for j in range(width // LANES):
            xx = src[at, j * LANES : (j + 1) * LANES].astype(F32)
            sums = sums + xx * xx
        total = jnp.sum(sums, axis=1, keepdims=True)
        dst[at, :] = jnp.broadcast_to(lax.rsqrt(total / width + EPSILON), (rows, LANES))

    loads[3].wait()
    rms_rows(ctx, 0, nctx, rinvc)
    loads[4].wait()
    rblock = 64

    def rms_own(i, _):
        rms_rows(lat, pl.multiple_of(own0 + i * rblock, rblock), rblock, rinv)
        return 0

    lax.fori_loop(0, half_rows // rblock, rms_own, 0)
    remote(latent, lat.at[pl.ds(oth0, half_rows)], lats, latr, {"dp": 1 - c}).wait_recv()

    def rms_oth(i, _):
        rms_rows(lat, pl.multiple_of(oth0 + i * rblock, rblock), rblock, rinv)
        return 0

    lax.fori_loop(0, half_rows // rblock, rms_oth, 0)

    phase("p_zwait")
    def add_z(d, acc):
        src = lax.rem(z + nz - d, nz)
        remote(pay, zrecv.at[src], zs.at[d], zr.at[src], {"sp": src}).wait_recv()
        return acc + zrecv[src].astype(F32)

    total = lax.fori_loop(1, nz, add_z, pay[...].astype(F32))
    msum[...] = total
    mods[me] = total

    def mcast(d):
        k = lax.rem(me + d, nk)
        return remote(msum, mods.at[me], ms.at[d], mr.at[me], {"tp": k // 2, "dp": lax.rem(k, 2)})

    def mcast_start(d, _):
        mcast(d).start()
        return 0

    lax.fori_loop(1, nk, mcast_start, 0)
    phase("p_mwait")

    def gcast(d):
        return remote(gpay, grecv.at[z], gzs.at[d], gzr.at[z], {"sp": lax.rem(z + d, nz)})

    def gcast_start(d, _):
        gcast(d).start()
        return 0

    lax.fori_loop(1, nz, gcast_start, 0)

    def mcast_take(d, _):
        k = lax.rem(me + nk - d, nk)
        remote(msum, mods.at[k], ms.at[d], mr.at[k], {"tp": k // 2, "dp": lax.rem(k, 2)}).wait_recv()
        return 0

    lax.fori_loop(1, nk, mcast_take, 0)
    for k in range(nk):
        for j in range(cols // LANES):
            m = mods[k, j * 4 : j * 4 + 4, :]
            at = slice(k * cols + j * LANES, k * cols + (j + 1) * LANES)
            g = gain[:, at]
            ab[0:1, at] = g * (1.0 + m[2:3])
            ab[1:2, at] = m[0:1]
            ab[2:3, at] = g * (1.0 + m[3:4])
            ab[3:4, at] = m[1:2]
    phase("p_mod0")
    tile = hid1.shape[0]
    both = chan + LANES
    piece_cols = 512
    steps = width // piece_cols

    def modulate(src, base, rows, inv, row, dst, to, kk):
        for j in range(piece_cols // LANES):
            start = kk * piece_cols + j * LANES
            at = pl.ds(start if isinstance(start, int) else pl.multiple_of(start, LANES), LANES)
            up_row = ab[row : row + 1, at]
            add_row = ab[row + 1 : row + 2, at]
            for i in range(rows // 32):
                r = inv[base + i * 32 : base + (i + 1) * 32, :]
                xx = src[base + i * 32 : base + (i + 1) * 32, at].astype(F32)
                dst[to + i * 32 : to + (i + 1) * 32, at] = (xx * r * up_row + add_row).astype(BF16)

    def multiply(h):
        rows = h.shape[0]
        acc[0:rows, 0:chan] = dot(h[...], wsg[...])
        acc[0:rows, chan : chan + 2 * LANES] = dot(h[...], wsw[...])

    def modulate_tile(t, dst):
        if OVERLAP:
            for kk in range(steps):
                modulate(lat, t * tile, tile, rinv, 0, dst, 0, kk)
        else:

            def turn(kk, _):
                modulate(lat, t * tile, tile, rinv, 0, dst, 0, kk)
                return 0

            lax.fori_loop(0, steps, turn, 0)

    def mod_ctx(kk, _):
        modulate(ctx, 0, nctx, rinvc, 2, hidc, 0, kk)
        modulate(lat, 0, 32, rinv, 0, hidc, nctx, kk)
        modulate(lat, span - 32, 32, rinv, 0, hidc, nctx + 32, kk)
        return 0

    lax.fori_loop(0, steps, mod_ctx, 0)
    for i in range(5, 8):
        loads[i].wait()
    multiply(hidc)
    craw[8 : 8 + nctx, :] = acc[0:nctx, 0:both]
    cstepc[0:nctx, :] = acc[0:nctx, both : both + LANES]
    cedge_up = remote(craw.at[nctx : nctx + 8], cedge.at[0], ces.at[0], cer.at[0], {"sp": up})
    cedge_down = remote(craw.at[8:16], cedge.at[1], ces.at[1], cer.at[1], {"sp": down})
    cedge_up.start()
    cedge_down.start()
    esend[0] = acc[nctx + 56 : nctx + 64, 0:both]
    esend[1] = acc[nctx : nctx + 8, 0:both]
    rends = dot(hidc[nctx : nctx + 64, :], wrd[...])
    rsend[0] = rends[56:64, :]
    rsend[1] = rends[0:8, :]
    edge_up = remote(esend.at[0], edge.at[0], es.at[0], er.at[0], {"sp": up})
    edge_down = remote(esend.at[1], edge.at[1], es.at[1], er.at[1], {"sp": down})
    redge_up = remote(rsend.at[0], redge.at[0], res.at[0], rer.at[0], {"sp": up})
    redge_down = remote(rsend.at[1], redge.at[1], res.at[1], rer.at[1], {"sp": down})
    for sent in (edge_up, edge_down, redge_up, redge_down):
        sent.start()

    def mod_first(kk, _):
        modulate(lat, 0, tile, rinv, 0, hid0, 0, kk)
        return 0

    lax.fori_loop(0, steps, mod_first, 0)
    phase("p_dots0")
    modulate_tile(2, hid2)
    multiply(hid0)
    raw[8 : 8 + tile, :] = acc[0:tile, 0:both]
    stepc[0:tile, :] = acc[0:tile, both : both + LANES]
    phase("p_ctxstate")
    def conv(block, at):
        n = block.shape[0]
        mix = (
            taps[0:1, at] * pltpu.roll(block, 1, 0)
            + taps[1:2, at] * block
            + taps[2:3, at] * pltpu.roll(block, n - 1, 0)
        )
        return silu(mix[8 : n - 8])

    first = (z == 0).astype(F32)
    last = (z == nz - 1).astype(F32)
    cedge_up.wait_recv()
    cedge_down.wait_recv()
    craw[7:8, :] = cedge[0, 7:8, :] * (1.0 - first)
    craw[8 + nctx : 9 + nctx, :] = cedge[1, 0:1, :] * (1.0 - last)
    is_fwd = row_iota((8, LANES)) < 4
    lane8 = lane_iota((8, LANES))
    tri = (
        lax.broadcasted_iota(jnp.int32, (LANES, LANES), 0)
        <= lax.broadcasted_iota(jnp.int32, (LANES, LANES), 1)
    ).astype(F32)

    def cumulate(a):
        return jnp.dot(a, tri, precision=lax.Precision.HIGHEST, preferred_element_type=F32)

    cstep = jnp.transpose(cstepc[...])[0:8, :]
    cst = softplus(cstep.astype(BF16).astype(F32) + bias)
    cst = jnp.where(lane8 < nctx, cst, 0.0)
    cld = rate * cst
    ccum = cumulate(cld)
    cend = ccum[:, LANES - 1 : LANES]
    cw = jnp.where(is_fwd, jnp.exp(cend - ccum), jnp.exp(ccum - cld)) * cst
    xrows[0, 0:8, :] = cw
    cwt = jnp.transpose(xrows[0:4].reshape(LANES, LANES))[0:nctx, :]
    cblock = [
        conv(craw[0 : nctx + 16, j * LANES : (j + 1) * LANES], slice(j * LANES, (j + 1) * LANES))
        for j in range(chan // LANES + 1)
    ]
    cwr = cblock[-1].astype(BF16)
    for k in range(2):
        for p in range(chan // LANES):
            sc = (cblock[p] * expand(cwt, 4 * k, p)).astype(BF16)
            st = dot_tn(sc, cwr).astype(BF16)
            per = LANES // po
            ctsend[p * per : (p + 1) * per, k] = st.reshape(per, po, LANES)

    def ctcast(d):
        t = lax.rem(z + d, nz)
        return remote(ctsend.at[t], ctrecv.at[z], cs.at[d], cr.at[z], {"sp": t})

    def ctcast_start(d, _):
        ctcast(d).start()
        return 0

    lax.fori_loop(1, nz, ctcast_start, 0)
    ctrecv[z] = ctsend[z]
    phase("p_dots2")
    modulate_tile(1, hid1)
    multiply(hid2)
    raw[8 + 2 * tile : 8 + 3 * tile, :] = acc[0:tile, 0:both]
    stepc[2 * tile : 3 * tile, :] = acc[0:tile, both : both + LANES]
    phase("p_dots1")
    multiply(hid1)
    raw[8 + tile : 8 + 2 * tile, :] = acc[0:tile, 0:both]
    stepc[tile : 2 * tile, :] = acc[0:tile, both : both + LANES]

    phase("p_edge")
    edge_up.wait_recv()
    edge_down.wait_recv()
    raw[7:8, :] = edge[0, 7:8, :] * (1.0 - first)
    raw[8 + span : 9 + span, :] = edge[1, 0:1, :] * (1.0 - last)

    phase("p_conv")

    def conv_block(b, _):
        base = aligned(b, LANES)
        for j in range(chan // LANES + 1):
            at = slice(j * LANES, (j + 1) * LANES)
            val = conv(raw[pl.ds(base, LANES + 16), at], at)
            if j < chan // LANES:
                sbf[pl.ds(base, LANES), at] = val.astype(BF16)
            else:
                wtr[b] = jnp.transpose(val).astype(BF16)
        return 0

    lax.fori_loop(0, nb, conv_block, 0)

    phase("p_rows")
    for b in range(nb):
        turned = jnp.transpose(stepc[b * LANES : (b + 1) * LANES, :])[0:8, :]
        st = softplus(turned.astype(BF16).astype(F32) + bias)
        strow[b] = st
        ldrow[b] = rate * st + jnp.concatenate(
            [extra[0, :, b * LANES : (b + 1) * LANES], extra[1, :, b * LANES : (b + 1) * LANES]], axis=0
        )
    cum = cumulate(ldrow[...].reshape(nb * 8, LANES))
    ends = [cum[b * 8 : b * 8 + 8, LANES - 1 : LANES] for b in range(nb)]
    zero = jnp.zeros((8, 1), F32)
    before = [zero]
    for b in range(nb):
        before.append(before[-1] + ends[b])
    after = [zero]
    for b in reversed(range(nb)):
        after.append(after[-1] + ends[b])
    after = after[::-1]
    isf1 = row_iota((8, 1)) < 4
    for b in range(nb):
        cb = cum[b * 8 : b * 8 + 8]
        e = cb - ldrow[b]
        end = ends[b]
        near = jnp.where(is_fwd, cb, end - e)
        xrows[b, 0:8, :] = jnp.where(is_fwd, cb, e)
        xrows[b, 8:16, :] = jnp.where(is_fwd, jnp.exp(end - cb), jnp.exp(e)) * strow[b]
        xrows[b, 16:24, :] = jnp.exp(near)
        xrows[b, 24:32, :] = jnp.exp(near + jnp.where(isf1, before[b], after[b + 1]))
        eexp[b] = jnp.broadcast_to(jnp.exp(end), (8, LANES))
    for g in range(-(-nb // 4)):
        turned = jnp.transpose(xrows[g * 4 : g * 4 + 4].reshape(LANES, LANES))
        for b in range(g * 4, min(nb, g * 4 + 4)):
            xt[b] = turned[:, (b - g * 4) * 32 : (b - g * 4 + 1) * 32]

    phase("p_states")
    npair = chan // LANES
    def decays(b, row):
        lanes = lane_iota((1, LANES)) < LANES // 2
        return [
            jnp.where(lanes, eexp[b, r : r + 1, :], eexp[b, r + 1 : r + 2, :])
            for r in range(row, row + 2 * npair, 2)
        ]

    sub8 = row_iota((8, LANES))
    dsend[...] = jnp.sum(
        jnp.where(lane8 == sub8, before[nb], 0.0) + jnp.where(lane8 == sub8 + 8, cend, 0.0),
        axis=0,
        keepdims=True,
    )

    def dcast(d):
        return remote(dsend, drecv.at[z], ds.at[d], dr.at[z], {"sp": lax.rem(z + d, nz)})

    def fcast(d):
        t = lax.rem(z + d, nz)
        return remote(fsend.at[t], frecv.at[z], fs.at[d], fr.at[z], {"sp": t})

    def bcast(d):
        t = lax.rem(z + d, nz)
        return remote(bsend.at[t], brecv.at[z], bs.at[d], br.at[z], {"sp": t})

    def dcast_start(d, _):
        dcast(d).start()
        return 0

    def fcast_start(d, _):
        fcast(d).start()
        return 0

    def bcast_start(d, _):
        bcast(d).start()
        return 0

    lax.fori_loop(1, nz, dcast_start, 0)
    drecv[z] = dsend[...]

    def contribute(first):
        for b in range(nb):
            cl = xt[b]
            parts = [
                sbf[b * LANES : (b + 1) * LANES, p * LANES : (p + 1) * LANES].astype(F32)
                * expand(cl, first, p)
                for p in range(npair)
            ]
            loc[b] = dot(wtr[b], jnp.concatenate(parts, axis=1).astype(BF16))

    def chain(order, row, before_ref, send_ref):
        per = LANES // po
        state = [jnp.zeros((LANES, LANES), F32) for _ in range(npair)]
        for b in order:
            by = decays(b, row)
            for p in range(npair):
                at = slice(p * LANES, (p + 1) * LANES)
                before_ref[b, :, at] = state[p].astype(BF16)
                state[p] = state[p] * by[p] + loc[b, :, at]
        for p in range(npair):
            turned = jnp.transpose(state[p]).astype(BF16)
            send_ref[p * per : (p + 1) * per] = turned.reshape(per, po, LANES)

    contribute(8)
    chain(range(nb), 0, fpre, fsend)
    lax.fori_loop(1, nz, fcast_start, 0)
    frecv[z] = fsend[z]
    contribute(12)
    chain(range(nb - 1, -1, -1), 4, bpre, bsend)
    lax.fori_loop(1, nz, bcast_start, 0)
    brecv[z] = bsend[z]

    phase("p_gate")
    loads[8].wait()
    hids = (hid0, hid1, hid2)
    for t in (0, 2, 1):
        rraw[8 + t * tile : 8 + (t + 1) * tile, :] = dot(hids[t][...], wrd[...])
    for t in range(3):
        gbuf[t * tile : (t + 1) * tile, :] = silu(dot(hids[t][...], wog[...]))
    redge_up.wait_recv()
    redge_down.wait_recv()
    rraw[7:8, :] = redge[0, 7:8, :] * (1.0 - first)
    rraw[8 + span : 9 + span, :] = redge[1, 0:1, :] * (1.0 - last)

    def conv_reader(b, _):
        base = aligned(b, LANES)
        block = rraw[pl.ds(base, LANES + 16), :]
        rbf[pl.ds(base, LANES), :] = conv(block, slice(both, both + LANES)).astype(BF16)
        return 0

    lax.fori_loop(0, nb, conv_reader, 0)

    phase("p_inside")
    lower = lax.broadcasted_iota(jnp.int32, (LANES, LANES), 1) <= lax.broadcasted_iota(
        jnp.int32, (LANES, LANES), 0
    )
    upper = lax.broadcasted_iota(jnp.int32, (LANES, LANES), 1) >= lax.broadcasted_iota(
        jnp.int32, (LANES, LANES), 0
    )

    def inside(b, _):
        base = aligned(b, LANES)
        r = rbf[pl.ds(base, LANES), :]
        g = dot(r, wtr[b])
        from_left = dot(r, fpre[b])
        from_right = dot(r, bpre[b])
        cl = xt[b]
        for p in range(npair):
            at = slice(p * LANES, (p + 1) * LANES)
            s = sbf[pl.ds(base, LANES), at]
            own = []
            for h in (2 * p, 2 * p + 1):
                arg = jnp.where(
                    lower,
                    cl[:, h : h + 1] - xrows[b, h : h + 1, :],
                    xrows[b, 4 + h : 5 + h, :] - cl[:, 4 + h : 5 + h],
                )
                wgt = jnp.where(lower, strow[b, h : h + 1, :], 0.0) + jnp.where(
                    upper, strow[b, 4 + h : 5 + h, :], 0.0
                )
                own.append(dot((g * jnp.exp(arg) * wgt).astype(BF16), s))
            carried = expand(cl, 16, p) * from_left[:, at] + expand(cl, 20, p) * from_right[:, at]
            ybuf[pl.ds(base, LANES), at] = carried + jnp.where(
                lane_iota((LANES, LANES)) < LANES // 2, own[0], own[1]
            )
        return 0

    def inside2(i, _):
        inside(2 * i, 0)
        inside(2 * i + 1, 0)
        return 0

    lax.fori_loop(0, nb // 2, inside2, 0)

    phase("p_fwait")

    def take_forward(d, _):
        src = lax.rem(z + nz - d, nz)
        remote(dsend, drecv.at[src], ds.at[d], dr.at[src], {"sp": src}).wait_recv()
        remote(ctsend.at[src], ctrecv.at[src], cs.at[d], cr.at[src], {"sp": src}).wait_recv()
        remote(fsend.at[src], frecv.at[src], fs.at[d], fr.at[src], {"sp": src}).wait_recv()
        return 0

    lax.fori_loop(1, nz, take_forward, 0)
    phase("p_fscan")
    for k in range(nz):
        dm[k : k + 1, :] = drecv[k]
    head = z * po // (LANES // 2)
    dall = dm[...]
    lane_z = lane_iota((nz, LANES))
    for i in range(4):
        col = jnp.sum(jnp.where(lane_z == 4 * i + head, dall, 0.0), axis=1, keepdims=True)
        ed[i] = jnp.exp(jnp.broadcast_to(col, (nz, LANES)))
    state = jnp.zeros((po, LANES), F32)
    for k in range(nz):
        state = ed[2, k : k + 1, :] * state + ctrecv[k, 0].astype(F32)
    for k in range(nz):
        fback[k] = state.astype(BF16)
        state = ed[0, k : k + 1, :] * state + frecv[k].astype(F32)

    def fret(d):
        t = lax.rem(z + d, nz)
        return remote(fback.at[t], fin.at[z], rs.at[d], rr.at[z], {"sp": t})

    def fret_start(d, _):
        fret(d).start()
        return 0

    def bret(d):
        t = lax.rem(z + d, nz)
        return remote(bback.at[t], bin_.at[z], rbs.at[d], rbr.at[z], {"sp": t})

    def bret_start(d, _):
        bret(d).start()
        return 0

    lax.fori_loop(1, nz, fret_start, 0)
    fin[z] = fback[z]
    phase("p_bwait")

    def take_backward(d, _):
        src = lax.rem(z + nz - d, nz)
        remote(bsend.at[src], brecv.at[src], bs.at[d], br.at[src], {"sp": src}).wait_recv()
        return 0

    lax.fori_loop(1, nz, take_backward, 0)
    phase("p_bscan")
    state = jnp.zeros((po, LANES), F32)
    for k in reversed(range(nz)):
        state = ed[3, k : k + 1, :] * state + ctrecv[k, 1].astype(F32)
    for k in reversed(range(nz)):
        bback[k] = state.astype(BF16)
        state = ed[1, k : k + 1, :] * state + brecv[k].astype(F32)
    lax.fori_loop(1, nz, bret_start, 0)
    bin_[z] = bback[z]
    phase("p_retwait")
    lat_copy.wait_send()
    for sent in (cedge_up, cedge_down, edge_up, edge_down, redge_up, redge_down):
        sent.wait_send()

    def drain_z(d, _):
        zcast(d).wait_send()
        ctcast(d).wait_send()
        gcast(d).wait_send()
        fcast(d).wait_send()
        bcast(d).wait_send()
        dcast(d).wait_send()
        return 0

    lax.fori_loop(1, nz, drain_z, 0)

    def drain_k(d, _):
        mcast(d).wait_send()
        return 0

    lax.fori_loop(1, nk, drain_k, 0)

    def take_return(d, _):
        src = lax.rem(z + nz - d, nz)
        remote(bback.at[src], bin_.at[src], rbs.at[d], rbr.at[src], {"sp": src}).wait_recv()
        return 0

    def add_gate(d, total):
        src = lax.rem(z + nz - d, nz)
        remote(gpay, grecv.at[src], gzs.at[d], gzr.at[src], {"sp": src}).wait_recv()
        return total + grecv[src]

    gate = lax.fori_loop(1, nz, add_gate, gpay[...])

    def take_left(d, _):
        src = lax.rem(z + nz - d, nz)
        remote(fback.at[src], fin.at[src], rs.at[d], rr.at[src], {"sp": src}).wait_recv()
        return 0

    lax.fori_loop(1, nz, take_left, 0)

    def add_left(b, _):
        rows = pl.ds(aligned(b, LANES), LANES)
        r = rbf[rows, :]
        cl = xt[b]
        per = LANES // po
        for p in range(npair):
            at = slice(p * LANES, (p + 1) * LANES)
            f_in = fin[p * per : (p + 1) * per].reshape(LANES, LANES)
            ybuf[rows, at] += expand(cl, 24, p) * dot_nt(r, f_in)
        return 0

    lax.fori_loop(0, nb, add_left, 0)
    lax.fori_loop(1, nz, take_return, 0)

    phase("p_finish")
    hrow = LANES // 2

    def piece(k, b):
        return nall.at[k, pl.ds(aligned(b, LANES), LANES)]

    def part(k, b, h):
        return nall.at[k, pl.ds(pl.multiple_of(b * LANES + h * hrow, hrow), hrow)]

    def to_partner(k, i, b):
        return remote(piece(k, b), piece(k, b), ps.at[i, b], pr.at[i, b], {"dp": 1 - c})

    k_left = left * 2 + c
    k_right = right * 2 + c
    k_far = lax.rem(x + 2, nx) * 2 + c

    def own_right(b):
        return remote(piece(me, b), piece(me, b), gs.at[0, b], gr.at[0, b], {"tp": right})

    def own_left(b):
        return remote(piece(me, b), piece(me, b), gs.at[1, b], gr.at[1, b], {"tp": left})

    def relay_right(b):
        return remote(part(k_left, b, 0), part(k_left, b, 0), gs2.at[0, b], gr2.at[0, b], {"tp": right})

    def relay_left(b):
        return remote(part(k_right, b, 1), part(k_right, b, 1), gs2.at[1, b], gr2.at[1, b], {"tp": left})

    def finish(b, _):
        base = aligned(b, LANES)
        r = rbf[pl.ds(base, LANES), :]
        cl = xt[b]
        vals = []
        for p in range(npair):
            at = slice(p * LANES, (p + 1) * LANES)
            per = LANES // po
            b_in = bin_[p * per : (p + 1) * per].reshape(LANES, LANES)
            yy = (
                ybuf[pl.ds(base, LANES), at]
                + expand(cl, 28, p) * dot_nt(r, b_in)
            )
            vals.append(yy * gbuf[pl.ds(base, LANES), at])
        sq = sum(jnp.sum(a * a, axis=1, keepdims=True) for a in vals)
        inv = lax.rsqrt(sq / chan + EPSILON)
        for p in range(npair):
            at = slice(p * LANES, (p + 1) * LANES)
            nall[me, pl.ds(base, LANES), at] = (vals[p] * inv * ggain[:, at]).astype(BF16)
        own_right(b).start()
        own_left(b).start()
        to_partner(me, 0, b).start()
        return 0

    lax.fori_loop(0, nb, finish, 0)
    loads[9].wait()

    phase("p_collect")
    out0 = pl.multiple_of(me * cols, cols)

    flip = 1 - 2 * c

    def product(b, ks):
        base = aligned(b, LANES)
        total = None
        for k in ks:
            w = wout[pl.ds(aligned(k, chan), chan), :]
            part_sum = dot(nall[k, pl.ds(base, LANES), :], w)
            total = part_sum if total is None else total + part_sum
        return total

    def near(b):
        remote(piece(k_left, b), piece(k_left, b), gs.at[0, b], gr.at[0, b], {"tp": left}).wait_recv()
        relay_right(b).start()
        to_partner(k_left, 1, b).start()
        remote(piece(k_right, b), piece(k_right, b), gs.at[1, b], gr.at[1, b], {"tp": right}).wait_recv()
        relay_left(b).start()
        to_partner(k_right, 2, b).start()

    def near_product(b):
        for n, k in enumerate((me, k_left, k_right)):
            to_partner(k + flip, n, b).wait_recv()
        ks = (me, k_left, k_right, me + flip, k_left + flip, k_right + flip)
        oacc[pl.ds(aligned(b, LANES), LANES), :] = product(b, ks)

    near(0)

    def near_turn(b, _):
        near(b)
        near_product(b - 1)
        return 0

    lax.fori_loop(1, nb, near_turn, 0)
    near_product(nb - 1)
    phase("p_far")

    def far(b):
        for h in range(2):
            remote(part(k_far, b, h), part(k_far, b, h), gs2.at[h, b], gr2.at[h, b], {"tp": left}).wait_recv()
        to_partner(k_far, 3, b).start()

    def store(b):
        rows = pl.ds(aligned(b, LANES), LANES)
        return pltpu.make_async_copy(obuf.at[rows], out.at[rows], osem.at[b])

    def far_product(b):
        to_partner(k_far + flip, 3, b).wait_recv()
        rows = pl.ds(aligned(b, LANES), LANES)
        mix = oacc[rows, :] + product(b, (k_far, k_far + flip))
        res_rows = lat[rows, pl.ds(out0, cols)].astype(F32)
        obuf[rows, :] = (res_rows + gate * mix).astype(BF16)
        store(b).start()

    far(0)

    def far_turn(b, _):
        far(b)
        far_product(b - 1)
        return 0

    lax.fori_loop(1, nb, far_turn, 0)
    far_product(nb - 1)

    phase("p_drain")

    def drain_back(d, _):
        fret(d).wait_send()
        bret(d).wait_send()
        return 0

    lax.fori_loop(1, nz, drain_back, 0)

    def drain_b(b, _):
        own_right(b).wait_send()
        own_left(b).wait_send()
        relay_right(b).wait_send()
        relay_left(b).wait_send()
        for i in range(4):
            to_partner(me, i, b).wait_send()
        store(b).wait()
        return 0

    lax.fori_loop(0, nb, drain_b, 0)
    phase(None)


def on_device(
    latent,
    context,
    condition,
    context_condition,
    shift_weight,
    scale_weight,
    gate_weight,
    norm_gain,
    out_gate_weight,
    signal_weight,
    writer_weight,
    reader_matrix,
    step_weight,
    signal_taps,
    writer_taps,
    reader_taps,
    step_bias,
    decay_log,
    decay_extra,
    group_gain,
    output_weight,
):
    nz, nx = lax.axis_size("sp"), lax.axis_size("tp")
    half_rows, width = latent.shape
    span, nctx = 2 * half_rows, context.shape[0]
    chan, cols = out_gate_weight.shape[1], shift_weight.shape[1]
    nb, nk, po = span // LANES, 2 * nx, chan // nz
    full = chan + 2 * LANES
    tile = span // 3
    both = chan + LANES
    hbm = pl.BlockSpec(memory_space=pl.ANY)
    dma = pltpu.SemaphoreType.DMA
    heads = step_bias.shape[1]
    scratch = [
        (condition.shape, BF16),
        (context_condition.shape, BF16),
        ((2, heads, width), BF16),
        ((1, width), F32),
        (signal_taps.shape, F32),
        (writer_taps.shape, F32),
        (reader_taps.shape, F32),
        (step_bias.shape, F32),
        (decay_log.shape, F32),
        (decay_extra.shape, F32),
        ((1, chan), F32),
        ((8, width), F32),
        ((3, full), F32),
        ((3, *shift_weight.shape), BF16),
        ((span, width), BF16),
        ((nctx, width), BF16),
        ((nctx + 64, width), BF16),
        ((tile, width), BF16),
        ((tile, width), BF16),
        ((tile, width), BF16),
        ((tile, full), F32),
        ((width, chan), BF16),
        ((width, chan), BF16),
        ((width, 2 * LANES), BF16),
        ((width, LANES), BF16),
        (output_weight.shape, BF16),
        ((cols // LANES * 4, LANES), BF16),
        ((nz, cols // LANES * 4, LANES), BF16),
        ((1, cols), F32),
        ((nz, 1, cols), F32),
        ((cols // LANES * 4, LANES), F32),
        ((nk, cols // LANES * 4, LANES), F32),
        ((8, width), F32),
        ((span, LANES), F32),
        ((nctx, LANES), F32),
        ((nctx + 16, both), F32),
        ((2, 8, both), F32),
        ((LANES, LANES), F32),
        ((span + 16, both), F32),
        ((2, 8, both), F32),
        ((span + 16, LANES), F32),
        ((2, 8, LANES), F32),
        ((2, 8, LANES), F32),
        ((2, 8, both), F32),
        ((span, chan), F32),
        ((span, LANES), F32),
        ((span, chan), BF16),
        ((nb, LANES, LANES), BF16),
        ((span, LANES), BF16),
        ((nb, 8, LANES), F32),
        ((nb, 8, LANES), F32),
        ((-(-nb // 4) * 4, 32, LANES), F32),
        ((nb, LANES, 32), F32),
        ((nb, 8, LANES), F32),
        ((nb, LANES, chan), F32),
        ((nb, LANES, chan), BF16),
        ((nb, LANES, chan), BF16),
        ((nz, po, LANES), BF16),
        ((nz, po, LANES), BF16),
        ((nz, po, LANES), BF16),
        ((nz, po, LANES), BF16),
        ((nz, 2, po, LANES), BF16),
        ((nz, 2, po, LANES), BF16),
        ((1, LANES), F32),
        ((nz, 1, LANES), F32),
        ((nz, LANES), F32),
        ((4, nz, LANES), F32),
        ((nz, po, LANES), BF16),
        ((nz, po, LANES), BF16),
        ((nz, po, LANES), BF16),
        ((nz, po, LANES), BF16),
        ((span, chan), F32),
        ((nk, span, chan), BF16),
        ((span, cols), F32),
        ((span, cols), BF16),
    ]
    sems = (
        [(21,), (nz,), (nz,), (nk,), (nk,)]
        + [(2,)] * 6
        + [(nz,)] * 14
        + [None, None]
        + [(2, nb)] * 4
        + [(4, nb)] * 2
        + [(nb,)]
    )
    return pl.pallas_call(
        functools.partial(kernel, nz, nx),
        out_shape=jax.ShapeDtypeStruct((span, cols), BF16),
        in_specs=[hbm] * 21,
        out_specs=hbm,
        scratch_shapes=[pltpu.VMEM(s, t) for s, t in scratch]
        + [dma if s is None else dma(s) for s in sems],
        compiler_params=pltpu.CompilerParams(
            collective_id=0, has_side_effects=True, vmem_limit_bytes=56 * 1024 * 1024
        ),
        name="mixing",
    )(
        latent,
        context,
        shift_weight,
        scale_weight,
        gate_weight,
        out_gate_weight,
        signal_weight,
        writer_weight,
        reader_matrix,
        output_weight,
        condition,
        context_condition,
        jnp.transpose(step_weight, (0, 2, 1)),
        norm_gain.reshape(1, width),
        signal_taps,
        writer_taps,
        reader_taps,
        step_bias,
        decay_log,
        decay_extra,
        group_gain.reshape(1, chan),
    )


def solution(mesh):
    in_specs = (
        P(("grp", "sp", "dp"), None),
        P(("grp", "sp"), None),
        P("grp"),
        P(),
        P("sp", ("tp", "dp")),
        P("sp", ("tp", "dp")),
        P("sp", ("tp", "dp")),
        P(),
        P(None, ("tp", "dp")),
        P(None, ("tp", "dp")),
        P(None, ("tp", "dp")),
        P(None, ("tp", "dp")),
        P(None, None, ("tp", "dp")),
        P(None, ("tp", "dp")),
        P(None, ("tp", "dp")),
        P(None, ("tp", "dp")),
        P(None, ("tp", "dp")),
        P(None, ("tp", "dp")),
        P(None, ("tp", "dp"), ("grp", "sp")),
        P(("tp", "dp")),
        P(None, ("tp", "dp")),
    )
    out_specs = P(("grp", "sp"), ("tp", "dp"))
    return jax.shard_map(
        on_device, mesh=mesh, in_specs=in_specs, out_specs=out_specs, check_vma=False
    )
```
